32 devices in a mesh: sp: 8 (over z, y), tp: 4 (over x, core).
Axes of the slice: x: 2, y: 2, z: 4, core: 2. Of those that a mesh axis runs over, the one named last changes fastest.
Arguments:
- queries: bfloat16 [4096, 1024], P('sp', 'tp'), may hold values from -6 to 6
- key_heads: bfloat16 [4096, 512], P('sp', 'tp'), may hold values from -6 to 6
- value_heads: bfloat16 [4096, 512], P('sp', 'tp'), may hold values from -70 to 70
- documents: int32 [4096], P('sp'), may hold values from 0 to 2, never falling along the last dimension, each value on 1 to 2560 neighbouring positions
- query_gain: float32 [128], replicated, may hold values from 0.1 to 8
- key_gain: float32 [128], replicated, may hold values from 0.1 to 8
- out_gain: float32 [1024], replicated, may hold values from 0.1 to 1.9
- out_proj: bfloat16 [1024, 2048], replicated, may hold values from -0.1875 to 0.1875
- residual: bfloat16 [4096, 2048], P(('sp', 'tp')), may hold values from -6 to 6
- mid_gain: float32 [2048], replicated, may hold values from 0.1 to 1.9
- mid_bias: float32 [2048], replicated, may hold values from -1.5 to 1.5
- routes: int32 [4096, 2], P(('sp', 'tp')), may hold values from 0 to 31, all different within a row; in each aligned block of 128 rows (0 to 127, 128 to 255, ...) at most 16 rows name the same one
- route_weights: float32 [4096, 2], P(('sp', 'tp')), may hold values from 0.2 to 2
- expert_gate: bfloat16 [32, 2048, 512], P(('sp', 'tp')), may hold values from -0.125 to 0.125
- expert_up: bfloat16 [32, 2048, 512], P(('sp', 'tp')), may hold values from -0.125 to 0.125
- expert_down: bfloat16 [32, 512, 2048], P(('sp', 'tp')), may hold values from -0.25 to 0.25
- final_gain: float32 [2048], replicated, may hold values from 0.1 to 1.9
- final_bias: float32 [2048], replicated, may hold values from -1.5 to 1.5
Outputs:
- layer_out: bfloat16 [4096, 2048], P(('sp', 'tp'))
The draws below stay inside these ranges and needn't reach their ends.
Inputs may be any that keep to these rules, and one draw needn't show every extreme that they name: `documents`: never falls along the sequence; each document holds 1 to 2560 positions and one holds exactly 2560. `routes`: each row names 2 different experts; among the rows of one device (aligned blocks of 128 rows) no expert is named more than 16 times, and exactly 16 times in some block.
All inputs are finite; a program needn't handle non-finite values.
Results may differ from the reference program's by a relative error of at most 0.014.
The reference program's roundings to bfloat16 on the way count: a program that leaves them out, or rounds other values in their place, can miss the bound.
Values may be sent and summed in bfloat16 or wider, within the bound.
A program may use at most 128 MiB of HBM per device.

```python
import math
import jax
import jax.numpy as jnp
import numpy as np
from jax import lax

D = 2048
HEAD = 128
QH = 8
KVH = 4
GRID = 64
DE = 512
TOP_K = 2
TOKENS = 4096
ROWS = 128
EXPERTS = 32
CAP = 16
DOCS = 3
DOC_MOST = 2560
N_SP = 8
N_TP = 4


def drawn_keys(key):
    sub_key = jax.random.fold_in(key, 202)
    drawn = jnp.clip(jax.random.normal(sub_key, (TOKENS, KVH * HEAD), jnp.float32), -6.0, 6.0)
    return drawn


def draw_key_heads(key, part):
    return drawn_keys(key).astype(jnp.bfloat16)


def draw_queries(key, part):
    sub_key = jax.random.fold_in(key, 301)
    drawn = jnp.clip(jax.random.normal(sub_key, (TOKENS, QH * HEAD), jnp.float32), -6.0, 6.0)
    return drawn.astype(jnp.bfloat16)


def draw_value_heads(key, part):
    sub_key = jax.random.fold_in(key, 501)
    head_index = jnp.arange(KVH, dtype=jnp.float32)
    head_scale = jnp.repeat(4.0 ** (head_index / (KVH - 1)), HEAD)
    drawn = jnp.clip(jax.random.normal(sub_key, (TOKENS, KVH * HEAD), jnp.float32), -4.0, 4.0)
    return (drawn * head_scale[None, :]).astype(jnp.bfloat16)


def gain_values(key):
    return jnp.clip(1.0 + 0.18 * jax.random.normal(key, (HEAD,), jnp.float32), 0.1, 1.9)


def draw_query_gain(key, part):
    return gain_values(jax.random.fold_in(key, 401))


def draw_key_gain(key, part):
    return gain_values(jax.random.fold_in(key, 402))


def levels(stream_key, shape, shards, smallest, largest):
    loudness, own = 1.0, jax.random.fold_in(stream_key, 6)
    for position, shards_of in shards:
        heights = jnp.exp(jax.random.uniform(jax.random.fold_in(own, position), (shards_of,), jnp.float32, smallest / len(shards), largest / len(shards)))
        loudness = loudness * jnp.repeat(heights, shape[position] // shards_of).reshape([-1 if axis == position else 1 for axis in range(len(shape))])
    return loudness


def profile(amount, total, limit, skew):
    portions = [(1 << 20) // math.isqrt(rank ** skew) + 1 for rank in range(2, amount + 1)]
    surplus, holding = total - limit - (amount - 1), [1] * (amount - 1)
    while surplus > 0:
        movable = [i for i in range(amount - 1) if holding[i] < limit]
        whole, left = sum([portions[i] for i in movable]), surplus
        for i in movable:
            extra = min(limit - holding[i], max(1, left * portions[i] // whole), surplus)
            holding[i] = holding[i] + extra
            surplus = surplus - extra
    return np.array([limit] + holding)


def uneven_parts(rng, amount, total, limit, skew):
    if amount == 2:
        one = jax.random.randint(rng, (), max(1, total - limit), min(limit, total - 1) + 1)
        return jnp.stack([one, total - one])
    tallies = jnp.asarray(profile(amount, total, limit, skew), jnp.int32)
    twos = (amount - 1) // 2
    donor, taker = tallies[1:1 + 2 * twos:2], tallies[2:2 + 2 * twos:2]
    room = jnp.minimum(donor - 1, limit - taker)
    passed = jax.random.randint(jax.random.fold_in(rng, 1), (twos,), 0, 1 << 20) % (room + 1)
    tallies = tallies.at[1:1 + 2 * twos:2].set(donor - passed).at[2:2 + 2 * twos:2].set(taker + passed)
    return tallies[jax.random.permutation(jax.random.fold_in(rng, 2), amount)]


def assign_block(key, own, number, rows, number_of, top, limit, slope):
    order = jax.random.permutation(key, number_of)
    crowded, common = portions_of(number_of, rows * top, limit, slope, True), portions_of(number_of, rows * top, limit, slope, False)
    places = jnp.arange(number_of)

    def named(sizes, offset_by):
        used = int((sizes > 0).sum())
        fixed = max(1, used // 4)
        passed = fixed + (places - fixed + offset_by * (used - fixed)) % max(1, number_of - fixed)
        return jnp.zeros((number_of,), jnp.int32).at[order[jnp.where(places < fixed, places, passed)]].set(jnp.asarray(sizes, jnp.int32))

    sizes = jnp.where(number % 4 == 0, named(crowded, number // 4), named(common, number - number // 4 - 1))
    mixed = jax.random.permutation(jax.random.fold_in(own, 3), number_of)
    giver, receiver = mixed[0:number_of // 2 * 2:2], mixed[1:number_of // 2 * 2:2]
    slack = jnp.minimum(sizes[giver] - 1, limit - sizes[receiver]) // 2
    slack = jnp.where((giver == order[0]) | (receiver == order[0]) | (sizes[receiver] == 0), 0, jnp.maximum(slack, 0))
    passed = jax.random.randint(jax.random.fold_in(own, 4), (number_of // 2,), 0, 1 << 20) % (slack + 1)
    sizes = sizes.at[giver].add(-passed).at[receiver].add(passed)
    items = jnp.searchsorted(jnp.cumsum(sizes), jnp.arange(rows * top), side="right").astype(jnp.int32)
    table = items.reshape(top, rows).T
    table = table[jax.random.permutation(jax.random.fold_in(own, 1), rows)]
    offset_by = jax.random.randint(jax.random.fold_in(own, 2), (rows, 1), 0, top)
    return jnp.take_along_axis(table, (jnp.arange(top)[None, :] + offset_by) % top, axis=1)


def portions_of(amount, total, most, lean, full):
    loads = [(1 << 20) // math.isqrt(standing ** lean) + 1 for standing in range(1, amount + 1)]
    largest = most if full else min(most, max(-(-total // amount), total * loads[0] // sum(loads)))
    least = 1 if total - largest >= amount - 1 else 0
    given, spare = [largest] + [least] * (amount - 1), total - largest - least * (amount - 1)
    while spare > 0:
        candidates = [i for i in range(1, amount) if given[i] < largest] or [i for i in range(1, amount) if given[i] < most]
        mass, left = sum([loads[i] for i in candidates]), spare
        for i in candidates:
            extra = min(most - given[i], max(1, left * loads[i] // mass), spare)
            given[i] = given[i] + extra
            spare = spare - extra
    return np.array(given)


def gaussian(stream_key, extent, deviation, limit, shards=(), kind=jnp.bfloat16):
    array = deviation * jax.random.normal(stream_key, extent, jnp.float32)
    if shards:
        array = array * levels(stream_key, extent, shards, -0.22, 0.18)
    return jnp.clip(array, -limit, limit).astype(kind)


def setup_inputs(seed: int = 0) -> dict:
    streams_of = jax.random.split(jax.random.key(seed), 19)
    queries = draw_queries(jax.random.fold_in(streams_of[18], 71), 0)
    key_heads = draw_key_heads(jax.random.fold_in(streams_of[18], 71), 0)
    value_heads = draw_value_heads(jax.random.fold_in(streams_of[18], 71), 0)
    documents = jnp.searchsorted(jnp.cumsum(uneven_parts(streams_of[3], DOCS, TOKENS, DOC_MOST, 1)), jnp.arange(TOKENS), side="right").astype(jnp.int32)
    query_gain = draw_query_gain(jax.random.fold_in(streams_of[18], 71), 0)
    key_gain = draw_key_gain(jax.random.fold_in(streams_of[18], 71), 0)
    out_gain = jnp.clip(1.0 + 0.18 * jax.random.normal(streams_of[6], (QH * HEAD,), jnp.float32), 0.1, 1.9)
    out_proj = gaussian(streams_of[7], (QH * HEAD, D), (QH * HEAD) ** -0.5, 0.1875)
    residual = gaussian(streams_of[8], (TOKENS, D), 1.0, 6.0, ((0, 32),))
    mid_gain = jnp.clip(1.0 + 0.18 * jax.random.normal(streams_of[9], (D,), jnp.float32), 0.1, 1.9)
    mid_bias = gaussian(streams_of[10], (D,), 0.3, 1.5, (), jnp.float32)
    routes_keys = jax.random.split(jax.random.fold_in(streams_of[11], 1), TOKENS // ROWS)
    routes_turns = jax.random.permutation(jax.random.fold_in(streams_of[11], 3), TOKENS // ROWS)
    routes = jax.vmap(lambda own, number: assign_block(jax.random.fold_in(streams_of[11], 2), own, number, ROWS, EXPERTS, TOP_K, CAP, 2))(routes_keys, routes_turns).reshape((TOKENS, TOP_K))
    route_weights = jnp.clip(jnp.exp(math.log(2.0) - 2.3025851 * jax.random.uniform(streams_of[12], (TOKENS, TOP_K), jnp.float32) ** levels(streams_of[12], (TOKENS, TOP_K), ((0, 32),), -0.2, 0.2)), 0.2, 2.0)
    expert_gate = gaussian(streams_of[13], (EXPERTS, D, DE), D ** -0.5, 0.125, ((0, 32),))
    expert_up = gaussian(streams_of[14], (EXPERTS, D, DE), D ** -0.5, 0.125, ((0, 32),))
    expert_down = gaussian(streams_of[15], (EXPERTS, DE, D), DE ** -0.5, 0.25, ((0, 32),))
    final_gain = jnp.clip(1.0 + 0.18 * jax.random.normal(streams_of[16], (D,), jnp.float32), 0.1, 1.9)
    final_bias = gaussian(streams_of[17], (D,), 0.3, 1.5, (), jnp.float32)
    return dict(queries=queries, key_heads=key_heads, value_heads=value_heads, documents=documents, query_gain=query_gain, key_gain=key_gain, out_gain=out_gain, out_proj=out_proj, residual=residual, mid_gain=mid_gain, mid_bias=mid_bias, routes=routes, route_weights=route_weights, expert_gate=expert_gate, expert_up=expert_up, expert_down=expert_down, final_gain=final_gain, final_bias=final_bias)


eps_norm = 1e-06
alpha_mix = 8.0 ** 0.25
theta_base = 10000.0

def rotary_tables(row_total, offset):
    positions = offset + jnp.arange(row_total, dtype=jnp.int32)
    grid_row = (positions // GRID).astype(jnp.float32)
    grid_col = (positions % GRID).astype(jnp.float32)
    pair_count = HEAD // 4
    inv_freq = theta_base ** (-jnp.arange(pair_count, dtype=jnp.float32) / pair_count)
    angles = jnp.concatenate([grid_row[:, None] * inv_freq[None, :], grid_col[:, None] * inv_freq[None, :]], axis=1)
    return (jnp.cos(angles), jnp.sin(angles))

def normed_rotated(heads_in, gain_vec, cosine_table, sine_table):
    values = heads_in.astype(jnp.float32)
    inv_rms = lax.rsqrt(lax.optimization_barrier(jnp.mean(values * values, axis=-1, keepdims=True)) + eps_norm)
    values = values * inv_rms * gain_vec
    half_dim = HEAD // 2
    first_half = values[..., :half_dim]
    second_half = values[..., half_dim:]
    cosine_part = cosine_table[:, None, :]
    sine_part = sine_table[:, None, :]
    turned = jnp.concatenate([first_half * cosine_part - second_half * sine_part, second_half * cosine_part + first_half * sine_part], axis=-1)
    return turned.astype(jnp.bfloat16)

def layer_norm(stream, gain_vec, bias_vec):
    center = lax.optimization_barrier(jnp.mean(stream, axis=-1, keepdims=True))
    spread = lax.optimization_barrier(jnp.mean(jnp.square(stream - center), axis=-1, keepdims=True))
    return (stream - center) * lax.rsqrt(spread + eps_norm) * gain_vec + bias_vec

def reference(queries, key_heads, value_heads, documents, query_gain, key_gain, out_gain, out_proj, residual, mid_gain, mid_bias, routes, route_weights, expert_gate, expert_up, expert_down, final_gain, final_bias):
    cosine_table, sine_table = rotary_tables(TOKENS, 0)
    grouped = QH // KVH
    query_rot = normed_rotated(queries.reshape(TOKENS, QH, HEAD), query_gain, cosine_table, sine_table).reshape(TOKENS, KVH, grouped, HEAD)
    key_rot = normed_rotated(key_heads.reshape(TOKENS, KVH, HEAD), key_gain, cosine_table, sine_table).astype(jnp.float32)
    value_all = value_heads.reshape(TOKENS, KVH, HEAD).astype(jnp.float32)
    block_rows = math.gcd(TOKENS, 512)

    def query_block(number):
        first_row = number * block_rows
        query_part = lax.dynamic_slice_in_dim(query_rot, first_row, block_rows, 0).astype(jnp.float32)
        doc_part = lax.dynamic_slice_in_dim(documents, first_row, block_rows, 0)
        scores = jnp.einsum('qkgd,tkd->kgqt', query_part, key_rot) * HEAD ** (-0.5)
        allowed = (doc_part[:, None] == documents[None, :])[None, None]
        scores = jnp.where(allowed, scores, -1e+30)
        row_max = lax.optimization_barrier(jnp.max(scores, axis=-1, keepdims=True))
        weights = jnp.where(allowed, jnp.exp(scores - row_max), 0.0)
        totals = lax.optimization_barrier(jnp.sum(weights, axis=-1))
        rounded = lax.optimization_barrier(weights.astype(jnp.bfloat16)).astype(jnp.float32)
        summed = jnp.einsum('kgqt,tkd->kgqd', rounded, value_all) / totals[..., None]
        return jnp.transpose(summed, (2, 0, 1, 3)).reshape(block_rows, QH * HEAD).astype(jnp.bfloat16)
    attention = lax.map(query_block, jnp.arange(TOKENS // block_rows, dtype=jnp.int32))
    attention = attention.reshape(TOKENS, QH * HEAD)
    attn_float = attention.astype(jnp.float32)
    mean_square = lax.optimization_barrier(jnp.mean(attn_float * attn_float, axis=1, keepdims=True))
    scaled = (attn_float * out_gain).astype(jnp.bfloat16)
    projected = jnp.dot(scaled, out_proj, preferred_element_type=jnp.float32) * lax.rsqrt(mean_square + eps_norm)
    middle = layer_norm(alpha_mix * residual.astype(jnp.float32) + projected, mid_gain, mid_bias).astype(jnp.bfloat16)
    flat_routes = routes.reshape(-1).astype(jnp.int32)
    pair_total = flat_routes.shape[0]
    receive = N_SP * N_TP * CAP
    sorted_order = jnp.argsort(flat_routes, stable=True).astype(jnp.int32)
    counts = lax.optimization_barrier(jnp.sum((flat_routes[:, None] == jnp.arange(EXPERTS, dtype=jnp.int32)[None, :]).astype(jnp.int32), axis=0))
    starts = jnp.cumsum(counts) - counts
    inverse = jnp.zeros((pair_total,), jnp.int32).at[sorted_order].set(jnp.arange(pair_total, dtype=jnp.int32))
    token_of = sorted_order // TOP_K

    def expert_pass(expert):
        slot_index = starts[expert] + jnp.arange(receive, dtype=jnp.int32)
        live_rows = slot_index < starts[expert] + counts[expert]
        source_rows = middle[token_of[jnp.minimum(slot_index, pair_total - 1)]]
        picked = jnp.where(live_rows[:, None], source_rows, jnp.zeros((), jnp.bfloat16))
        gate_part = jnp.dot(picked, expert_gate[expert], preferred_element_type=jnp.float32)
        up_part = jnp.dot(picked, expert_up[expert], preferred_element_type=jnp.float32)
        hidden = (jax.nn.silu(gate_part) * up_part).astype(jnp.bfloat16)
        return jnp.dot(hidden, expert_down[expert], preferred_element_type=jnp.float32).astype(jnp.bfloat16)
    served = lax.map(expert_pass, jnp.arange(EXPERTS, dtype=jnp.int32)).reshape(EXPERTS * receive, D)
    slot_rows = flat_routes * receive + (inverse - starts[flat_routes])
    gathered = served[slot_rows].astype(jnp.float32).reshape(TOKENS, TOP_K, D)
    routed = lax.optimization_barrier(jnp.sum(gathered * route_weights[:, :, None], axis=1))
    return layer_norm(alpha_mix * middle.astype(jnp.float32) + routed, final_gain, final_bias).astype(jnp.bfloat16)
```

```python
import functools

import jax
import jax.numpy as jnp
from jax import lax
from jax.experimental import pallas as pl
from jax.experimental.pallas import tpu as pltpu
from jax.sharding import PartitionSpec as P

HEAD = 128
GRID = 64


eps_norm = 1e-06
alpha_mix = 8.0**0.25
theta_base = 10000.0
score_factor = HEAD ** (-0.5) * 1.4426950408889634
VMEM = pl.BlockSpec(memory_space=pltpu.VMEM)
ANY = pl.BlockSpec(memory_space=pl.ANY)
SMEM = pl.BlockSpec(memory_space=pltpu.SMEM)


def layer_norm(stream, gain_vec, bias_vec):
    center = jnp.mean(stream, axis=-1, keepdims=True)
    spread = jnp.mean(jnp.square(stream - center), axis=-1, keepdims=True)
    return (stream - center) * lax.rsqrt(spread + eps_norm) * gain_vec + bias_vec


def flipped(number, pattern):
    bit = 1
    while bit <= pattern:
        if pattern & bit:
            number = number + bit - 2 * bit * lax.rem(number // bit, 2)
        bit *= 2
    return number


def turned(values, gain, cosine, sine):
    inv_rms = lax.rsqrt(jnp.mean(values * values, axis=1, keepdims=True) + eps_norm)
    values = values * inv_rms * gain
    return (values * cosine + pltpu.roll(values, HEAD // 2, 1) * sine).astype(jnp.bfloat16)


def front_kernel(
    size,
    pair,
    tp_size,
    capacity,
    q_ref,
    k_ref,
    v_ref,
    doc_ref,
    qdoc_ref,
    q_gain_ref,
    k_gain_ref,
    row_ref,
    col_ref,
    route_ref,
    gain_ref,
    proj_hbm,
    res_ref,
    mid_gain_ref,
    mid_bias_ref,
    mid_ref,
    out_ref,
    column_ref,
    kv,
    docs,
    q_rot,
    m_ref,
    l_ref,
    acc_ref,
    o_buf,
    whole,
    proj,
    line_send,
    line_recv,
    mate_send,
    mate_recv,
    tp_send,
    tp_recv,
    own_sem,
):
    me = lax.axis_index("sp")
    lane = lax.axis_index("tp")
    inner = lax.rem(me, pair)
    outer = me // pair
    steps = size // pair
    mate = outer * pair + lax.rem(inner + 1, pair)
    rows = k_ref.shape[0]
    pieces = doc_ref.shape[0]
    grouped = q_rot.shape[0]
    parts = 3

    load = pltpu.make_async_copy(proj_hbm, proj, own_sem.at[0])
    load.start()
    own = [
        pltpu.make_async_copy(v_ref, kv.at[me, 1], own_sem.at[1]),
        pltpu.make_async_copy(doc_ref, docs.at[me], own_sem.at[2]),
    ]
    for copy in own:
        copy.start()

    def on_line(place):
        return (place >= 0) & (place < steps)

    barrier = pltpu.get_barrier_semaphore()

    def greet(target):
        pl.semaphore_signal(
            barrier, inc=1, device_id=target, device_id_type=pl.DeviceIdType.MESH
        )

    peers = jnp.int32(tp_size - 1 + (pair - 1))
    for sign in (1, -1):
        there = on_line(outer + sign)
        pl.when(there)(lambda sign=sign: greet({"sp": (outer + sign) * pair + inner}))
        peers = peers + there.astype(jnp.int32)
    if pair == 2:
        greet({"sp": mate})
    tp_targets = [lax.rem(lane + step, tp_size) for step in range(1, tp_size)]
    for target in tp_targets:
        greet({"tp": target})
    pl.semaphore_wait(barrier, peers)

    def piece(place, part, first):
        if part == 2:
            return (doc_ref if first else docs.at[place]), docs.at[place]
        return (v_ref if first and part == 1 else kv.at[place, part]), kv.at[place, part]

    def line_copy(way, step, part, first=False):
        sign = 1 - 2 * way
        place = (outer - sign * (step - 1)) * pair + inner
        src, dst = piece(place, part, first)
        return pltpu.make_async_remote_copy(
            src_ref=src,
            dst_ref=dst,
            send_sem=line_send.at[way, step, part],
            recv_sem=line_recv.at[way, step, part],
            device_id={"sp": (outer + sign) * pair + inner},
            device_id_type=pl.DeviceIdType.MESH,
        )

    def mate_copy(way, step, part, first=False):
        sign = 1 - 2 * way
        place = (outer - sign * step) * pair + inner
        src, dst = piece(place, part, first)
        return pltpu.make_async_remote_copy(
            src_ref=src,
            dst_ref=dst,
            send_sem=mate_send.at[way, step, part],
            recv_sem=mate_recv.at[way, step, part],
            device_id={"sp": mate},
            device_id_type=pl.DeviceIdType.MESH,
        )

    def send_own(part):
        for way in range(2):
            pl.when(on_line(outer + 1 - 2 * way))(
                lambda way=way: line_copy(way, 1, part, True).start()
            )
        if pair == 2:
            mate_copy(0, 0, part, True).start()

    send_own(1)
    send_own(2)
    grid_rows = row_ref.shape[1]
    span = col_ref.shape[1]

    def tables(block):
        cosine = row_ref[0, pl.ds(block, 1)] + col_ref[0]
        sine = row_ref[1, pl.ds(block, 1)] + col_ref[1]
        return cosine, sine

    def turn_keys(block, unused):
        cosine, sine = tables(block)
        here = pl.ds(pl.multiple_of(block * span, span), span)
        kv[me, 0, here] = turned(k_ref[here].astype(jnp.float32), k_gain_ref[...], cosine, sine)
        return unused

    lax.fori_loop(0, grid_rows, turn_keys, 0)
    send_own(0)

    def turn_queries(block, unused):
        cosine, sine = tables(block)
        here = pl.ds(pl.multiple_of(block * span, span), span)
        for head in range(grouped):
            q_rot[head, here] = turned(
                q_ref[here, head * HEAD : (head + 1) * HEAD].astype(jnp.float32),
                q_gain_ref[...],
                cosine,
                sine,
            )
        return unused

    lax.fori_loop(0, grid_rows, turn_queries, 0)
    m_ref[...] = jnp.full(m_ref.shape, -1e30, jnp.float32)
    l_ref[...] = jnp.zeros(l_ref.shape, jnp.float32)
    acc_ref[...] = jnp.zeros(acc_ref.shape, jnp.float32)
    for copy in own:
        copy.wait()
    chunk = 256

    def advance(place):
        keys = kv[place, 0]
        values = kv[place, 1]
        doc_rows = docs[place]
        key_docs = jnp.concatenate([doc_rows[i : i + 1] for i in range(pieces)], axis=1)
        for head in range(grouped):
            for first in range(0, rows, chunk):
                part = pl.ds(first, chunk)
                scores = lax.dot_general(
                    q_rot[head, part],
                    keys,
                    (((1,), (1,)), ((), ())),
                    preferred_element_type=jnp.float32,
                )
                allowed = qdoc_ref[part, 0:1] == key_docs
                scores = jnp.where(allowed, scores * score_factor, -1e30)
                old_max = m_ref[head, part]
                new_max = jnp.maximum(old_max, jnp.max(scores, axis=1, keepdims=True))
                base = jnp.maximum(new_max[:, 0:1], -1e29)
                weights = jnp.exp2(scores - base)
                rescale = jnp.exp2(old_max - new_max)
                l_ref[head, part] = l_ref[head, part] * rescale + jnp.sum(
                    weights, axis=1, keepdims=True
                )
                acc_ref[head, part] = acc_ref[head, part] * rescale + jnp.dot(
                    weights.astype(jnp.bfloat16), values, preferred_element_type=jnp.float32
                )
                m_ref[head, part] = new_max

    def stage(step, unused):
        for group in ((1, 2), (0,)):
            for way in range(2):
                sign = 1 - 2 * way

                def take(way=way, sign=sign, group=group):
                    for part in group:
                        line_copy(way, step, part).wait_recv()

                    def pass_on():
                        for part in group:
                            line_copy(way, step + 1, part).start()

                    pl.when(on_line(outer + sign))(pass_on)
                    if pair == 2:
                        for part in group:
                            mate_copy(way, step, part).start()

                pl.when((step > 0) & on_line(outer - sign * step))(take)

        def visit(number, unused):
            way = lax.rem(number, 2)
            across = number // 2
            there = outer - (1 - 2 * way) * step

            def work():
                if pair == 2:

                    def arrive():
                        for part in range(parts):
                            mate_copy(way, step, part).wait_recv()

                    pl.when(across == 1)(arrive)
                advance(there * pair + lax.rem(inner + across, pair))

            pl.when(on_line(there) & ((step > 0) | (way == 0)))(work)
            return unused

        lax.fori_loop(0, 2 * pair, visit, 0)
        return unused

    lax.fori_loop(0, steps, stage, 0)
    for head in range(grouped):
        o_buf[:, head * HEAD : (head + 1) * HEAD] = (acc_ref[head] / l_ref[head]).astype(
            o_buf.dtype
        )

    out_rows, width = whole.shape[0], o_buf.shape[1]

    def rows_of(number):
        return pl.ds(pl.multiple_of(number * out_rows, out_rows), out_rows)

    mine = whole.at[:, pl.ds(pl.multiple_of(lane * width, width), width)]
    swaps = []
    for step, target in enumerate(tp_targets):
        copy = pltpu.make_async_remote_copy(
            src_ref=o_buf.at[rows_of(target)],
            dst_ref=mine,
            send_sem=tp_send.at[step],
            recv_sem=tp_recv.at[step],
            device_id={"tp": target},
            device_id_type=pl.DeviceIdType.MESH,
        )
        copy.start()
        swaps.append(copy)
    keep = pltpu.make_async_copy(o_buf.at[rows_of(lane)], mine, own_sem.at[3])
    keep.start()

    top, tokens = route_ref.shape
    experts = 2 * tokens * top // capacity
    down = lax.broadcasted_iota(jnp.int32, (tokens, tokens), 0)
    over = lax.broadcasted_iota(jnp.int32, (tokens, tokens), 1)
    earlier = jnp.where(down < over, 1.0, 0.0).astype(jnp.bfloat16)
    names = lax.broadcasted_iota(jnp.int32, (experts, tokens), 0)
    passed = jnp.zeros((experts, 1), jnp.float32)
    slots = out_ref.shape[0]
    slot = lax.broadcasted_iota(jnp.int32, (slots, tokens), 0)
    chosen = None
    for route in range(top):
        named = route_ref[route : route + 1, :]
        one_hot = jnp.where(names == named, 1.0, 0.0)
        before = passed + jnp.dot(
            one_hot.astype(jnp.bfloat16), earlier, preferred_element_type=jnp.float32
        )
        rank = jnp.sum(before * one_hot, axis=0, keepdims=True)
        target = named.astype(jnp.float32) * capacity + rank
        column_ref[:, route : route + 1] = jnp.sum(
            jnp.where(down == over, target, 0.0), axis=1, keepdims=True
        ).astype(jnp.int32)
        passed = passed + jnp.sum(one_hot, axis=1, keepdims=True)
        match = slot == target.astype(jnp.int32)
        chosen = match if chosen is None else chosen | match
    select = jnp.where(chosen, 1.0, 0.0).astype(jnp.bfloat16)

    load.wait()
    for copy in swaps:
        copy.wait_recv()
    keep.wait()
    taken = whole[...].astype(jnp.float32)
    mean_square = jnp.mean(taken * taken, axis=1, keepdims=True)
    scaled = (taken * gain_ref[...]).astype(jnp.bfloat16)
    projected = jnp.dot(scaled, proj[...], preferred_element_type=jnp.float32)
    projected = projected * lax.rsqrt(mean_square + eps_norm)
    stream = alpha_mix * res_ref[...].astype(jnp.float32) + projected
    middle = layer_norm(stream, mid_gain_ref[...], mid_bias_ref[...]).astype(jnp.bfloat16)
    mid_ref[...] = middle
    out_ref[...] = jnp.dot(select, middle, preferred_element_type=jnp.float32).astype(
        jnp.bfloat16
    )

    for copy in swaps:
        copy.wait_send()

    def settle(step, unused):
        for way in range(2):
            sign = 1 - 2 * way

            def sent(way=way):
                for part in range(parts):
                    line_copy(way, step + 1, part).wait_send()

            pl.when(on_line(outer - sign * step) & on_line(outer + sign))(sent)
            if pair == 2:

                def gave(way=way):
                    for part in range(parts):
                        mate_copy(way, step, part).wait_send()

                first = (step > 0) | (way == 0)
                pl.when(on_line(outer - sign * step) & first)(gave)
        return unused

    lax.fori_loop(0, steps, settle, 0)


def trig_tables(tok_rows, offset):
    pair_count = HEAD // 4
    inv_freq = theta_base ** (-jnp.arange(pair_count, dtype=jnp.float32) / pair_count)
    grid_rows = (offset // GRID + jnp.arange(tok_rows // GRID, dtype=jnp.int32)).astype(jnp.float32)
    grid_cols = jnp.arange(GRID, dtype=jnp.int32).astype(jnp.float32)
    tables = []
    for at, place in enumerate((grid_rows, grid_cols)):
        angles = place[:, None] * inv_freq[None, :]
        blank = jnp.zeros_like(angles)
        cosine, sine = jnp.cos(angles), jnp.sin(angles)
        order = (lambda a, b: [a, blank, b, blank]) if at == 0 else (lambda a, b: [blank, a, blank, b])
        tables.append(
            jnp.stack(
                [
                    jnp.concatenate(order(cosine, cosine), axis=1),
                    jnp.concatenate(order(-sine, sine), axis=1),
                ]
            )
        )
    return tables


def run_front(
    queries,
    keys,
    values,
    documents,
    query_gain,
    key_gain,
    routes,
    out_gain,
    out_proj,
    residual,
    mid_gain,
    mid_bias,
    size,
    tp_size,
    capacity,
):
    pair = 2 if size % 2 == 0 else 1
    rows, width = queries.shape
    grouped = width // HEAD
    out_rows, model_width = residual.shape
    steps = size // pair
    row_table, col_table = trig_tables(rows, lax.axis_index("sp") * rows)
    query_docs = jnp.broadcast_to(documents[:, None], (rows, HEAD))
    slots = 2 * out_rows * routes.shape[1]
    dma = pltpu.SemaphoreType.DMA
    return pl.pallas_call(
        functools.partial(front_kernel, size, pair, tp_size, capacity),
        out_shape=(
            jax.ShapeDtypeStruct((out_rows, model_width), jnp.bfloat16),
            jax.ShapeDtypeStruct((slots, model_width), jnp.bfloat16),
            jax.ShapeDtypeStruct(routes.shape, jnp.int32),
        ),
        in_specs=[VMEM] * 11 + [ANY] + [VMEM] * 3,
        out_specs=(VMEM, VMEM, VMEM),
        scratch_shapes=[
            pltpu.VMEM((size, 2, rows, HEAD), jnp.bfloat16),
            pltpu.VMEM((size, rows // HEAD, HEAD), jnp.int32),
            pltpu.VMEM((grouped, rows, HEAD), jnp.bfloat16),
            pltpu.VMEM((grouped, rows, HEAD), jnp.float32),
            pltpu.VMEM((grouped, rows, HEAD), jnp.float32),
            pltpu.VMEM((grouped, rows, HEAD), jnp.float32),
            pltpu.VMEM((rows, width), jnp.bfloat16),
            pltpu.VMEM((out_rows, width * tp_size), jnp.bfloat16),
            pltpu.VMEM(out_proj.shape, out_proj.dtype),
            dma((2, steps + 1, 3)),
            dma((2, steps + 1, 3)),
            dma((2, steps, 3)),
            dma((2, steps, 3)),
            dma((tp_size,)),
            dma((tp_size,)),
            dma((4,)),
        ],
        compiler_params=pltpu.CompilerParams(
            collective_id=0, has_side_effects=True, vmem_limit_bytes=56 * 1024 * 1024
        ),
    )(
        queries,
        keys,
        values,
        documents.reshape(rows // HEAD, HEAD),
        query_docs,
        query_gain[None, :],
        key_gain[None, :],
        row_table,
        col_table,
        routes.T,
        out_gain[None, :],
        out_proj,
        residual,
        mid_gain[None, :],
        mid_bias[None, :],
    )


def expert_kernel(
    outer_size,
    inner_size,
    tp_size,
    x_ref,
    gate_ref,
    up_ref,
    down_ref,
    o_ref,
    held,
    served,
    out_send,
    out_recv,
    back_send,
    back_recv,
    own_sem,
):
    me = lax.axis_index("sp") * tp_size + lax.axis_index("tp")
    outer = me // inner_size
    inner = lax.rem(me, inner_size)
    size = outer_size * inner_size
    paired = outer_size & (outer_size - 1) == 0
    half = outer_size // 2
    upper, lower = list(range(half, outer_size)), list(range(1, half))
    if outer_size == 1:
        send_order, work_order = [0], [0]
    else:
        send_order = [group for group in upper + lower if group] + [0]
        work_order = [0] + [group for group in upper[:1] + lower + upper[1:] if group]

    def mesh_place(index):
        return {"sp": index // tp_size, "tp": lax.rem(index, tp_size)}

    def plane_to(group):
        if paired:
            return flipped(outer, group)
        return lax.rem(outer + group, outer_size)

    def plane_from(group):
        if paired:
            return flipped(outer, group)
        return lax.rem(outer - group + outer_size, outer_size)

    def target_of(group, step):
        return plane_to(group) * inner_size + lax.rem(inner + step, inner_size)

    def source_of(group, step):
        return plane_from(group) * inner_size + lax.rem(inner - step + inner_size, inner_size)

    def out_copy(group, step):
        target = target_of(group, step)
        return pltpu.make_async_remote_copy(
            src_ref=x_ref.at[target],
            dst_ref=held.at[me],
            send_sem=out_send.at[group * inner_size + step],
            recv_sem=out_recv.at[group * inner_size + step],
            device_id=mesh_place(target),
            device_id_type=pl.DeviceIdType.MESH,
        )

    def back_copy(group, step):
        source = source_of(group, step)
        return pltpu.make_async_remote_copy(
            src_ref=served.at[source],
            dst_ref=o_ref.at[me],
            send_sem=back_send.at[group * inner_size + step],
            recv_sem=back_recv.at[group * inner_size + step],
            device_id=mesh_place(source),
            device_id_type=pl.DeviceIdType.MESH,
        )

    def each(group, act):
        def once(step, unused):
            act(group, step)
            return unused

        lax.fori_loop(1 if group == 0 else 0, inner_size, once, 0)

    own_out = pltpu.make_async_copy(x_ref.at[me], held.at[me], own_sem.at[0])
    own_out.start()
    barrier = pltpu.get_barrier_semaphore()

    def greet(group, step):
        pl.semaphore_signal(
            barrier,
            inc=1,
            device_id=mesh_place(target_of(group, step)),
            device_id_type=pl.DeviceIdType.MESH,
        )

    for group in send_order:
        each(group, greet)
    pl.semaphore_wait(barrier, size - 1)
    for group in send_order:
        each(group, lambda g, step: out_copy(g, step).start())
    own_out.wait()
    local_experts = gate_ref.shape[0]
    block = held.shape[1]
    capacity = block // local_experts
    width = held.shape[2]
    for group in work_order:
        each(group, lambda g, step: out_copy(g, step).wait_recv())
        span = pl.ds(plane_from(group) * inner_size, inner_size)
        arrived = held[span]
        for expert in range(local_experts):
            part = slice(expert * capacity, (expert + 1) * capacity)
            rows = arrived[:, part].reshape(inner_size * capacity, width)
            gate = jnp.dot(rows, gate_ref[expert], preferred_element_type=jnp.float32)
            up = jnp.dot(rows, up_ref[expert], preferred_element_type=jnp.float32)
            hidden = (gate / (1.0 + jnp.exp(-gate)) * up).astype(jnp.bfloat16)
            result = jnp.dot(hidden, down_ref[expert], preferred_element_type=jnp.float32)
            served[span, part] = result.astype(jnp.bfloat16).reshape(inner_size, capacity, width)
        each(group, lambda g, step: back_copy(g, step).start())
    own_back = pltpu.make_async_copy(served.at[me], o_ref.at[me], own_sem.at[1])
    own_back.start()
    for group in work_order:
        each(group, lambda g, step: back_copy(g, step).wait_recv())
    for group in work_order:
        each(group, lambda g, step: out_copy(g, step).wait_send())
        each(group, lambda g, step: back_copy(g, step).wait_send())
    own_back.wait()


def run_experts(blocks, gate, up, down, sp_size, tp_size):
    size = blocks.shape[0]
    pair = 2 if sp_size % 2 == 0 else 1
    return pl.pallas_call(
        functools.partial(expert_kernel, sp_size // pair, pair * tp_size, tp_size),
        out_shape=jax.ShapeDtypeStruct(blocks.shape, blocks.dtype),
        in_specs=[VMEM] * 4,
        out_specs=VMEM,
        scratch_shapes=[pltpu.VMEM(blocks.shape, blocks.dtype) for unused in range(2)]
        + [pltpu.SemaphoreType.DMA((size,)) for unused in range(4)]
        + [pltpu.SemaphoreType.DMA((2,))],
        compiler_params=pltpu.CompilerParams(
            collective_id=2, has_side_effects=True, vmem_limit_bytes=48 * 1024 * 1024
        ),
    )(blocks, gate, up, down)


def final_kernel(back_ref, target_ref, weight_ref, mid_ref, gain_ref, bias_ref, o_ref):
    rows, slots = mid_ref.shape[0], back_ref.shape[0]
    slot = lax.broadcasted_iota(jnp.int32, (rows, slots), 1)
    routed = None
    for route in range(target_ref.shape[1]):
        select = jnp.where(slot == target_ref[:, route : route + 1], 1.0, 0.0)
        picked = jnp.dot(
            select.astype(jnp.bfloat16), back_ref[...], preferred_element_type=jnp.float32
        )
        term = picked * weight_ref[:, route : route + 1]
        routed = term if routed is None else routed + term
    stream = alpha_mix * mid_ref[...].astype(jnp.float32) + routed
    o_ref[...] = layer_norm(stream, gain_ref[...], bias_ref[...]).astype(o_ref.dtype)


def per_device(
    queries,
    key_heads,
    value_heads,
    documents,
    query_gain,
    key_gain,
    out_gain,
    out_proj,
    residual,
    mid_gain,
    mid_bias,
    routes,
    route_weights,
    expert_gate,
    expert_up,
    expert_down,
    final_gain,
    final_bias,
):
    sp_size = lax.axis_size("sp")
    tp_size = lax.axis_size("tp")
    if key_heads.shape[1] != HEAD or expert_gate.shape[0] != 1:
        raise ValueError("unsupported placement")
    out_rows, model_width = residual.shape
    local_experts = expert_gate.shape[0]
    device_total = sp_size * tp_size
    expert_total = local_experts * device_total
    capacity = 2 * out_rows * routes.shape[1] // expert_total
    slots = expert_total * capacity
    middle, outbound, target_columns = run_front(
        queries,
        key_heads,
        value_heads,
        documents,
        query_gain,
        key_gain,
        routes,
        out_gain,
        out_proj,
        residual,
        mid_gain,
        mid_bias,
        sp_size,
        tp_size,
        capacity,
    )
    returned = run_experts(
        outbound.reshape(device_total, local_experts * capacity, model_width),
        expert_gate,
        expert_up,
        expert_down,
        sp_size,
        tp_size,
    )
    return pl.pallas_call(
        final_kernel,
        out_shape=jax.ShapeDtypeStruct((out_rows, model_width), jnp.bfloat16),
        in_specs=[VMEM] * 6,
        out_specs=VMEM,
        compiler_params=pltpu.CompilerParams(vmem_limit_bytes=48 * 1024 * 1024),
    )(
        returned.reshape(slots, model_width),
        target_columns,
        route_weights,
        middle,
        final_gain[None, :],
        final_bias[None, :],
    )


def solution(mesh):
    return jax.shard_map(
        per_device,
        mesh=mesh,
        in_specs=(
            P("sp", "tp"),
            P("sp", "tp"),
            P("sp", "tp"),
            P("sp"),
            P(),
            P(),
            P(),
            P(),
            P(("sp", "tp"), None),
            P(),
            P(),
            P(("sp", "tp"), None),
            P(("sp", "tp"), None),
            P(("sp", "tp"), None, None),
            P(("sp", "tp"), None, None),
            P(("sp", "tp"), None, None),
            P(),
            P(),
        ),
        out_specs=P(("sp", "tp"), None),
        check_vma=False,
    )
```

```python
import functools

import jax
import jax.numpy as jnp
from jax import lax
from jax.experimental import pallas as pl
from jax.experimental.pallas import tpu as pltpu
from jax.sharding import PartitionSpec as P

HEAD = 128
GRID = 64
CHUNKS = 4


eps_norm = 1e-06
alpha_mix = 8.0**0.25
theta_base = 10000.0
score_factor = HEAD ** (-0.5) * 1.4426950408889634
VMEM = pl.BlockSpec(memory_space=pltpu.VMEM)
ANY = pl.BlockSpec(memory_space=pl.ANY)
SMEM = pl.BlockSpec(memory_space=pltpu.SMEM)


def layer_norm(stream, gain_vec, bias_vec):
    center = jnp.mean(stream, axis=-1, keepdims=True)
    spread = jnp.mean(jnp.square(stream - center), axis=-1, keepdims=True)
    return (stream - center) * lax.rsqrt(spread + eps_norm) * gain_vec + bias_vec


def turned(values, gain, cosine, sine):
    inv_rms = lax.rsqrt(jnp.mean(values * values, axis=1, keepdims=True) + eps_norm)
    values = values * inv_rms * gain
    return (values * cosine + pltpu.roll(values, HEAD // 2, 1) * sine).astype(jnp.bfloat16)


def front_kernel(
    size,
    pair,
    tp_size,
    q_ref,
    k_ref,
    v_ref,
    doc_ref,
    qdoc_ref,
    q_gain_ref,
    k_gain_ref,
    row_ref,
    col_ref,
    gain_ref,
    proj_hbm,
    res_ref,
    mid_gain_ref,
    mid_bias_ref,
    mid_ref,
    kv,
    docs,
    q_rot,
    m_ref,
    l_ref,
    acc_ref,
    o_buf,
    whole,
    proj,
    line_send,
    line_recv,
    mate_send,
    mate_recv,
    tp_send,
    tp_recv,
    own_sem,
):
    me = lax.axis_index("sp")
    lane = lax.axis_index("tp")
    inner = lax.rem(me, pair)
    outer = me // pair
    steps = size // pair
    mate = outer * pair + lax.rem(inner + 1, pair)
    rows = k_ref.shape[0]
    pieces = doc_ref.shape[0]
    grouped = q_rot.shape[0]
    parts = 3

    load = pltpu.make_async_copy(proj_hbm, proj, own_sem.at[0])
    load.start()
    own = [
        pltpu.make_async_copy(v_ref, kv.at[me, 1], own_sem.at[1]),
        pltpu.make_async_copy(doc_ref, docs.at[me], own_sem.at[2]),
    ]
    for copy in own:
        copy.start()

    def on_line(place):
        return (place >= 0) & (place < steps)

    barrier = pltpu.get_barrier_semaphore()

    def greet(target):
        pl.semaphore_signal(
            barrier, inc=1, device_id=target, device_id_type=pl.DeviceIdType.MESH
        )

    peers = jnp.int32(tp_size - 1 + (pair - 1))
    for sign in (1, -1):
        there = on_line(outer + sign)
        pl.when(there)(lambda sign=sign: greet({"sp": (outer + sign) * pair + inner}))
        peers = peers + there.astype(jnp.int32)
    if pair == 2:
        greet({"sp": mate})
    tp_targets = [lax.rem(lane + step, tp_size) for step in range(1, tp_size)]
    for target in tp_targets:
        greet({"tp": target})
    pl.semaphore_wait(barrier, peers)

    def piece(place, part, first):
        if part == 2:
            return (doc_ref if first else docs.at[place]), docs.at[place]
        return (v_ref if first and part == 1 else kv.at[place, part]), kv.at[place, part]

    def line_copy(way, step, part, first=False):
        sign = 1 - 2 * way
        place = (outer - sign * (step - 1)) * pair + inner
        src, dst = piece(place, part, first)
        return pltpu.make_async_remote_copy(
            src_ref=src,
            dst_ref=dst,
            send_sem=line_send.at[way, step, part],
            recv_sem=line_recv.at[way, step, part],
            device_id={"sp": (outer + sign) * pair + inner},
            device_id_type=pl.DeviceIdType.MESH,
        )

    def mate_copy(way, step, part, first=False):
        sign = 1 - 2 * way
        place = (outer - sign * step) * pair + inner
        src, dst = piece(place, part, first)
        return pltpu.make_async_remote_copy(
            src_ref=src,
            dst_ref=dst,
            send_sem=mate_send.at[way, step, part],
            recv_sem=mate_recv.at[way, step, part],
            device_id={"sp": mate},
            device_id_type=pl.DeviceIdType.MESH,
        )

    def send_own(part):
        for way in range(2):
            pl.when(on_line(outer + 1 - 2 * way))(
                lambda way=way: line_copy(way, 1, part, True).start()
            )
        if pair == 2:
            mate_copy(0, 0, part, True).start()

    send_own(1)
    send_own(2)
    grid_rows = row_ref.shape[1]
    span = col_ref.shape[1]

    def tables(block):
        cosine = row_ref[0, pl.ds(block, 1)] + col_ref[0]
        sine = row_ref[1, pl.ds(block, 1)] + col_ref[1]
        return cosine, sine

    def turn_keys(block, unused):
        cosine, sine = tables(block)
        here = pl.ds(pl.multiple_of(block * span, span), span)
        kv[me, 0, here] = turned(k_ref[here].astype(jnp.float32), k_gain_ref[...], cosine, sine)
        return unused

    lax.fori_loop(0, grid_rows, turn_keys, 0)
    send_own(0)

    def turn_queries(block, unused):
        cosine, sine = tables(block)
        here = pl.ds(pl.multiple_of(block * span, span), span)
        for head in range(grouped):
            q_rot[head, here] = turned(
                q_ref[here, head * HEAD : (head + 1) * HEAD].astype(jnp.float32),
                q_gain_ref[...],
                cosine,
                sine,
            )
        return unused

    lax.fori_loop(0, grid_rows, turn_queries, 0)
    m_ref[...] = jnp.full(m_ref.shape, -1e30, jnp.float32)
    l_ref[...] = jnp.zeros(l_ref.shape, jnp.float32)
    acc_ref[...] = jnp.zeros(acc_ref.shape, jnp.float32)
    for copy in own:
        copy.wait()
    chunk = 256

    def advance(place):
        keys = kv[place, 0]
        values = kv[place, 1]
        doc_rows = docs[place]
        key_docs = jnp.concatenate([doc_rows[i : i + 1] for i in range(pieces)], axis=1)
        for head in range(grouped):
            for first in range(0, rows, chunk):
                part = pl.ds(first, chunk)
                scores = lax.dot_general(
                    q_rot[head, part],
                    keys,
                    (((1,), (1,)), ((), ())),
                    preferred_element_type=jnp.float32,
                )
                allowed = qdoc_ref[part, 0:1] == key_docs
                scores = jnp.where(allowed, scores * score_factor, -1e30)
                old_max = m_ref[head, part]
                new_max = jnp.maximum(old_max, jnp.max(scores, axis=1, keepdims=True))
                base = jnp.maximum(new_max[:, 0:1], -1e29)
                weights = jnp.exp2(scores - base)
                rescale = jnp.exp2(old_max - new_max)
                l_ref[head, part] = l_ref[head, part] * rescale + jnp.sum(
                    weights, axis=1, keepdims=True
                )
                acc_ref[head, part] = acc_ref[head, part] * rescale + jnp.dot(
                    weights.astype(jnp.bfloat16), values, preferred_element_type=jnp.float32
                )
                m_ref[head, part] = new_max

    def stage(step, unused):
        for group in ((1, 2), (0,)):
            for way in range(2):
                sign = 1 - 2 * way

                def take(way=way, sign=sign, group=group):
                    for part in group:
                        line_copy(way, step, part).wait_recv()

                    def pass_on():
                        for part in group:
                            line_copy(way, step + 1, part).start()

                    pl.when(on_line(outer + sign))(pass_on)
                    if pair == 2:
                        for part in group:
                            mate_copy(way, step, part).start()

                pl.when((step > 0) & on_line(outer - sign * step))(take)

        def visit(number, unused):
            way = lax.rem(number, 2)
            across = number // 2
            there = outer - (1 - 2 * way) * step

            def work():
                if pair == 2:

                    def arrive():
                        for part in range(parts):
                            mate_copy(way, step, part).wait_recv()

                    pl.when(across == 1)(arrive)
                advance(there * pair + lax.rem(inner + across, pair))

            pl.when(on_line(there) & ((step > 0) | (way == 0)))(work)
            return unused

        lax.fori_loop(0, 2 * pair, visit, 0)
        return unused

    lax.fori_loop(0, steps, stage, 0)
    for head in range(grouped):
        o_buf[:, head * HEAD : (head + 1) * HEAD] = (acc_ref[head] / l_ref[head]).astype(
            o_buf.dtype
        )

    out_rows, width = whole.shape[0], o_buf.shape[1]

    def rows_of(number):
        return pl.ds(pl.multiple_of(number * out_rows, out_rows), out_rows)

    mine = whole.at[:, pl.ds(pl.multiple_of(lane * width, width), width)]
    swaps = []
    for step, target in enumerate(tp_targets):
        copy = pltpu.make_async_remote_copy(
            src_ref=o_buf.at[rows_of(target)],
            dst_ref=mine,
            send_sem=tp_send.at[step],
            recv_sem=tp_recv.at[step],
            device_id={"tp": target},
            device_id_type=pl.DeviceIdType.MESH,
        )
        copy.start()
        swaps.append(copy)
    keep = pltpu.make_async_copy(o_buf.at[rows_of(lane)], mine, own_sem.at[3])
    keep.start()

    load.wait()
    for copy in swaps:
        copy.wait_recv()
    keep.wait()
    taken = whole[...].astype(jnp.float32)
    mean_square = jnp.mean(taken * taken, axis=1, keepdims=True)
    scaled = (taken * gain_ref[...]).astype(jnp.bfloat16)
    projected = jnp.dot(scaled, proj[...], preferred_element_type=jnp.float32)
    projected = projected * lax.rsqrt(mean_square + eps_norm)
    stream = alpha_mix * res_ref[...].astype(jnp.float32) + projected
    middle = layer_norm(stream, mid_gain_ref[...], mid_bias_ref[...]).astype(jnp.bfloat16)
    block = mid_ref.shape[2]
    for chunk in range(mid_ref.shape[0]):
        mid_ref[chunk] = middle[:, chunk * block : (chunk + 1) * block]

    for copy in swaps:
        copy.wait_send()

    def settle(step, unused):
        for way in range(2):
            sign = 1 - 2 * way

            def sent(way=way):
                for part in range(parts):
                    line_copy(way, step + 1, part).wait_send()

            pl.when(on_line(outer - sign * step) & on_line(outer + sign))(sent)
            if pair == 2:

                def gave(way=way):
                    for part in range(parts):
                        mate_copy(way, step, part).wait_send()

                first = (step > 0) | (way == 0)
                pl.when(on_line(outer - sign * step) & first)(gave)
        return unused

    lax.fori_loop(0, steps, settle, 0)


def trig_tables(tok_rows, offset):
    pair_count = HEAD // 4
    inv_freq = theta_base ** (-jnp.arange(pair_count, dtype=jnp.float32) / pair_count)
    grid_rows = (offset // GRID + jnp.arange(tok_rows // GRID, dtype=jnp.int32)).astype(jnp.float32)
    grid_cols = jnp.arange(GRID, dtype=jnp.int32).astype(jnp.float32)
    tables = []
    for at, place in enumerate((grid_rows, grid_cols)):
        angles = place[:, None] * inv_freq[None, :]
        blank = jnp.zeros_like(angles)
        cosine, sine = jnp.cos(angles), jnp.sin(angles)
        order = (lambda a, b: [a, blank, b, blank]) if at == 0 else (lambda a, b: [blank, a, blank, b])
        tables.append(
            jnp.stack(
                [
                    jnp.concatenate(order(cosine, cosine), axis=1),
                    jnp.concatenate(order(-sine, sine), axis=1),
                ]
            )
        )
    return tables


def run_front(
    queries,
    keys,
    values,
    documents,
    query_gain,
    key_gain,
    out_gain,
    out_proj,
    residual,
    mid_gain,
    mid_bias,
    size,
    tp_size,
    chunks,
):
    pair = 2 if size % 2 == 0 else 1
    rows, width = queries.shape
    grouped = width // HEAD
    out_rows, model_width = residual.shape
    steps = size // pair
    row_table, col_table = trig_tables(rows, lax.axis_index("sp") * rows)
    query_docs = jnp.broadcast_to(documents[:, None], (rows, HEAD))
    dma = pltpu.SemaphoreType.DMA
    return pl.pallas_call(
        functools.partial(front_kernel, size, pair, tp_size),
        out_shape=jax.ShapeDtypeStruct((chunks, out_rows, model_width // chunks), jnp.bfloat16),
        in_specs=[VMEM] * 10 + [ANY] + [VMEM] * 3,
        out_specs=VMEM,
        scratch_shapes=[
            pltpu.VMEM((size, 2, rows, HEAD), jnp.bfloat16),
            pltpu.VMEM((size, rows // HEAD, HEAD), jnp.int32),
            pltpu.VMEM((grouped, rows, HEAD), jnp.bfloat16),
            pltpu.VMEM((grouped, rows, HEAD), jnp.float32),
            pltpu.VMEM((grouped, rows, HEAD), jnp.float32),
            pltpu.VMEM((grouped, rows, HEAD), jnp.float32),
            pltpu.VMEM((rows, width), jnp.bfloat16),
            pltpu.VMEM((out_rows, width * tp_size), jnp.bfloat16),
            pltpu.VMEM(out_proj.shape, out_proj.dtype),
            dma((2, steps + 1, 3)),
            dma((2, steps + 1, 3)),
            dma((2, steps, 3)),
            dma((2, steps, 3)),
            dma((tp_size,)),
            dma((tp_size,)),
            dma((4,)),
        ],
        compiler_params=pltpu.CompilerParams(
            collective_id=0, has_side_effects=True, vmem_limit_bytes=56 * 1024 * 1024
        ),
    )(
        queries,
        keys,
        values,
        documents.reshape(rows // HEAD, HEAD),
        query_docs,
        query_gain[None, :],
        key_gain[None, :],
        row_table,
        col_table,
        out_gain[None, :],
        out_proj,
        residual,
        mid_gain[None, :],
        mid_bias[None, :],
    )


def expert_kernel(
    steps,
    plane,
    tp_size,
    x_ref,
    route_ref,
    weight_ref,
    gate_hbm,
    up_hbm,
    down_hbm,
    gain_ref,
    bias_ref,
    o_ref,
    xs,
    routes,
    weights,
    slots,
    outb,
    held,
    served,
    back,
    given,
    brought,
    own_sum,
    gate_acc,
    up_acc,
    gate_w,
    up_w,
    down_w,
    line_send,
    line_recv,
    out_send,
    out_recv,
    back_send,
    back_recv,
    sum_send,
    sum_recv,
    own_sem,
):
    me = lax.axis_index("sp") * tp_size + lax.axis_index("tp")
    outer = me // plane
    inner = lax.rem(me, plane)
    chunks, rows, width = x_ref.shape
    block = outb.shape[3]
    spots = plane * block
    top = route_ref.shape[0]
    parts = chunks + 2
    order = [chunks, chunks + 1] + list(range(chunks))

    loads = [
        pltpu.make_async_copy(x_ref, xs.at[outer], own_sem.at[0]),
        pltpu.make_async_copy(route_ref, routes.at[outer], own_sem.at[1]),
        pltpu.make_async_copy(weight_ref, weights.at[outer], own_sem.at[2]),
        pltpu.make_async_copy(gate_hbm, gate_w, own_sem.at[3]),
        pltpu.make_async_copy(up_hbm, up_w, own_sem.at[4]),
        pltpu.make_async_copy(down_hbm, down_w, own_sem.at[5]),
    ]
    for copy in loads:
        copy.start()

    def device(place, number):
        index = place * plane + number
        return {"sp": index // tp_size, "tp": lax.rem(index, tp_size)}

    def on_line(place):
        return (place >= 0) & (place < steps)

    barrier = pltpu.get_barrier_semaphore()

    def greet(place, number):
        pl.semaphore_signal(
            barrier,
            inc=1,
            device_id=device(place, number),
            device_id_type=pl.DeviceIdType.MESH,
        )

    peers = jnp.int32(plane - 1)
    for sign in (1, -1):
        there = on_line(outer + sign)
        pl.when(there)(lambda sign=sign: greet(outer + sign, inner))
        peers = peers + there.astype(jnp.int32)

    def greet_plane(step, unused):
        greet(outer, lax.rem(inner + step, plane))
        return unused

    lax.fori_loop(1, plane, greet_plane, 0)
    pl.semaphore_wait(barrier, peers)

    def piece(place, part, first):
        if part == chunks:
            return (route_ref if first else routes.at[place]), routes.at[place]
        if part == chunks + 1:
            return (weight_ref if first else weights.at[place]), weights.at[place]
        return (x_ref.at[part] if first else xs.at[place, part]), xs.at[place, part]

    def line_copy(way, step, part, first=False):
        sign = 1 - 2 * way
        place = outer - sign * (step - 1)
        src, dst = piece(place, part, first)
        return pltpu.make_async_remote_copy(
            src_ref=src,
            dst_ref=dst,
            send_sem=line_send.at[way, step, part],
            recv_sem=line_recv.at[way, step, part],
            device_id=device(outer + sign, inner),
            device_id_type=pl.DeviceIdType.MESH,
        )

    for part in order:
        for way in range(2):
            pl.when(on_line(outer + 1 - 2 * way))(
                lambda way=way, part=part: line_copy(way, 1, part, True).start()
            )

    def out_copy(source, chunk, target):
        return pltpu.make_async_remote_copy(
            src_ref=outb.at[source, chunk, target],
            dst_ref=held.at[source, chunk, inner],
            send_sem=out_send.at[source, chunk],
            recv_sem=out_recv.at[source, chunk],
            device_id=device(outer, target),
            device_id_type=pl.DeviceIdType.MESH,
        )

    def back_copy(source, chunk, target):
        return pltpu.make_async_remote_copy(
            src_ref=served.at[source, chunk, target],
            dst_ref=back.at[source, chunk, inner],
            send_sem=back_send.at[source, chunk],
            recv_sem=back_recv.at[source, chunk],
            device_id=device(outer, target),
            device_id_type=pl.DeviceIdType.MESH,
        )

    def others(from_buffer, to_buffer, source, chunk, send_sem, recv_sem):
        return pltpu.make_async_remote_copy(
            src_ref=from_buffer.at[source, chunk, pl.ds(0, plane - 1)],
            dst_ref=to_buffer.at[source, chunk, pl.ds(0, plane - 1)],
            send_sem=send_sem.at[source, chunk],
            recv_sem=recv_sem.at[source, chunk],
            device_id=device(outer, inner),
            device_id_type=pl.DeviceIdType.MESH,
        )

    def all_out(source, chunk):
        return others(outb, held, source, chunk, out_send, out_recv)

    def all_back(source, chunk):
        return others(served, back, source, chunk, back_send, back_recv)

    def sum_copy(way, dest, chunk):
        target = outer + 1 - 2 * way
        slot = jnp.where((dest == target) & (way == 1), steps, dest)
        return pltpu.make_async_remote_copy(
            src_ref=given.at[dest, chunk],
            dst_ref=brought.at[slot, chunk],
            send_sem=sum_send.at[way, dest, chunk],
            recv_sem=sum_recv.at[way, dest, chunk],
            device_id=device(target, inner),
            device_id_type=pl.DeviceIdType.MESH,
        )

    def over_ways(step, act):
        def one(way, unused):
            source = outer - (1 - 2 * way) * step
            pl.when(on_line(source) & ((step > 0) | (way == 0)))(lambda: act(way, source))
            return unused

        lax.fori_loop(0, 2, one, 0)

    def over_chunks(act):
        def one(chunk, unused):
            act(chunk)
            return unused

        lax.fori_loop(0, chunks, one, 0)

    down_iota = lax.broadcasted_iota(jnp.int32, (rows, rows), 0)
    over_iota = lax.broadcasted_iota(jnp.int32, (rows, rows), 1)

    def place_rows(source):
        earlier = jnp.where(down_iota < over_iota, 1.0, 0.0).astype(jnp.bfloat16)
        names = outer * plane + lax.broadcasted_iota(jnp.int32, (plane, rows), 0)
        start = lax.broadcasted_iota(jnp.int32, (plane, rows), 0).astype(jnp.float32) * block
        passed = jnp.zeros((plane, 1), jnp.float32)
        for route in range(top):
            one_hot = jnp.where(names == routes[source, route : route + 1, :], 1.0, 0.0)
            before = passed + jnp.dot(
                one_hot.astype(jnp.bfloat16), earlier, preferred_element_type=jnp.float32
            )
            there = jnp.sum(one_hot, axis=0, keepdims=True)
            slot = jnp.sum((before + start) * one_hot, axis=0, keepdims=True)
            slots[source, route : route + 1, :] = slot + there - 1.0
            passed = passed + jnp.sum(one_hot, axis=1, keepdims=True)

    def take_in(step):
        def small(way, source):
            def fetch():
                for part in order[:2]:
                    wait_part(way, step, part)

            pl.when(step > 0)(fetch)
            place_rows(source)

        over_ways(step, small)

        def per_chunk(chunk):
            def forward(way, source):
                line_dynamic(way, step, chunk).wait_recv()
                pl.when(on_line(outer + 1 - 2 * way))(
                    lambda: line_dynamic(way, step + 1, chunk).start()
                )

            pl.when(step > 0)(lambda: over_ways(step, forward))

            def dispatch(way, source):
                spot = lax.broadcasted_iota(jnp.int32, (spots, rows), 0).astype(jnp.float32)
                chosen = spot == slots[source, 0:1, :]
                for route in range(1, top):
                    chosen = chosen | (spot == slots[source, route : route + 1, :])
                select = jnp.where(chosen, 1.0, 0.0).astype(jnp.bfloat16)
                picked = jnp.dot(select, xs[source, chunk], preferred_element_type=jnp.float32)
                outb[source, chunk] = picked.astype(jnp.bfloat16).reshape(plane, block, width)
                held[source, chunk, inner] = outb[source, chunk, inner]

                def give(number, unused):
                    out_copy(source, chunk, lax.rem(inner + number, plane)).start()
                    return unused

                lax.fori_loop(1, plane, give, 0)

            over_ways(step, dispatch)

        over_chunks(per_chunk)

    def wait_part(way, step, part):
        line_copy(way, step, part).wait_recv()
        pl.when(on_line(outer + 1 - 2 * way))(lambda: line_copy(way, step + 1, part).start())

    def line_dynamic(way, step, chunk):
        sign = 1 - 2 * way
        place = outer - sign * (step - 1)
        return pltpu.make_async_remote_copy(
            src_ref=xs.at[place, chunk],
            dst_ref=xs.at[place, chunk],
            send_sem=line_send.at[way, step, chunk],
            recv_sem=line_recv.at[way, step, chunk],
            device_id=device(outer + sign, inner),
            device_id_type=pl.DeviceIdType.MESH,
        )

    def serve(step):
        def run(way, source):
            gate_acc[...] = jnp.zeros(gate_acc.shape, jnp.float32)
            up_acc[...] = jnp.zeros(up_acc.shape, jnp.float32)

            def first(chunk):
                all_out(source, chunk).wait_recv()
                taken = held[source, chunk].reshape(spots, width)
                gate_acc[...] += jnp.dot(
                    taken, gate_w[chunk], preferred_element_type=jnp.float32
                )
                up_acc[...] += jnp.dot(taken, up_w[chunk], preferred_element_type=jnp.float32)

            over_chunks(first)
            gate = gate_acc[...]
            hidden = (gate / (1.0 + jnp.exp(-gate)) * up_acc[...]).astype(jnp.bfloat16)
            for chunk in range(chunks):
                part = slice(chunk * width, (chunk + 1) * width)
                result = jnp.dot(hidden, down_w[:, part], preferred_element_type=jnp.float32)
                served[source, chunk] = result.astype(jnp.bfloat16).reshape(plane, block, width)
                back[source, chunk, inner] = served[source, chunk, inner]

                def give(number, unused, chunk=chunk):
                    back_copy(source, chunk, lax.rem(inner + number, plane)).start()
                    return unused

                lax.fori_loop(1, plane, give, 0)

        over_ways(step, run)

    def column(row):
        return jnp.sum(jnp.where(down_iota == over_iota, row, 0.0), axis=1, keepdims=True)

    def combine(step):
        def run(way, source):
            spot = lax.broadcasted_iota(jnp.int32, (rows, spots), 1).astype(jnp.float32)
            picks, scales = [], []
            for route in range(top):
                at = column(slots[source, route : route + 1, :])
                picks.append(jnp.where(spot == at, 1.0, 0.0).astype(jnp.bfloat16))
                scales.append(column(weights[source, route : route + 1, :]))

            def one(chunk):
                all_back(source, chunk).wait_recv()
                came = back[source, chunk].reshape(spots, width)
                total = None
                for pick, scale in zip(picks, scales):
                    term = jnp.dot(pick, came, preferred_element_type=jnp.float32) * scale
                    total = term if total is None else total + term

                def keep():
                    own_sum[chunk] = total

                def hand():
                    given[source, chunk] = total.astype(jnp.bfloat16)
                    pl.when(jnp.logical_not(on_line(outer - (1 - 2 * (1 - way)))))(
                        lambda: sum_copy(1 - way, source, chunk).start()
                    )

                pl.when(step == 0)(keep)
                pl.when(step > 0)(hand)

            over_chunks(one)

        over_ways(step, run)

    for copy in loads:
        copy.wait()
    take_in(jnp.int32(0))
    at_end = (outer == 0) | (outer == steps - 1)
    late = jnp.where(at_end, 2, 1)

    def task(number, unused):
        step = number // 3
        kind = lax.rem(number, 3)
        pl.when(kind == 0)(lambda: serve(step))
        pl.when((kind == late) & (step + 1 < steps))(lambda: take_in(step + 1))
        pl.when((kind > 0) & (kind != late))(lambda: combine(step))
        return unused

    lax.fori_loop(0, 3 * steps, task, 0)

    def pass_sums(turn, unused):
        def one(chunk):
            def onward(way, unused):
                dest = jnp.where(way == 0, turn, steps - 1 - turn)
                beyond = jnp.where(way == 0, dest > outer, dest < outer)

                def add():
                    sum_copy(way, dest, chunk).wait_recv()
                    given[dest, chunk] = (
                        given[dest, chunk].astype(jnp.float32)
                        + brought[dest, chunk].astype(jnp.float32)
                    ).astype(jnp.bfloat16)
                    sum_copy(way, dest, chunk).start()

                pl.when(beyond & on_line(outer - (1 - 2 * way)))(add)
                return unused

            lax.fori_loop(0, 2, onward, 0)

        over_chunks(one)
        return unused

    lax.fori_loop(1, steps, pass_sums, 0)

    def gather(chunk):
        def from_way(way, unused):
            def add():
                sum_copy(way, outer, chunk).wait_recv()
                slot = jnp.where(way == 0, outer, steps)
                own_sum[chunk] += brought[slot, chunk].astype(jnp.float32)

            pl.when(on_line(outer - (1 - 2 * way)))(add)
            return unused

        lax.fori_loop(0, 2, from_way, 0)
        own_sum[chunk] += alpha_mix * x_ref[chunk].astype(jnp.float32)

    over_chunks(gather)
    features = chunks * width
    total = None
    for chunk in range(chunks):
        term = jnp.sum(own_sum[chunk], axis=1, keepdims=True)
        total = term if total is None else total + term
    center = total / features
    total = None
    for chunk in range(chunks):
        term = jnp.sum(jnp.square(own_sum[chunk] - center), axis=1, keepdims=True)
        total = term if total is None else total + term
    spread = lax.rsqrt(total / features + eps_norm)
    for chunk in range(chunks):
        part = slice(chunk * width, (chunk + 1) * width)
        o_ref[:, part] = (
            (own_sum[chunk] - center) * spread * gain_ref[:, part] + bias_ref[:, part]
        ).astype(o_ref.dtype)

    def settle(step, unused):
        def sent(way, source):
            def onward():
                for part in range(parts):
                    line_copy(way, step + 1, part).wait_send()

            pl.when(on_line(outer + 1 - 2 * way))(onward)

            def one(chunk):
                all_out(source, chunk).wait_send()
                all_back(source, chunk).wait_send()
                pl.when(step > 0)(lambda: sum_copy(1 - way, source, chunk).wait_send())

            over_chunks(one)

        def own_up(way, unused):
            pl.when((step == 0) & (way == 1) & on_line(outer - 1))(own_down)
            return unused

        def own_down():
            for part in range(parts):
                line_copy(1, 1, part).wait_send()

        over_ways(step, sent)
        own_up(1, 0)
        return unused

    lax.fori_loop(0, steps, settle, 0)


def run_experts(x, routes, route_weights, gate, up, down, gain, bias, sp_size, tp_size):
    pair = 2 if sp_size % 2 == 0 else 1
    steps, plane = sp_size // pair, pair * tp_size
    chunks, rows, width = x.shape
    top = routes.shape[1]
    hidden = gate.shape[2]
    spots = plane * (2 * rows * top // (sp_size * tp_size))
    bf16, f32, dma = jnp.bfloat16, jnp.float32, pltpu.SemaphoreType.DMA
    blocks = pltpu.VMEM((steps, chunks, plane, spots // plane, width), bf16)
    return pl.pallas_call(
        functools.partial(expert_kernel, steps, plane, tp_size),
        out_shape=jax.ShapeDtypeStruct((rows, chunks * width), bf16),
        in_specs=[VMEM] * 3 + [ANY] * 3 + [VMEM] * 2,
        out_specs=VMEM,
        scratch_shapes=[
            pltpu.VMEM((steps, chunks, rows, width), bf16),
            pltpu.VMEM((steps, top, rows), jnp.int32),
            pltpu.VMEM((steps, top, rows), f32),
            pltpu.VMEM((steps, top, rows), f32),
            blocks,
            blocks,
            blocks,
            blocks,
            pltpu.VMEM((steps, chunks, rows, width), bf16),
            pltpu.VMEM((steps + 1, chunks, rows, width), bf16),
            pltpu.VMEM((chunks, rows, width), f32),
            pltpu.VMEM((spots, hidden), f32),
            pltpu.VMEM((spots, hidden), f32),
            pltpu.VMEM((chunks, width, hidden), gate.dtype),
            pltpu.VMEM((chunks, width, hidden), up.dtype),
            pltpu.VMEM(down.shape[1:], down.dtype),
            dma((2, steps + 1, chunks + 2)),
            dma((2, steps + 1, chunks + 2)),
            dma((steps, chunks)),
            dma((steps, chunks)),
            dma((steps, chunks)),
            dma((steps, chunks)),
            dma((2, steps, chunks)),
            dma((2, steps, chunks)),
            dma((6,)),
        ],
        compiler_params=pltpu.CompilerParams(
            collective_id=2, has_side_effects=True, vmem_limit_bytes=60 * 1024 * 1024
        ),
    )(
        x,
        routes.T,
        route_weights.T,
        gate.reshape(chunks, width, hidden),
        up.reshape(chunks, width, hidden),
        down.reshape(down.shape[1:]),
        gain[None, :],
        bias[None, :],
    )


def per_device(
    queries,
    key_heads,
    value_heads,
    documents,
    query_gain,
    key_gain,
    out_gain,
    out_proj,
    residual,
    mid_gain,
    mid_bias,
    routes,
    route_weights,
    expert_gate,
    expert_up,
    expert_down,
    final_gain,
    final_bias,
):
    sp_size = lax.axis_size("sp")
    tp_size = lax.axis_size("tp")
    if key_heads.shape[1] != HEAD or expert_gate.shape[0] != 1:
        raise ValueError("unsupported placement")
    middle = run_front(
        queries,
        key_heads,
        value_heads,
        documents,
        query_gain,
        key_gain,
        out_gain,
        out_proj,
        residual,
        mid_gain,
        mid_bias,
        sp_size,
        tp_size,
        CHUNKS,
    )
    return run_experts(
        middle,
        routes,
        route_weights,
        expert_gate,
        expert_up,
        expert_down,
        final_gain,
        final_bias,
        sp_size,
        tp_size,
    )


def solution(mesh):
    return jax.shard_map(
        per_device,
        mesh=mesh,
        in_specs=(
            P("sp", "tp"),
            P("sp", "tp"),
            P("sp", "tp"),
            P("sp"),
            P(),
            P(),
            P(),
            P(),
            P(("sp", "tp"), None),
            P(),
            P(),
            P(("sp", "tp"), None),
            P(("sp", "tp"), None),
            P(("sp", "tp"), None, None),
            P(("sp", "tp"), None, None),
            P(("sp", "tp"), None, None),
            P(),
            P(),
        ),
        out_specs=P(("sp", "tp"), None),
        check_vma=False,
    )
```

```python
import functools

import jax
import jax.numpy as jnp
from jax import lax
from jax.experimental import pallas as pl
from jax.experimental.pallas import tpu as pltpu
from jax.sharding import PartitionSpec as P

HEAD = 128
GRID = 64
CHUNKS = 4
SERVE_LAG = 3
COMBINE_LAG = 2


eps_norm = 1e-06
alpha_mix = 8.0**0.25
theta_base = 10000.0
score_factor = HEAD ** (-0.5) * 1.4426950408889634
VMEM = pl.BlockSpec(memory_space=pltpu.VMEM)
ANY = pl.BlockSpec(memory_space=pl.ANY)
SMEM = pl.BlockSpec(memory_space=pltpu.SMEM)


def layer_norm(stream, gain_vec, bias_vec):
    center = jnp.mean(stream, axis=-1, keepdims=True)
    spread = jnp.mean(jnp.square(stream - center), axis=-1, keepdims=True)
    return (stream - center) * lax.rsqrt(spread + eps_norm) * gain_vec + bias_vec


def turned(values, gain, cosine, sine):
    inv_rms = lax.rsqrt(jnp.mean(values * values, axis=1, keepdims=True) + eps_norm)
    values = values * inv_rms * gain
    return (values * cosine + pltpu.roll(values, HEAD // 2, 1) * sine).astype(jnp.bfloat16)


def front_kernel(
    size,
    pair,
    tp_size,
    q_ref,
    k_ref,
    v_ref,
    doc_ref,
    qdoc_ref,
    q_gain_ref,
    k_gain_ref,
    row_ref,
    col_ref,
    gain_ref,
    proj_hbm,
    res_ref,
    mid_gain_ref,
    mid_bias_ref,
    mid_ref,
    kv,
    docs,
    q_rot,
    m_ref,
    l_ref,
    acc_ref,
    o_buf,
    whole,
    proj,
    line_send,
    line_recv,
    mate_send,
    mate_recv,
    tp_send,
    tp_recv,
    own_sem,
):
    me = lax.axis_index("sp")
    lane = lax.axis_index("tp")
    inner = lax.rem(me, pair)
    outer = me // pair
    steps = size // pair
    mate = outer * pair + lax.rem(inner + 1, pair)
    rows = k_ref.shape[0]
    pieces = doc_ref.shape[0]
    grouped = q_rot.shape[0]
    parts = 3

    load = pltpu.make_async_copy(proj_hbm, proj, own_sem.at[0])
    load.start()
    own = [
        pltpu.make_async_copy(v_ref, kv.at[me, 1], own_sem.at[1]),
        pltpu.make_async_copy(doc_ref, docs.at[me], own_sem.at[2]),
    ]
    for copy in own:
        copy.start()

    def on_line(place):
        return (place >= 0) & (place < steps)

    barrier = pltpu.get_barrier_semaphore()

    def greet(target):
        pl.semaphore_signal(
            barrier, inc=1, device_id=target, device_id_type=pl.DeviceIdType.MESH
        )

    peers = jnp.int32(tp_size - 1 + (pair - 1))
    for sign in (1, -1):
        there = on_line(outer + sign)
        pl.when(there)(lambda sign=sign: greet({"sp": (outer + sign) * pair + inner}))
        peers = peers + there.astype(jnp.int32)
    if pair == 2:
        greet({"sp": mate})
    tp_targets = [lax.rem(lane + step, tp_size) for step in range(1, tp_size)]
    for target in tp_targets:
        greet({"tp": target})
    pl.semaphore_wait(barrier, peers)

    def piece(place, part, first):
        if part == 2:
            return (doc_ref if first else docs.at[place]), docs.at[place]
        return (v_ref if first and part == 1 else kv.at[place, part]), kv.at[place, part]

    def line_copy(way, step, part, first=False):
        sign = 1 - 2 * way
        place = (outer - sign * (step - 1)) * pair + inner
        src, dst = piece(place, part, first)
        return pltpu.make_async_remote_copy(
            src_ref=src,
            dst_ref=dst,
            send_sem=line_send.at[way, step, part],
            recv_sem=line_recv.at[way, step, part],
            device_id={"sp": (outer + sign) * pair + inner},
            device_id_type=pl.DeviceIdType.MESH,
        )

    def mate_copy(way, step, part, first=False):
        sign = 1 - 2 * way
        place = (outer - sign * step) * pair + inner
        src, dst = piece(place, part, first)
        return pltpu.make_async_remote_copy(
            src_ref=src,
            dst_ref=dst,
            send_sem=mate_send.at[way, step, part],
            recv_sem=mate_recv.at[way, step, part],
            device_id={"sp": mate},
            device_id_type=pl.DeviceIdType.MESH,
        )

    def send_own(part):
        for way in range(2):
            pl.when(on_line(outer + 1 - 2 * way))(
                lambda way=way: line_copy(way, 1, part, True).start()
            )
        if pair == 2:
            mate_copy(0, 0, part, True).start()

    send_own(1)
    send_own(2)
    grid_rows = row_ref.shape[1]
    span = col_ref.shape[1]

    def tables(block):
        cosine = row_ref[0, pl.ds(block, 1)] + col_ref[0]
        sine = row_ref[1, pl.ds(block, 1)] + col_ref[1]
        return cosine, sine

    def turn_keys(block, unused):
        cosine, sine = tables(block)
        here = pl.ds(pl.multiple_of(block * span, span), span)
        kv[me, 0, here] = turned(k_ref[here].astype(jnp.float32), k_gain_ref[...], cosine, sine)
        return unused

    lax.fori_loop(0, grid_rows, turn_keys, 0)
    send_own(0)

    def turn_queries(block, unused):
        cosine, sine = tables(block)
        here = pl.ds(pl.multiple_of(block * span, span), span)
        for head in range(grouped):
            q_rot[head, here] = turned(
                q_ref[here, head * HEAD : (head + 1) * HEAD].astype(jnp.float32),
                q_gain_ref[...],
                cosine,
                sine,
            )
        return unused

    lax.fori_loop(0, grid_rows, turn_queries, 0)
    m_ref[...] = jnp.full(m_ref.shape, -1e30, jnp.float32)
    l_ref[...] = jnp.zeros(l_ref.shape, jnp.float32)
    acc_ref[...] = jnp.zeros(acc_ref.shape, jnp.float32)
    for copy in own:
        copy.wait()
    chunk = 256

    def advance(place):
        keys = kv[place, 0]
        values = kv[place, 1]
        doc_rows = docs[place]
        key_docs = jnp.concatenate([doc_rows[i : i + 1] for i in range(pieces)], axis=1)
        for head in range(grouped):
            for first in range(0, rows, chunk):
                part = pl.ds(first, chunk)
                scores = lax.dot_general(
                    q_rot[head, part],
                    keys,
                    (((1,), (1,)), ((), ())),
                    preferred_element_type=jnp.float32,
                )
                allowed = qdoc_ref[part, 0:1] == key_docs
                scores = jnp.where(allowed, scores * score_factor, -1e30)
                old_max = m_ref[head, part]
                new_max = jnp.maximum(old_max, jnp.max(scores, axis=1, keepdims=True))
                base = jnp.maximum(new_max[:, 0:1], -1e29)
                weights = jnp.exp2(scores - base)
                rescale = jnp.exp2(old_max - new_max)
                l_ref[head, part] = l_ref[head, part] * rescale + jnp.sum(
                    weights, axis=1, keepdims=True
                )
                acc_ref[head, part] = acc_ref[head, part] * rescale + jnp.dot(
                    weights.astype(jnp.bfloat16), values, preferred_element_type=jnp.float32
                )
                m_ref[head, part] = new_max

    def stage(step, unused):
        for group in ((1, 2), (0,)):
            for way in range(2):
                sign = 1 - 2 * way

                def take(way=way, sign=sign, group=group):
                    for part in group:
                        line_copy(way, step, part).wait_recv()

                    def pass_on():
                        for part in group:
                            line_copy(way, step + 1, part).start()

                    pl.when(on_line(outer + sign))(pass_on)
                    if pair == 2:
                        for part in group:
                            mate_copy(way, step, part).start()

                pl.when((step > 0) & on_line(outer - sign * step))(take)

        def visit(number, unused):
            way = lax.rem(number, 2)
            across = number // 2
            there = outer - (1 - 2 * way) * step

            def work():
                if pair == 2:

                    def arrive():
                        for part in range(parts):
                            mate_copy(way, step, part).wait_recv()

                    pl.when(across == 1)(arrive)
                advance(there * pair + lax.rem(inner + across, pair))

            pl.when(on_line(there) & ((step > 0) | (way == 0)))(work)
            return unused

        lax.fori_loop(0, 2 * pair, visit, 0)
        return unused

    lax.fori_loop(0, steps, stage, 0)
    for head in range(grouped):
        o_buf[:, head * HEAD : (head + 1) * HEAD] = (acc_ref[head] / l_ref[head]).astype(
            o_buf.dtype
        )

    out_rows, width = whole.shape[0], o_buf.shape[1]

    def rows_of(number):
        return pl.ds(pl.multiple_of(number * out_rows, out_rows), out_rows)

    mine = whole.at[:, pl.ds(pl.multiple_of(lane * width, width), width)]
    swaps = []
    for step, target in enumerate(tp_targets):
        copy = pltpu.make_async_remote_copy(
            src_ref=o_buf.at[rows_of(target)],
            dst_ref=mine,
            send_sem=tp_send.at[step],
            recv_sem=tp_recv.at[step],
            device_id={"tp": target},
            device_id_type=pl.DeviceIdType.MESH,
        )
        copy.start()
        swaps.append(copy)
    keep = pltpu.make_async_copy(o_buf.at[rows_of(lane)], mine, own_sem.at[3])
    keep.start()

    load.wait()
    for copy in swaps:
        copy.wait_recv()
    keep.wait()
    taken = whole[...].astype(jnp.float32)
    mean_square = jnp.mean(taken * taken, axis=1, keepdims=True)
    scaled = (taken * gain_ref[...]).astype(jnp.bfloat16)
    projected = jnp.dot(scaled, proj[...], preferred_element_type=jnp.float32)
    projected = projected * lax.rsqrt(mean_square + eps_norm)
    stream = alpha_mix * res_ref[...].astype(jnp.float32) + projected
    middle = layer_norm(stream, mid_gain_ref[...], mid_bias_ref[...]).astype(jnp.bfloat16)
    block = mid_ref.shape[2]
    for chunk in range(mid_ref.shape[0]):
        mid_ref[chunk] = middle[:, chunk * block : (chunk + 1) * block]

    for copy in swaps:
        copy.wait_send()

    def settle(step, unused):
        for way in range(2):
            sign = 1 - 2 * way

            def sent(way=way):
                for part in range(parts):
                    line_copy(way, step + 1, part).wait_send()

            pl.when(on_line(outer - sign * step) & on_line(outer + sign))(sent)
            if pair == 2:

                def gave(way=way):
                    for part in range(parts):
                        mate_copy(way, step, part).wait_send()

                first = (step > 0) | (way == 0)
                pl.when(on_line(outer - sign * step) & first)(gave)
        return unused

    lax.fori_loop(0, steps, settle, 0)


def trig_tables(tok_rows, offset):
    pair_count = HEAD // 4
    inv_freq = theta_base ** (-jnp.arange(pair_count, dtype=jnp.float32) / pair_count)
    grid_rows = (offset // GRID + jnp.arange(tok_rows // GRID, dtype=jnp.int32)).astype(jnp.float32)
    grid_cols = jnp.arange(GRID, dtype=jnp.int32).astype(jnp.float32)
    tables = []
    for at, place in enumerate((grid_rows, grid_cols)):
        angles = place[:, None] * inv_freq[None, :]
        blank = jnp.zeros_like(angles)
        cosine, sine = jnp.cos(angles), jnp.sin(angles)
        order = (lambda a, b: [a, blank, b, blank]) if at == 0 else (lambda a, b: [blank, a, blank, b])
        tables.append(
            jnp.stack(
                [
                    jnp.concatenate(order(cosine, cosine), axis=1),
                    jnp.concatenate(order(-sine, sine), axis=1),
                ]
            )
        )
    return tables


def run_front(
    queries,
    keys,
    values,
    documents,
    query_gain,
    key_gain,
    out_gain,
    out_proj,
    residual,
    mid_gain,
    mid_bias,
    size,
    tp_size,
    chunks,
):
    pair = 2 if size % 2 == 0 else 1
    rows, width = queries.shape
    grouped = width // HEAD
    out_rows, model_width = residual.shape
    steps = size // pair
    row_table, col_table = trig_tables(rows, lax.axis_index("sp") * rows)
    query_docs = jnp.broadcast_to(documents[:, None], (rows, HEAD))
    dma = pltpu.SemaphoreType.DMA
    return pl.pallas_call(
        functools.partial(front_kernel, size, pair, tp_size),
        out_shape=jax.ShapeDtypeStruct((chunks, out_rows, model_width // chunks), jnp.bfloat16),
        in_specs=[VMEM] * 10 + [ANY] + [VMEM] * 3,
        out_specs=VMEM,
        scratch_shapes=[
            pltpu.VMEM((size, 2, rows, HEAD), jnp.bfloat16),
            pltpu.VMEM((size, rows // HEAD, HEAD), jnp.int32),
            pltpu.VMEM((grouped, rows, HEAD), jnp.bfloat16),
            pltpu.VMEM((grouped, rows, HEAD), jnp.float32),
            pltpu.VMEM((grouped, rows, HEAD), jnp.float32),
            pltpu.VMEM((grouped, rows, HEAD), jnp.float32),
            pltpu.VMEM((rows, width), jnp.bfloat16),
            pltpu.VMEM((out_rows, width * tp_size), jnp.bfloat16),
            pltpu.VMEM(out_proj.shape, out_proj.dtype),
            dma((2, steps + 1, 3)),
            dma((2, steps + 1, 3)),
            dma((2, steps, 3)),
            dma((2, steps, 3)),
            dma((tp_size,)),
            dma((tp_size,)),
            dma((4,)),
        ],
        compiler_params=pltpu.CompilerParams(
            collective_id=0, has_side_effects=True, vmem_limit_bytes=56 * 1024 * 1024
        ),
    )(
        queries,
        keys,
        values,
        documents.reshape(rows // HEAD, HEAD),
        query_docs,
        query_gain[None, :],
        key_gain[None, :],
        row_table,
        col_table,
        out_gain[None, :],
        out_proj,
        residual,
        mid_gain[None, :],
        mid_bias[None, :],
    )


def expert_kernel(
    steps,
    plane,
    tp_size,
    x_ref,
    route_ref,
    weight_ref,
    gate_hbm,
    up_hbm,
    down_hbm,
    gain_ref,
    bias_ref,
    o_ref,
    xs,
    routes,
    weights,
    slots,
    outb,
    held,
    served,
    back,
    given,
    brought,
    own_sum,
    gate_acc,
    up_acc,
    picks,
    scales,
    gate_w,
    up_w,
    down_w,
    line_send,
    line_recv,
    out_send,
    out_recv,
    back_send,
    back_recv,
    sum_send,
    sum_recv,
    own_sem,
):
    me = lax.axis_index("sp") * tp_size + lax.axis_index("tp")
    outer = me // plane
    inner = lax.rem(me, plane)
    chunks, rows, width = x_ref.shape
    block = outb.shape[3]
    spots = plane * block
    top = route_ref.shape[0]
    parts = chunks + 2
    order = [chunks, chunks + 1] + list(range(chunks))

    loads = [
        pltpu.make_async_copy(x_ref, xs.at[outer], own_sem.at[0]),
        pltpu.make_async_copy(route_ref, routes.at[outer], own_sem.at[1]),
        pltpu.make_async_copy(weight_ref, weights.at[outer], own_sem.at[2]),
        pltpu.make_async_copy(gate_hbm, gate_w, own_sem.at[3]),
        pltpu.make_async_copy(up_hbm, up_w, own_sem.at[4]),
        pltpu.make_async_copy(down_hbm, down_w, own_sem.at[5]),
    ]
    for copy in loads:
        copy.start()

    def device(place, number):
        index = place * plane + number
        return {"sp": index // tp_size, "tp": lax.rem(index, tp_size)}

    def on_line(place):
        return (place >= 0) & (place < steps)

    barrier = pltpu.get_barrier_semaphore()

    def greet(place, number):
        pl.semaphore_signal(
            barrier,
            inc=1,
            device_id=device(place, number),
            device_id_type=pl.DeviceIdType.MESH,
        )

    peers = jnp.int32(plane - 1)
    for sign in (1, -1):
        there = on_line(outer + sign)
        pl.when(there)(lambda sign=sign: greet(outer + sign, inner))
        peers = peers + there.astype(jnp.int32)

    def greet_plane(step, unused):
        greet(outer, lax.rem(inner + step, plane))
        return unused

    lax.fori_loop(1, plane, greet_plane, 0)
    pl.semaphore_wait(barrier, peers)

    def piece(place, part, first):
        if part == chunks:
            return (route_ref if first else routes.at[place]), routes.at[place]
        if part == chunks + 1:
            return (weight_ref if first else weights.at[place]), weights.at[place]
        return (x_ref.at[part] if first else xs.at[place, part]), xs.at[place, part]

    def line_copy(way, step, part, first=False):
        sign = 1 - 2 * way
        place = outer - sign * (step - 1)
        src, dst = piece(place, part, first)
        return pltpu.make_async_remote_copy(
            src_ref=src,
            dst_ref=dst,
            send_sem=line_send.at[way, step, part],
            recv_sem=line_recv.at[way, step, part],
            device_id=device(outer + sign, inner),
            device_id_type=pl.DeviceIdType.MESH,
        )

    half = chunks // 2
    depth = (outer, steps - 1 - outer)

    def send_own(way, send):
        there = on_line(outer + 1 - 2 * way)
        for part in send:
            pl.when(there)(lambda part=part: line_copy(way, 1, part, True).start())

    for way in range(2):
        send_own(way, order[: 2 + half])
        pl.when(depth[way] == 0)(lambda way=way: send_own(way, order[2 + half :]))

    def out_copy(source, chunk, target):
        return pltpu.make_async_remote_copy(
            src_ref=outb.at[source, chunk, target],
            dst_ref=held.at[source, chunk, inner],
            send_sem=out_send.at[source, chunk],
            recv_sem=out_recv.at[source, chunk],
            device_id=device(outer, target),
            device_id_type=pl.DeviceIdType.MESH,
        )

    def back_copy(source, chunk, target):
        return pltpu.make_async_remote_copy(
            src_ref=served.at[source, chunk, target],
            dst_ref=back.at[source, chunk, inner],
            send_sem=back_send.at[source, chunk],
            recv_sem=back_recv.at[source, chunk],
            device_id=device(outer, target),
            device_id_type=pl.DeviceIdType.MESH,
        )

    def others(from_buffer, to_buffer, source, chunk, send_sem, recv_sem):
        return pltpu.make_async_remote_copy(
            src_ref=from_buffer.at[source, chunk, pl.ds(0, plane - 1)],
            dst_ref=to_buffer.at[source, chunk, pl.ds(0, plane - 1)],
            send_sem=send_sem.at[source, chunk],
            recv_sem=recv_sem.at[source, chunk],
            device_id=device(outer, inner),
            device_id_type=pl.DeviceIdType.MESH,
        )

    def all_out(source, chunk):
        return others(outb, held, source, chunk, out_send, out_recv)

    def all_back(source, chunk):
        return others(served, back, source, chunk, back_send, back_recv)

    def sum_copy(way, dest, chunk):
        target = outer + 1 - 2 * way
        slot = jnp.where((dest == target) & (way == 1), steps, dest)
        return pltpu.make_async_remote_copy(
            src_ref=given.at[dest, chunk],
            dst_ref=brought.at[slot, chunk],
            send_sem=sum_send.at[way, dest, chunk],
            recv_sem=sum_recv.at[way, dest, chunk],
            device_id=device(target, inner),
            device_id_type=pl.DeviceIdType.MESH,
        )

    def over_ways(step, act):
        def one(way, unused):
            source = outer - (1 - 2 * way) * step
            pl.when(on_line(source) & ((step > 0) | (way == 0)))(lambda: act(way, source))
            return unused

        lax.fori_loop(0, 2, one, 0)

    def over_chunks(act):
        def one(chunk, unused):
            act(chunk)
            return unused

        lax.fori_loop(0, chunks, one, 0)

    down_iota = lax.broadcasted_iota(jnp.int32, (rows, rows), 0)
    over_iota = lax.broadcasted_iota(jnp.int32, (rows, rows), 1)

    def place_rows(source):
        earlier = jnp.where(down_iota < over_iota, 1.0, 0.0).astype(jnp.bfloat16)
        names = outer * plane + lax.broadcasted_iota(jnp.int32, (plane, rows), 0)
        start = lax.broadcasted_iota(jnp.int32, (plane, rows), 0).astype(jnp.float32) * block
        passed = jnp.zeros((plane, 1), jnp.float32)
        for route in range(top):
            one_hot = jnp.where(names == routes[source, route : route + 1, :], 1.0, 0.0)
            before = passed + jnp.dot(
                one_hot.astype(jnp.bfloat16), earlier, preferred_element_type=jnp.float32
            )
            there = jnp.sum(one_hot, axis=0, keepdims=True)
            slot = jnp.sum((before + start) * one_hot, axis=0, keepdims=True)
            slots[source, route : route + 1, :] = slot + there - 1.0
            passed = passed + jnp.sum(one_hot, axis=1, keepdims=True)

    def dispatch(source, chunk):
        pl.when(chunk == 0)(lambda: place_rows(source))
        spot = lax.broadcasted_iota(jnp.int32, (spots, rows), 0).astype(jnp.float32)
        chosen = spot == slots[source, 0:1, :]
        for route in range(1, top):
            chosen = chosen | (spot == slots[source, route : route + 1, :])
        select = jnp.where(chosen, 1.0, 0.0).astype(jnp.bfloat16)
        picked = jnp.dot(select, xs[source, chunk], preferred_element_type=jnp.float32)
        outb[source, chunk] = picked.astype(jnp.bfloat16).reshape(plane, block, width)
        held[source, chunk, inner] = outb[source, chunk, inner]

        def give(number, unused):
            out_copy(source, chunk, lax.rem(inner + number, plane)).start()
            return unused

        lax.fori_loop(1, plane, give, 0)

    def place_of(way, number, full):
        pairs = number // half
        out = pairs < full
        step = jnp.where(out, pairs + 1, 2 * full - pairs)
        chunk = jnp.where(out, 0, half) + lax.rem(number, half)
        return step, chunk, outer - (1 - 2 * way) * step

    def receive(way, number, full):
        step, chunk, source = place_of(way, number, full)

        def small():
            for part in order[:2]:
                wait_part(way, step, part)

        pl.when(chunk == 0)(small)
        line_dynamic(way, step, chunk).wait_recv()
        pl.when(on_line(outer + 1 - 2 * way))(
            lambda: line_dynamic(way, step + 1, chunk).start()
        )

    def wait_part(way, step, part):
        line_copy(way, step, part).wait_recv()
        pl.when(on_line(outer + 1 - 2 * way))(lambda: line_copy(way, step + 1, part).start())

    def line_dynamic(way, step, chunk):
        sign = 1 - 2 * way
        place = outer - sign * (step - 1)
        return pltpu.make_async_remote_copy(
            src_ref=xs.at[place, chunk],
            dst_ref=xs.at[place, chunk],
            send_sem=line_send.at[way, step, chunk],
            recv_sem=line_recv.at[way, step, chunk],
            device_id=device(outer + sign, inner),
            device_id_type=pl.DeviceIdType.MESH,
        )

    def serve(source, chunk):
        all_out(source, chunk).wait_recv()
        taken = held[source, chunk].reshape(spots, width)
        gate = jnp.dot(taken, gate_w[chunk], preferred_element_type=jnp.float32)
        up = jnp.dot(taken, up_w[chunk], preferred_element_type=jnp.float32)

        def fresh():
            gate_acc[source] = gate
            up_acc[source] = up

        def add():
            gate_acc[source] += gate
            up_acc[source] += up

        pl.when(chunk == 0)(fresh)
        pl.when(chunk > 0)(add)
        pl.when(chunk == chunks - 1)(lambda: finish(source))

    def finish(source):
        gate = gate_acc[source]
        hidden = (gate / (1.0 + jnp.exp(-gate)) * up_acc[source]).astype(jnp.bfloat16)
        for chunk in range(chunks):
            part = slice(chunk * width, (chunk + 1) * width)
            result = jnp.dot(hidden, down_w[:, part], preferred_element_type=jnp.float32)
            served[source, chunk] = result.astype(jnp.bfloat16).reshape(plane, block, width)
            back[source, chunk, inner] = served[source, chunk, inner]

            def give(number, unused, chunk=chunk):
                back_copy(source, chunk, lax.rem(inner + number, plane)).start()
                return unused

            lax.fori_loop(1, plane, give, 0)

    def column(row):
        return jnp.sum(jnp.where(down_iota == over_iota, row, 0.0), axis=1, keepdims=True)

    def combine(way, source, chunk):
        def prepare():
            spot = lax.broadcasted_iota(jnp.int32, (rows, spots), 1).astype(jnp.float32)
            for route in range(top):
                at = column(slots[source, route : route + 1, :])
                picks[way, route] = jnp.where(spot == at, 1.0, 0.0).astype(jnp.bfloat16)
                scale = column(weights[source, route : route + 1, :])
                scales[way, route] = jnp.broadcast_to(scale, scales.shape[2:])

        pl.when(chunk == 0)(prepare)
        all_back(source, chunk).wait_recv()
        came = back[source, chunk].reshape(spots, width)
        total = None
        for route in range(top):
            term = jnp.dot(picks[way, route], came, preferred_element_type=jnp.float32)
            term = term * scales[way, route][:, 0:1]
            total = term if total is None else total + term

        def keep():
            own_sum[chunk] = total

        def hand():
            given[source, chunk] = total.astype(jnp.bfloat16)
            pl.when(jnp.logical_not(on_line(outer - (1 - 2 * (1 - way)))))(
                lambda: sum_copy(1 - way, source, chunk).start()
            )

        pl.when(way == 2)(keep)
        pl.when(way < 2)(hand)

    for copy in loads[:3]:
        copy.wait()

    def first(chunk, unused):
        dispatch(outer, chunk)
        return unused

    lax.fori_loop(0, chunks, first, 0)

    def stage(number, unused):
        def load_weights():
            for copy in loads[3:]:
                copy.wait()

        def each_way(way, unused):
            full = jnp.where(way == 0, depth[0], depth[1])

            def take():
                receive(way, number, full)

                def rest():
                    for part in order[2 + half :]:
                        line_copy(way, 1, part, True).start()

                pl.when((number == full * chunks - 1) & on_line(outer + 1 - 2 * way))(rest)
                step, chunk, source = place_of(way, number, full)
                dispatch(source, chunk)

            pl.when(number < full * chunks)(take)
            return unused

        lax.fori_loop(0, 2, each_way, 0)
        pl.when(number == 0)(load_weights)

        def serve_way(way, unused):
            full = jnp.where(way == 0, depth[0], depth[1])
            at = number - SERVE_LAG
            step, chunk, source = place_of(way, at, full)
            mine = way == 2
            source = jnp.where(mine, outer, source)
            chunk = jnp.where(mine, number, chunk)
            live = jnp.where(mine, number < chunks, (at >= 0) & (at < full * chunks))
            pl.when(live)(lambda: serve(source, chunk))
            return unused

        lax.fori_loop(0, 3, serve_way, 0)

        def combine_way(turn, unused):
            way = turn // 2
            full = jnp.where(way == 0, depth[0], depth[1])
            start = (full + 1) * half - 1 + SERVE_LAG + COMBINE_LAG
            at = 2 * (number - start) + lax.rem(turn, 2)
            mine = way == 2
            at = jnp.where(mine, 2 * (number - (chunks + COMBINE_LAG)) + lax.rem(turn, 2), at)
            source = jnp.where(mine, outer, outer - (1 - 2 * way) * (full - at // chunks))
            limit = jnp.where(mine, chunks, full * chunks)
            live = (at >= 0) & (at < limit)
            pl.when(live)(lambda: combine(way, source, lax.rem(at, chunks)))
            return unused

        lax.fori_loop(0, 6, combine_way, 0)
        return unused

    last = chunks * (steps - 1) + SERVE_LAG + COMBINE_LAG + chunks
    lax.fori_loop(0, last, stage, 0)

    ahead = 2 * (2 * outer - (steps - 1))
    delays = (jnp.maximum(ahead, 0), jnp.maximum(-ahead, 0))

    def pass_sums(number, unused):
        for way in range(2):
            at = number - delays[way]
            turn = at // chunks
            chunk = lax.rem(at, chunks)
            dest = steps - 1 - turn if way == 0 else turn
            beyond = (dest > outer) if way == 0 else (dest < outer)
            live = (at >= 0) & (turn < steps - 1) & beyond & on_line(outer - (1 - 2 * way))

            def add(way=way, dest=dest, chunk=chunk):
                sum_copy(way, dest, chunk).wait_recv()
                given[dest, chunk] = (
                    given[dest, chunk].astype(jnp.float32)
                    + brought[dest, chunk].astype(jnp.float32)
                ).astype(jnp.bfloat16)
                sum_copy(way, dest, chunk).start()

            pl.when(live)(add)
        return unused

    lax.fori_loop(0, (steps - 1) * chunks + 2 * (steps - 1), pass_sums, 0)

    def gather(chunk):
        def from_way(way, unused):
            def add():
                sum_copy(way, outer, chunk).wait_recv()
                slot = jnp.where(way == 0, outer, steps)
                own_sum[chunk] += brought[slot, chunk].astype(jnp.float32)

            pl.when(on_line(outer - (1 - 2 * way)))(add)
            return unused

        lax.fori_loop(0, 2, from_way, 0)
        own_sum[chunk] += alpha_mix * x_ref[chunk].astype(jnp.float32)

    over_chunks(gather)
    features = chunks * width
    total = None
    for chunk in range(chunks):
        term = jnp.sum(own_sum[chunk], axis=1, keepdims=True)
        total = term if total is None else total + term
    center = total / features
    total = None
    for chunk in range(chunks):
        term = jnp.sum(jnp.square(own_sum[chunk] - center), axis=1, keepdims=True)
        total = term if total is None else total + term
    spread = lax.rsqrt(total / features + eps_norm)
    for chunk in range(chunks):
        part = slice(chunk * width, (chunk + 1) * width)
        o_ref[:, part] = (
            (own_sum[chunk] - center) * spread * gain_ref[:, part] + bias_ref[:, part]
        ).astype(o_ref.dtype)

    def settle(step, unused):
        def sent(way, source):
            def onward():
                for part in range(parts):
                    line_copy(way, step + 1, part).wait_send()

            pl.when(on_line(outer + 1 - 2 * way))(onward)

            def one(chunk):
                all_out(source, chunk).wait_send()
                all_back(source, chunk).wait_send()
                pl.when(step > 0)(lambda: sum_copy(1 - way, source, chunk).wait_send())

            over_chunks(one)

        def own_up(way, unused):
            pl.when((step == 0) & (way == 1) & on_line(outer - 1))(own_down)
            return unused

        def own_down():
            for part in range(parts):
                line_copy(1, 1, part).wait_send()

        over_ways(step, sent)
        own_up(1, 0)
        return unused

    lax.fori_loop(0, steps, settle, 0)


def run_experts(x, routes, route_weights, gate, up, down, gain, bias, sp_size, tp_size):
    pair = 2 if sp_size % 2 == 0 else 1
    steps, plane = sp_size // pair, pair * tp_size
    chunks, rows, width = x.shape
    top = routes.shape[1]
    hidden = gate.shape[2]
    spots = plane * (2 * rows * top // (sp_size * tp_size))
    bf16, f32, dma = jnp.bfloat16, jnp.float32, pltpu.SemaphoreType.DMA
    blocks = pltpu.VMEM((steps, chunks, plane, spots // plane, width), bf16)
    return pl.pallas_call(
        functools.partial(expert_kernel, steps, plane, tp_size),
        out_shape=jax.ShapeDtypeStruct((rows, chunks * width), bf16),
        in_specs=[VMEM] * 3 + [ANY] * 3 + [VMEM] * 2,
        out_specs=VMEM,
        scratch_shapes=[
            pltpu.VMEM((steps, chunks, rows, width), bf16),
            pltpu.VMEM((steps, top, rows), jnp.int32),
            pltpu.VMEM((steps, top, rows), f32),
            pltpu.VMEM((steps, top, rows), f32),
            blocks,
            blocks,
            blocks,
            blocks,
            pltpu.VMEM((steps, chunks, rows, width), bf16),
            pltpu.VMEM((steps + 1, chunks, rows, width), bf16),
            pltpu.VMEM((chunks, rows, width), f32),
            pltpu.VMEM((steps, spots, hidden), f32),
            pltpu.VMEM((steps, spots, hidden), f32),
            pltpu.VMEM((3, top, rows, spots), bf16),
            pltpu.VMEM((3, top, rows, HEAD), f32),
            pltpu.VMEM((chunks, width, hidden), gate.dtype),
            pltpu.VMEM((chunks, width, hidden), up.dtype),
            pltpu.VMEM(down.shape[1:], down.dtype),
            dma((2, steps + 1, chunks + 2)),
            dma((2, steps + 1, chunks + 2)),
            dma((steps, chunks)),
            dma((steps, chunks)),
            dma((steps, chunks)),
            dma((steps, chunks)),
            dma((2, steps, chunks)),
            dma((2, steps, chunks)),
            dma((6,)),
        ],
        compiler_params=pltpu.CompilerParams(
            collective_id=2, has_side_effects=True, vmem_limit_bytes=60 * 1024 * 1024
        ),
    )(
        x,
        routes.T,
        route_weights.T,
        gate.reshape(chunks, width, hidden),
        up.reshape(chunks, width, hidden),
        down.reshape(down.shape[1:]),
        gain[None, :],
        bias[None, :],
    )


def per_device(
    queries,
    key_heads,
    value_heads,
    documents,
    query_gain,
    key_gain,
    out_gain,
    out_proj,
    residual,
    mid_gain,
    mid_bias,
    routes,
    route_weights,
    expert_gate,
    expert_up,
    expert_down,
    final_gain,
    final_bias,
):
    sp_size = lax.axis_size("sp")
    tp_size = lax.axis_size("tp")
    if key_heads.shape[1] != HEAD or expert_gate.shape[0] != 1:
        raise ValueError("unsupported placement")
    middle = run_front(
        queries,
        key_heads,
        value_heads,
        documents,
        query_gain,
        key_gain,
        out_gain,
        out_proj,
        residual,
        mid_gain,
        mid_bias,
        sp_size,
        tp_size,
        CHUNKS,
    )
    return run_experts(
        middle,
        routes,
        route_weights,
        expert_gate,
        expert_up,
        expert_down,
        final_gain,
        final_bias,
        sp_size,
        tp_size,
    )


def solution(mesh):
    return jax.shard_map(
        per_device,
        mesh=mesh,
        in_specs=(
            P("sp", "tp"),
            P("sp", "tp"),
            P("sp", "tp"),
            P("sp"),
            P(),
            P(),
            P(),
            P(),
            P(("sp", "tp"), None),
            P(),
            P(),
            P(("sp", "tp"), None),
            P(("sp", "tp"), None),
            P(("sp", "tp"), None, None),
            P(("sp", "tp"), None, None),
            P(("sp", "tp"), None, None),
            P(),
            P(),
        ),
        out_specs=P(("sp", "tp"), None),
        check_vma=False,
    )
```

```python
import functools

import jax
import jax.numpy as jnp
from jax import lax
from jax.experimental import pallas as pl
from jax.experimental.pallas import tpu as pltpu
from jax.sharding import PartitionSpec as P

HEAD = 128
GRID = 64
CHUNKS = 4
SERVE_LAG = 3
COMBINE_LAG = 2
EDGE_SERVE_LAG = 2
EDGE_COMBINE_LAG = 2
PASS_LAG = 2
PASS_GAP = 2


eps_norm = 1e-06
alpha_mix = 8.0**0.25
theta_base = 10000.0
score_factor = HEAD ** (-0.5) * 1.4426950408889634
VMEM = pl.BlockSpec(memory_space=pltpu.VMEM)
ANY = pl.BlockSpec(memory_space=pl.ANY)
SMEM = pl.BlockSpec(memory_space=pltpu.SMEM)


def layer_norm(stream, gain_vec, bias_vec):
    center = jnp.mean(stream, axis=-1, keepdims=True)
    spread = jnp.mean(jnp.square(stream - center), axis=-1, keepdims=True)
    return (stream - center) * lax.rsqrt(spread + eps_norm) * gain_vec + bias_vec


def turned(values, gain, cosine, sine):
    inv_rms = lax.rsqrt(jnp.mean(values * values, axis=1, keepdims=True) + eps_norm)
    values = values * inv_rms * gain
    return (values * cosine + pltpu.roll(values, HEAD // 2, 1) * sine).astype(jnp.bfloat16)


def front_kernel(
    size,
    pair,
    tp_size,
    q_ref,
    k_ref,
    v_ref,
    doc_ref,
    q_gain_ref,
    k_gain_ref,
    freq_ref,
    gain_ref,
    proj_hbm,
    res_ref,
    mid_gain_ref,
    mid_bias_ref,
    mid_ref,
    kv,
    docs,
    qdoc_ref,
    row_ref,
    col_ref,
    q_rot,
    m_ref,
    l_ref,
    acc_ref,
    o_buf,
    whole,
    proj,
    line_send,
    line_recv,
    mate_send,
    mate_recv,
    tp_send,
    tp_recv,
    own_sem,
):
    me = lax.axis_index("sp")
    lane = lax.axis_index("tp")
    inner = lax.rem(me, pair)
    outer = me // pair
    steps = size // pair
    mate = outer * pair + lax.rem(inner + 1, pair)
    rows = k_ref.shape[0]
    pieces = doc_ref.shape[0]
    grouped = q_rot.shape[0]
    parts = 3

    load = pltpu.make_async_copy(proj_hbm, proj, own_sem.at[0])
    load.start()
    own = [
        pltpu.make_async_copy(v_ref, kv.at[me, 1], own_sem.at[1]),
        pltpu.make_async_copy(doc_ref, docs.at[me], own_sem.at[2]),
    ]
    for copy in own:
        copy.start()

    def on_line(place):
        return (place >= 0) & (place < steps)

    barrier = pltpu.get_barrier_semaphore()

    def greet(target):
        pl.semaphore_signal(
            barrier, inc=1, device_id=target, device_id_type=pl.DeviceIdType.MESH
        )

    peers = jnp.int32(tp_size - 1 + (pair - 1))
    for sign in (1, -1):
        there = on_line(outer + sign)
        pl.when(there)(lambda sign=sign: greet({"sp": (outer + sign) * pair + inner}))
        peers = peers + there.astype(jnp.int32)
    if pair == 2:
        greet({"sp": mate})
    tp_targets = [lax.rem(lane + step, tp_size) for step in range(1, tp_size)]
    for target in tp_targets:
        greet({"tp": target})
    pl.semaphore_wait(barrier, peers)

    def piece(place, part, first):
        if part == 2:
            return (doc_ref if first else docs.at[place]), docs.at[place]
        return (v_ref if first and part == 1 else kv.at[place, part]), kv.at[place, part]

    def line_copy(way, step, part, first=False):
        sign = 1 - 2 * way
        place = (outer - sign * (step - 1)) * pair + inner
        src, dst = piece(place, part, first)
        return pltpu.make_async_remote_copy(
            src_ref=src,
            dst_ref=dst,
            send_sem=line_send.at[way, step, part],
            recv_sem=line_recv.at[way, step, part],
            device_id={"sp": (outer + sign) * pair + inner},
            device_id_type=pl.DeviceIdType.MESH,
        )

    def mate_copy(way, step, part, first=False):
        sign = 1 - 2 * way
        place = (outer - sign * step) * pair + inner
        src, dst = piece(place, part, first)
        return pltpu.make_async_remote_copy(
            src_ref=src,
            dst_ref=dst,
            send_sem=mate_send.at[way, step, part],
            recv_sem=mate_recv.at[way, step, part],
            device_id={"sp": mate},
            device_id_type=pl.DeviceIdType.MESH,
        )

    def send_own(part):
        for way in range(2):
            pl.when(on_line(outer + 1 - 2 * way))(
                lambda way=way: line_copy(way, 1, part, True).start()
            )
        if pair == 2:
            mate_copy(0, 0, part, True).start()

    send_own(1)
    send_own(2)
    lanes = lax.broadcasted_iota(jnp.int32, (1, HEAD), 1)
    along = lax.rem(lanes, HEAD // 2) < HEAD // 4
    side = jnp.where(lanes < HEAD // 2, -1.0, 1.0)
    first_row = (me * (rows // GRID)).astype(jnp.float32)
    for table, start, mask in ((row_ref, first_row, along), (col_ref, 0.0, ~along)):
        numbers = lax.broadcasted_iota(jnp.int32, table.shape[1:], 0).astype(jnp.float32)
        angles = (numbers + start) * freq_ref[...]
        table[0] = jnp.where(mask, jnp.cos(angles), 0.0)
        table[1] = jnp.where(mask, jnp.sin(angles) * side, 0.0)
    grid_rows = row_ref.shape[1]
    span = col_ref.shape[1]

    def tables(block):
        cosine = row_ref[0, pl.ds(block, 1)] + col_ref[0]
        sine = row_ref[1, pl.ds(block, 1)] + col_ref[1]
        return cosine, sine

    def turn_keys(block, unused):
        cosine, sine = tables(block)
        here = pl.ds(pl.multiple_of(block * span, span), span)
        kv[me, 0, here] = turned(k_ref[here].astype(jnp.float32), k_gain_ref[...], cosine, sine)
        return unused

    lax.fori_loop(0, grid_rows, turn_keys, 0)
    send_own(0)

    def turn_queries(block, unused):
        cosine, sine = tables(block)
        here = pl.ds(pl.multiple_of(block * span, span), span)
        for head in range(grouped):
            q_rot[head, here] = turned(
                q_ref[here, head * HEAD : (head + 1) * HEAD].astype(jnp.float32),
                q_gain_ref[...],
                cosine,
                sine,
            )
        return unused

    lax.fori_loop(0, grid_rows, turn_queries, 0)
    down = lax.broadcasted_iota(jnp.int32, (HEAD, HEAD), 0)
    over = lax.broadcasted_iota(jnp.int32, (HEAD, HEAD), 1)
    for number in range(pieces):
        named = doc_ref[number : number + 1].astype(jnp.float32)
        column = jnp.sum(jnp.where(down == over, named, 0.0), axis=1, keepdims=True)
        qdoc_ref[number * HEAD : (number + 1) * HEAD] = jnp.broadcast_to(
            column, (HEAD, HEAD)
        ).astype(jnp.int32)
    m_ref[...] = jnp.full(m_ref.shape, -1e30, jnp.float32)
    l_ref[...] = jnp.zeros(l_ref.shape, jnp.float32)
    acc_ref[...] = jnp.zeros(acc_ref.shape, jnp.float32)
    for copy in own:
        copy.wait()
    chunk = 256

    def advance(place):
        keys = kv[place, 0]
        values = kv[place, 1]
        doc_rows = docs[place]
        key_docs = jnp.concatenate([doc_rows[i : i + 1] for i in range(pieces)], axis=1)
        for head in range(grouped):
            for first in range(0, rows, chunk):
                part = pl.ds(first, chunk)
                scores = lax.dot_general(
                    q_rot[head, part],
                    keys,
                    (((1,), (1,)), ((), ())),
                    preferred_element_type=jnp.float32,
                )
                allowed = qdoc_ref[part, 0:1] == key_docs
                scores = jnp.where(allowed, scores * score_factor, -1e30)
                old_max = m_ref[head, part]
                new_max = jnp.maximum(old_max, jnp.max(scores, axis=1, keepdims=True))
                base = jnp.maximum(new_max[:, 0:1], -1e29)
                weights = jnp.exp2(scores - base)
                rescale = jnp.exp2(old_max - new_max)
                l_ref[head, part] = l_ref[head, part] * rescale + jnp.sum(
                    weights, axis=1, keepdims=True
                )
                acc_ref[head, part] = acc_ref[head, part] * rescale + jnp.dot(
                    weights.astype(jnp.bfloat16), values, preferred_element_type=jnp.float32
                )
                m_ref[head, part] = new_max

    def receive(step):
        for group in ((1, 2), (0,)):
            for way in range(2):
                sign = 1 - 2 * way

                def take(way=way, sign=sign, group=group):
                    for part in group:
                        line_copy(way, step, part).wait_recv()

                    def pass_on():
                        for part in group:
                            line_copy(way, step + 1, part).start()

                    pl.when(on_line(outer + sign))(pass_on)
                    if pair == 2:
                        for part in group:
                            mate_copy(way, step, part).start()

                pl.when((step > 0) & on_line(outer - sign * step))(take)

    def stage(step, unused):
        def visit(number, unused):
            way = lax.rem(number, 2)
            across = number // 2
            there = outer - (1 - 2 * way) * step

            def work():
                if pair == 2:

                    def arrive():
                        for part in range(parts):
                            mate_copy(way, step, part).wait_recv()

                    pl.when(across == 1)(arrive)
                advance(there * pair + lax.rem(inner + across, pair))

            pl.when(on_line(there) & ((step > 0) | (way == 0)))(work)
            return unused

        lax.fori_loop(0, 2, visit, 0)
        pl.when(step + 1 < steps)(lambda: receive(step + 1))
        lax.fori_loop(2, 2 * pair, visit, 0)
        return unused

    lax.fori_loop(0, steps, stage, 0)
    for head in range(grouped):
        o_buf[:, head * HEAD : (head + 1) * HEAD] = (acc_ref[head] / l_ref[head]).astype(
            o_buf.dtype
        )

    out_rows, width = whole.shape[0], o_buf.shape[1]

    def rows_of(number):
        return pl.ds(pl.multiple_of(number * out_rows, out_rows), out_rows)

    mine = whole.at[:, pl.ds(pl.multiple_of(lane * width, width), width)]
    swaps = []
    for step, target in enumerate(tp_targets):
        copy = pltpu.make_async_remote_copy(
            src_ref=o_buf.at[rows_of(target)],
            dst_ref=mine,
            send_sem=tp_send.at[step],
            recv_sem=tp_recv.at[step],
            device_id={"tp": target},
            device_id_type=pl.DeviceIdType.MESH,
        )
        copy.start()
        swaps.append(copy)
    keep = pltpu.make_async_copy(o_buf.at[rows_of(lane)], mine, own_sem.at[3])
    keep.start()

    load.wait()
    for copy in swaps:
        copy.wait_recv()
    keep.wait()
    taken = whole[...].astype(jnp.float32)
    mean_square = jnp.mean(taken * taken, axis=1, keepdims=True)
    scaled = (taken * gain_ref[...]).astype(jnp.bfloat16)
    projected = jnp.dot(scaled, proj[...], preferred_element_type=jnp.float32)
    projected = projected * lax.rsqrt(mean_square + eps_norm)
    stream = alpha_mix * res_ref[...].astype(jnp.float32) + projected
    middle = layer_norm(stream, mid_gain_ref[...], mid_bias_ref[...]).astype(jnp.bfloat16)
    block = mid_ref.shape[2]
    for chunk in range(mid_ref.shape[0]):
        mid_ref[chunk] = middle[:, chunk * block : (chunk + 1) * block]

    for copy in swaps:
        copy.wait_send()

    def settle(step, unused):
        for way in range(2):
            sign = 1 - 2 * way

            def sent(way=way):
                for part in range(parts):
                    line_copy(way, step + 1, part).wait_send()

            pl.when(on_line(outer - sign * step) & on_line(outer + sign))(sent)
            if pair == 2:

                def gave(way=way):
                    for part in range(parts):
                        mate_copy(way, step, part).wait_send()

                first = (step > 0) | (way == 0)
                pl.when(on_line(outer - sign * step) & first)(gave)
        return unused

    lax.fori_loop(0, steps, settle, 0)


def run_front(
    queries,
    keys,
    values,
    documents,
    query_gain,
    key_gain,
    out_gain,
    out_proj,
    residual,
    mid_gain,
    mid_bias,
    size,
    tp_size,
    chunks,
):
    pair = 2 if size % 2 == 0 else 1
    rows, width = queries.shape
    grouped = width // HEAD
    out_rows, model_width = residual.shape
    steps = size // pair
    pair_count = HEAD // 4
    inv_freq = theta_base ** (-jnp.arange(pair_count, dtype=jnp.float32) / pair_count)
    dma = pltpu.SemaphoreType.DMA
    return pl.pallas_call(
        functools.partial(front_kernel, size, pair, tp_size),
        out_shape=jax.ShapeDtypeStruct((chunks, out_rows, model_width // chunks), jnp.bfloat16),
        in_specs=[VMEM] * 8 + [ANY] + [VMEM] * 3,
        out_specs=VMEM,
        scratch_shapes=[
            pltpu.VMEM((size, 2, rows, HEAD), jnp.bfloat16),
            pltpu.VMEM((size, rows // HEAD, HEAD), jnp.int32),
            pltpu.VMEM((rows, HEAD), jnp.int32),
            pltpu.VMEM((2, rows // GRID, HEAD), jnp.float32),
            pltpu.VMEM((2, GRID, HEAD), jnp.float32),
            pltpu.VMEM((grouped, rows, HEAD), jnp.bfloat16),
            pltpu.VMEM((grouped, rows, HEAD), jnp.float32),
            pltpu.VMEM((grouped, rows, HEAD), jnp.float32),
            pltpu.VMEM((grouped, rows, HEAD), jnp.float32),
            pltpu.VMEM((rows, width), jnp.bfloat16),
            pltpu.VMEM((out_rows, width * tp_size), jnp.bfloat16),
            pltpu.VMEM(out_proj.shape, out_proj.dtype),
            dma((2, steps + 1, 3)),
            dma((2, steps + 1, 3)),
            dma((2, steps, 3)),
            dma((2, steps, 3)),
            dma((tp_size,)),
            dma((tp_size,)),
            dma((4,)),
        ],
        compiler_params=pltpu.CompilerParams(
            collective_id=0, has_side_effects=True, vmem_limit_bytes=56 * 1024 * 1024
        ),
    )(
        queries,
        keys,
        values,
        documents.reshape(rows // HEAD, HEAD),
        query_gain[None, :],
        key_gain[None, :],
        jnp.tile(inv_freq, 4)[None, :],
        out_gain[None, :],
        out_proj,
        residual,
        mid_gain[None, :],
        mid_bias[None, :],
    )


def expert_kernel(
    steps,
    plane,
    tp_size,
    x_ref,
    route_ref,
    weight_ref,
    gate_hbm,
    up_hbm,
    down_hbm,
    gain_ref,
    bias_ref,
    o_ref,
    xs,
    routes,
    weights,
    slots,
    outb,
    held,
    served,
    back,
    given,
    brought,
    own_sum,
    gate_acc,
    up_acc,
    selects,
    picks,
    scales,
    gate_w,
    up_w,
    down_w,
    line_send,
    line_recv,
    out_send,
    out_recv,
    back_send,
    back_recv,
    sum_send,
    sum_recv,
    own_sem,
):
    me = lax.axis_index("sp") * tp_size + lax.axis_index("tp")
    outer = me // plane
    inner = lax.rem(me, plane)
    chunks, rows, width = x_ref.shape
    block = outb.shape[3]
    spots = plane * block
    top = route_ref.shape[0]
    parts = chunks + 2
    order = [chunks, chunks + 1] + list(range(chunks))

    loads = [
        pltpu.make_async_copy(x_ref, xs.at[outer], own_sem.at[0]),
        pltpu.make_async_copy(route_ref, routes.at[outer], own_sem.at[1]),
        pltpu.make_async_copy(weight_ref, weights.at[outer], own_sem.at[2]),
        pltpu.make_async_copy(gate_hbm, gate_w, own_sem.at[3]),
        pltpu.make_async_copy(up_hbm, up_w, own_sem.at[4]),
        pltpu.make_async_copy(down_hbm, down_w, own_sem.at[5]),
    ]
    for copy in loads:
        copy.start()

    def device(place, number):
        index = place * plane + number
        return {"sp": index // tp_size, "tp": lax.rem(index, tp_size)}

    def on_line(place):
        return (place >= 0) & (place < steps)

    barrier = pltpu.get_barrier_semaphore()

    def greet(place, number):
        pl.semaphore_signal(
            barrier,
            inc=1,
            device_id=device(place, number),
            device_id_type=pl.DeviceIdType.MESH,
        )

    peers = jnp.int32(plane - 1)
    for sign in (1, -1):
        there = on_line(outer + sign)
        pl.when(there)(lambda sign=sign: greet(outer + sign, inner))
        peers = peers + there.astype(jnp.int32)

    def greet_plane(step, unused):
        greet(outer, lax.rem(inner + step, plane))
        return unused

    lax.fori_loop(1, plane, greet_plane, 0)
    pl.semaphore_wait(barrier, peers)

    def piece(place, part, first):
        if part == chunks:
            return (route_ref if first else routes.at[place]), routes.at[place]
        if part == chunks + 1:
            return (weight_ref if first else weights.at[place]), weights.at[place]
        return (x_ref.at[part] if first else xs.at[place, part]), xs.at[place, part]

    def line_copy(way, step, part, first=False):
        sign = 1 - 2 * way
        place = outer - sign * (step - 1)
        src, dst = piece(place, part, first)
        return pltpu.make_async_remote_copy(
            src_ref=src,
            dst_ref=dst,
            send_sem=line_send.at[way, step, part],
            recv_sem=line_recv.at[way, step, part],
            device_id=device(outer + sign, inner),
            device_id_type=pl.DeviceIdType.MESH,
        )

    half = chunks // 2
    depth = (outer, steps - 1 - outer)

    def send_own(way, send):
        there = on_line(outer + 1 - 2 * way)
        for part in send:
            pl.when(there)(lambda part=part: line_copy(way, 1, part, True).start())

    for way in range(2):
        send_own(way, order[: 2 + half])
        pl.when(depth[way] == 0)(lambda way=way: send_own(way, order[2 + half :]))

    def out_copy(source, chunk, target):
        return pltpu.make_async_remote_copy(
            src_ref=outb.at[source, chunk, target],
            dst_ref=held.at[source, chunk, inner],
            send_sem=out_send.at[source, chunk],
            recv_sem=out_recv.at[source, chunk],
            device_id=device(outer, target),
            device_id_type=pl.DeviceIdType.MESH,
        )

    def back_copy(source, chunk, target):
        return pltpu.make_async_remote_copy(
            src_ref=served.at[source, chunk, target],
            dst_ref=back.at[source, chunk, inner],
            send_sem=back_send.at[source, chunk],
            recv_sem=back_recv.at[source, chunk],
            device_id=device(outer, target),
            device_id_type=pl.DeviceIdType.MESH,
        )

    def others(from_buffer, to_buffer, source, chunk, send_sem, recv_sem):
        return pltpu.make_async_remote_copy(
            src_ref=from_buffer.at[source, chunk, pl.ds(0, plane - 1)],
            dst_ref=to_buffer.at[source, chunk, pl.ds(0, plane - 1)],
            send_sem=send_sem.at[source, chunk],
            recv_sem=recv_sem.at[source, chunk],
            device_id=device(outer, inner),
            device_id_type=pl.DeviceIdType.MESH,
        )

    def all_out(source, chunk):
        return others(outb, held, source, chunk, out_send, out_recv)

    def all_back(source, chunk):
        return others(served, back, source, chunk, back_send, back_recv)

    def sum_copy(way, dest, chunk):
        target = outer + 1 - 2 * way
        slot = jnp.where((dest == target) & (way == 1), steps, dest)
        return pltpu.make_async_remote_copy(
            src_ref=given.at[dest, chunk],
            dst_ref=brought.at[slot, chunk],
            send_sem=sum_send.at[way, dest, chunk],
            recv_sem=sum_recv.at[way, dest, chunk],
            device_id=device(target, inner),
            device_id_type=pl.DeviceIdType.MESH,
        )

    def over_ways(step, act):
        def one(way, unused):
            source = outer - (1 - 2 * way) * step
            pl.when(on_line(source) & ((step > 0) | (way == 0)))(lambda: act(way, source))
            return unused

        lax.fori_loop(0, 2, one, 0)

    def over_chunks(act):
        def one(chunk, unused):
            act(chunk)
            return unused

        lax.fori_loop(0, chunks, one, 0)

    down_iota = lax.broadcasted_iota(jnp.int32, (rows, rows), 0)
    over_iota = lax.broadcasted_iota(jnp.int32, (rows, rows), 1)

    def place_rows(source):
        earlier = jnp.where(down_iota < over_iota, 1.0, 0.0).astype(jnp.bfloat16)
        names = outer * plane + lax.broadcasted_iota(jnp.int32, (plane, rows), 0)
        start = lax.broadcasted_iota(jnp.int32, (plane, rows), 0).astype(jnp.float32) * block
        passed = jnp.zeros((plane, 1), jnp.float32)
        for route in range(top):
            one_hot = jnp.where(names == routes[source, route : route + 1, :], 1.0, 0.0)
            before = passed + jnp.dot(
                one_hot.astype(jnp.bfloat16), earlier, preferred_element_type=jnp.float32
            )
            there = jnp.sum(one_hot, axis=0, keepdims=True)
            slot = jnp.sum((before + start) * one_hot, axis=0, keepdims=True)
            slots[source, route : route + 1, :] = slot + there - 1.0
            passed = passed + jnp.sum(one_hot, axis=1, keepdims=True)
        spot = lax.broadcasted_iota(jnp.int32, (spots, rows), 0).astype(jnp.float32)
        chosen = spot == slots[source, 0:1, :]
        for route in range(1, top):
            chosen = chosen | (spot == slots[source, route : route + 1, :])
        selects[source] = jnp.where(chosen, 1.0, 0.0).astype(jnp.bfloat16)

    def dispatch(source, chunk):
        pl.when(chunk == 0)(lambda: place_rows(source))
        picked = jnp.dot(selects[source], xs[source, chunk], preferred_element_type=jnp.float32)
        outb[source, chunk] = picked.astype(jnp.bfloat16).reshape(plane, block, width)
        held[source, chunk, inner] = outb[source, chunk, inner]

        def give(number, unused):
            out_copy(source, chunk, lax.rem(inner + number, plane)).start()
            return unused

        lax.fori_loop(1, plane, give, 0)

    def place_of(way, number, full):
        pairs = number // half
        out = pairs < full
        step = jnp.where(out, pairs + 1, 2 * full - pairs)
        chunk = jnp.where(out, 0, half) + lax.rem(number, half)
        return step, chunk, outer - (1 - 2 * way) * step

    def receive(way, number, full):
        step, chunk, source = place_of(way, number, full)

        def small():
            for part in order[:2]:
                wait_part(way, step, part)

        pl.when(chunk == 0)(small)
        line_dynamic(way, step, chunk).wait_recv()
        pl.when(on_line(outer + 1 - 2 * way))(
            lambda: line_dynamic(way, step + 1, chunk).start()
        )

    def wait_part(way, step, part):
        line_copy(way, step, part).wait_recv()
        pl.when(on_line(outer + 1 - 2 * way))(lambda: line_copy(way, step + 1, part).start())

    def line_dynamic(way, step, chunk):
        sign = 1 - 2 * way
        place = outer - sign * (step - 1)
        return pltpu.make_async_remote_copy(
            src_ref=xs.at[place, chunk],
            dst_ref=xs.at[place, chunk],
            send_sem=line_send.at[way, step, chunk],
            recv_sem=line_recv.at[way, step, chunk],
            device_id=device(outer + sign, inner),
            device_id_type=pl.DeviceIdType.MESH,
        )

    def serve(source, chunk):
        all_out(source, chunk).wait_recv()
        taken = held[source, chunk].reshape(spots, width)
        gate = jnp.dot(taken, gate_w[chunk], preferred_element_type=jnp.float32)
        up = jnp.dot(taken, up_w[chunk], preferred_element_type=jnp.float32)

        def fresh():
            gate_acc[source] = gate
            up_acc[source] = up

        def add():
            gate_acc[source] += gate
            up_acc[source] += up

        pl.when(chunk == 0)(fresh)
        pl.when(chunk > 0)(add)
        pl.when(chunk == chunks - 1)(lambda: finish(source))

    def finish(source):
        gate = gate_acc[source]
        hidden = (gate / (1.0 + jnp.exp(-gate)) * up_acc[source]).astype(jnp.bfloat16)
        for chunk in range(chunks):
            part = slice(chunk * width, (chunk + 1) * width)
            result = jnp.dot(hidden, down_w[:, part], preferred_element_type=jnp.float32)
            served[source, chunk] = result.astype(jnp.bfloat16).reshape(plane, block, width)
            back[source, chunk, inner] = served[source, chunk, inner]

            def give(number, unused, chunk=chunk):
                back_copy(source, chunk, lax.rem(inner + number, plane)).start()
                return unused

            lax.fori_loop(1, plane, give, 0)

    def column(row):
        return jnp.sum(jnp.where(down_iota == over_iota, row, 0.0), axis=1, keepdims=True)

    def combine(way, source, chunk):
        def prepare():
            spot = lax.broadcasted_iota(jnp.int32, (rows, spots), 1).astype(jnp.float32)
            for route in range(top):
                at = column(slots[source, route : route + 1, :])
                picks[way, route] = jnp.where(spot == at, 1.0, 0.0).astype(jnp.bfloat16)
                scale = column(weights[source, route : route + 1, :])
                scales[way, route] = jnp.broadcast_to(scale, scales.shape[2:])

        pl.when(chunk == 0)(prepare)
        all_back(source, chunk).wait_recv()
        came = back[source, chunk].reshape(spots, width)
        chosen = picks[way].reshape(top * rows, spots)
        picked = jnp.dot(chosen, came, preferred_element_type=jnp.float32)
        total = None
        for route in range(top):
            term = picked[route * rows : (route + 1) * rows] * scales[way, route][:, 0:1]
            total = term if total is None else total + term

        def keep():
            own_sum[chunk] = total

        def hand():
            given[source, chunk] = total.astype(jnp.bfloat16)
            pl.when(jnp.logical_not(on_line(outer - (1 - 2 * (1 - way)))))(
                lambda: sum_copy(1 - way, source, chunk).start()
            )

        pl.when(way == 2)(keep)
        pl.when(way < 2)(hand)

    ahead = 2 * (2 * outer - (steps - 1))
    delays = (jnp.maximum(ahead, 0), jnp.maximum(-ahead, 0))

    def pass_sums(number, unused):
        for way in range(2):
            at = number - delays[way]
            turn = at // chunks
            chunk = lax.rem(at, chunks)
            dest = steps - 1 - turn if way == 0 else turn
            beyond = (dest > outer) if way == 0 else (dest < outer)
            live = (at >= 0) & (turn < steps - 1) & beyond & on_line(outer - (1 - 2 * way))

            def add(way=way, dest=dest, chunk=chunk):
                sum_copy(way, dest, chunk).wait_recv()
                given[dest, chunk] = (
                    given[dest, chunk].astype(jnp.float32)
                    + brought[dest, chunk].astype(jnp.float32)
                ).astype(jnp.bfloat16)
                sum_copy(way, dest, chunk).start()

            pl.when(live)(add)
        return unused

    edge = (outer == 0) | (outer == steps - 1)
    serve_lag = jnp.where(edge, EDGE_SERVE_LAG, SERVE_LAG)
    combine_lag = jnp.where(edge, EDGE_COMBINE_LAG, COMBINE_LAG)
    for copy in loads[:3]:
        copy.wait()

    def first(chunk, unused):
        dispatch(outer, chunk)
        return unused

    lax.fori_loop(0, chunks, first, 0)

    def stage(number, unused):
        def load_weights():
            for copy in loads[3:]:
                copy.wait()

        def each_way(way, unused):
            full = jnp.where(way == 0, depth[0], depth[1])

            def take():
                receive(way, number, full)

                def rest():
                    for part in order[2 + half :]:
                        line_copy(way, 1, part, True).start()

                pl.when((number == full * chunks - 1) & on_line(outer + 1 - 2 * way))(rest)
                step, chunk, source = place_of(way, number, full)
                dispatch(source, chunk)

            pl.when(number < full * chunks)(take)
            return unused

        lax.fori_loop(0, 2, each_way, 0)
        pl.when(number == 0)(load_weights)

        def serve_way(way, unused):
            full = jnp.where(way == 0, depth[0], depth[1])
            at = number - serve_lag
            step, chunk, source = place_of(way, at, full)
            mine = way == 2
            source = jnp.where(mine, outer, source)
            chunk = jnp.where(mine, number, chunk)
            live = jnp.where(mine, number < chunks, (at >= 0) & (at < full * chunks))
            pl.when(live)(lambda: serve(source, chunk))
            return unused

        lax.fori_loop(0, 3, serve_way, 0)

        def combine_way(turn, unused):
            way = turn // 2
            full = jnp.where(way == 0, depth[0], depth[1])
            start = (full + 1) * half - 1 + serve_lag + combine_lag
            raw = 2 * (number - start) + lax.rem(turn, 2)
            later = raw - 2 * gap
            mine = way == 2
            at = jnp.where(raw < chunks, raw, later)
            at = jnp.where(mine, 2 * (number - (chunks + combine_lag)) + lax.rem(turn, 2), at)
            timely = mine | (raw < chunks) | (later >= chunks)
            source = jnp.where(mine, outer, outer - (1 - 2 * way) * (full - at // chunks))
            limit = jnp.where(mine, chunks, full * chunks)
            live = timely & (at >= 0) & (at < limit)
            pl.when(live)(lambda: combine(way, source, lax.rem(at, chunks)))
            return unused

        lax.fori_loop(0, 6, combine_way, 0)
        deep = jnp.maximum(depth[0], depth[1])
        opening = (deep + 1) * half - 1 + serve_lag + combine_lag + PASS_LAG

        def pass_one(turn, unused):
            def go():
                pass_sums(2 * (number - opening) + turn, 0)

            pl.when(number >= opening)(go)
            return unused

        lax.fori_loop(0, 2, pass_one, 0)
        return unused

    gap = jnp.where(edge, 0, PASS_GAP)
    most = max(SERVE_LAG + COMBINE_LAG, EDGE_SERVE_LAG + EDGE_COMBINE_LAG)
    last = chunks * (steps - 1) + most + chunks + PASS_LAG + half * (steps - 1)
    lax.fori_loop(0, last, stage, 0)

    def gather(chunk):
        def from_way(way, unused):
            def add():
                sum_copy(way, outer, chunk).wait_recv()
                slot = jnp.where(way == 0, outer, steps)
                own_sum[chunk] += brought[slot, chunk].astype(jnp.float32)

            pl.when(on_line(outer - (1 - 2 * way)))(add)
            return unused

        lax.fori_loop(0, 2, from_way, 0)
        own_sum[chunk] += alpha_mix * x_ref[chunk].astype(jnp.float32)

    over_chunks(gather)
    features = chunks * width
    total = None
    for chunk in range(chunks):
        term = jnp.sum(own_sum[chunk], axis=1, keepdims=True)
        total = term if total is None else total + term
    center = total / features
    total = None
    for chunk in range(chunks):
        term = jnp.sum(jnp.square(own_sum[chunk] - center), axis=1, keepdims=True)
        total = term if total is None else total + term
    spread = lax.rsqrt(total / features + eps_norm)
    for chunk in range(chunks):
        part = slice(chunk * width, (chunk + 1) * width)
        o_ref[:, part] = (
            (own_sum[chunk] - center) * spread * gain_ref[:, part] + bias_ref[:, part]
        ).astype(o_ref.dtype)

    def settle(step, unused):
        def sent(way, source):
            def onward():
                for part in range(parts):
                    line_copy(way, step + 1, part).wait_send()

            pl.when(on_line(outer + 1 - 2 * way))(onward)

            def one(chunk):
                all_out(source, chunk).wait_send()
                all_back(source, chunk).wait_send()
                pl.when(step > 0)(lambda: sum_copy(1 - way, source, chunk).wait_send())

            over_chunks(one)

        def own_up(way, unused):
            pl.when((step == 0) & (way == 1) & on_line(outer - 1))(own_down)
            return unused

        def own_down():
            for part in range(parts):
                line_copy(1, 1, part).wait_send()

        over_ways(step, sent)
        own_up(1, 0)
        return unused

    lax.fori_loop(0, steps, settle, 0)


def run_experts(x, routes, route_weights, gate, up, down, gain, bias, sp_size, tp_size):
    pair = 2 if sp_size % 2 == 0 else 1
    steps, plane = sp_size // pair, pair * tp_size
    chunks, rows, width = x.shape
    top = routes.shape[1]
    hidden = gate.shape[2]
    spots = plane * (2 * rows * top // (sp_size * tp_size))
    bf16, f32, dma = jnp.bfloat16, jnp.float32, pltpu.SemaphoreType.DMA
    blocks = pltpu.VMEM((steps, chunks, plane, spots // plane, width), bf16)
    return pl.pallas_call(
        functools.partial(expert_kernel, steps, plane, tp_size),
        out_shape=jax.ShapeDtypeStruct((rows, chunks * width), bf16),
        in_specs=[VMEM] * 3 + [ANY] * 3 + [VMEM] * 2,
        out_specs=VMEM,
        scratch_shapes=[
            pltpu.VMEM((steps, chunks, rows, width), bf16),
            pltpu.VMEM((steps, top, rows), jnp.int32),
            pltpu.VMEM((steps, top, rows), f32),
            pltpu.VMEM((steps, top, rows), f32),
            blocks,
            blocks,
            blocks,
            blocks,
            pltpu.VMEM((steps, chunks, rows, width), bf16),
            pltpu.VMEM((steps + 1, chunks, rows, width), bf16),
            pltpu.VMEM((chunks, rows, width), f32),
            pltpu.VMEM((steps, spots, hidden), f32),
            pltpu.VMEM((steps, spots, hidden), f32),
            pltpu.VMEM((steps, spots, rows), bf16),
            pltpu.VMEM((3, top, rows, spots), bf16),
            pltpu.VMEM((3, top, rows, HEAD), f32),
            pltpu.VMEM((chunks, width, hidden), gate.dtype),
            pltpu.VMEM((chunks, width, hidden), up.dtype),
            pltpu.VMEM(down.shape[1:], down.dtype),
            dma((2, steps + 1, chunks + 2)),
            dma((2, steps + 1, chunks + 2)),
            dma((steps, chunks)),
            dma((steps, chunks)),
            dma((steps, chunks)),
            dma((steps, chunks)),
            dma((2, steps, chunks)),
            dma((2, steps, chunks)),
            dma((6,)),
        ],
        compiler_params=pltpu.CompilerParams(
            collective_id=2, has_side_effects=True, vmem_limit_bytes=60 * 1024 * 1024
        ),
    )(
        x,
        routes.T,
        route_weights.T,
        gate.reshape(chunks, width, hidden),
        up.reshape(chunks, width, hidden),
        down.reshape(down.shape[1:]),
        gain[None, :],
        bias[None, :],
    )


def per_device(
    queries,
    key_heads,
    value_heads,
    documents,
    query_gain,
    key_gain,
    out_gain,
    out_proj,
    residual,
    mid_gain,
    mid_bias,
    routes,
    route_weights,
    expert_gate,
    expert_up,
    expert_down,
    final_gain,
    final_bias,
):
    sp_size = lax.axis_size("sp")
    tp_size = lax.axis_size("tp")
    if key_heads.shape[1] != HEAD or expert_gate.shape[0] != 1:
        raise ValueError("unsupported placement")
    middle = run_front(
        queries,
        key_heads,
        value_heads,
        documents,
        query_gain,
        key_gain,
        out_gain,
        out_proj,
        residual,
        mid_gain,
        mid_bias,
        sp_size,
        tp_size,
        CHUNKS,
    )
    return run_experts(
        middle,
        routes,
        route_weights,
        expert_gate,
        expert_up,
        expert_down,
        final_gain,
        final_bias,
        sp_size,
        tp_size,
    )


def solution(mesh):
    return jax.shard_map(
        per_device,
        mesh=mesh,
        in_specs=(
            P("sp", "tp"),
            P("sp", "tp"),
            P("sp", "tp"),
            P("sp"),
            P(),
            P(),
            P(),
            P(),
            P(("sp", "tp"), None),
            P(),
            P(),
            P(("sp", "tp"), None),
            P(("sp", "tp"), None),
            P(("sp", "tp"), None, None),
            P(("sp", "tp"), None, None),
            P(("sp", "tp"), None, None),
            P(),
            P(),
        ),
        out_specs=P(("sp", "tp"), None),
        check_vma=False,
    )
```

```python
import functools

import jax
import jax.numpy as jnp
import numpy as np
from jax import lax
from jax.experimental import pallas as pl
from jax.experimental.pallas import tpu as pltpu
from jax.sharding import PartitionSpec as P

HEAD = 128
GRID = 64
LONGEST = (5, 8)
CHUNKS = 4
SERVE_LAG = 4
COMBINE_LAG = 2
EDGE_SERVE_LAG = 2
EDGE_COMBINE_LAG = 1
PASS_LAG = 2
PASS_GAP = 2


eps_norm = 1e-06
alpha_mix = 8.0**0.25
theta_base = 10000.0
score_factor = HEAD ** (-0.5) * 1.4426950408889634
VMEM = pl.BlockSpec(memory_space=pltpu.VMEM)
ANY = pl.BlockSpec(memory_space=pl.ANY)
SMEM = pl.BlockSpec(memory_space=pltpu.SMEM)


def layer_norm(stream, gain_vec, bias_vec):
    center = jnp.mean(stream, axis=-1, keepdims=True)
    spread = jnp.mean(jnp.square(stream - center), axis=-1, keepdims=True)
    return (stream - center) * lax.rsqrt(spread + eps_norm) * gain_vec + bias_vec


def turned(values, gain, cosine, sine):
    inv_rms = lax.rsqrt(jnp.mean(values * values, axis=1, keepdims=True) + eps_norm)
    values = values * inv_rms * gain
    return (values * cosine + pltpu.roll(values, HEAD // 2, 1) * sine).astype(jnp.bfloat16)


def front_kernel(
    size,
    pair,
    tp_size,
    q_ref,
    k_ref,
    v_ref,
    doc_ref,
    q_gain_ref,
    k_gain_ref,
    freq_ref,
    gain_ref,
    proj_hbm,
    res_ref,
    mid_gain_ref,
    mid_bias_ref,
    mid_ref,
    kv,
    docs,
    qdoc_ref,
    row_ref,
    col_ref,
    q_rot,
    m_ref,
    l_ref,
    acc_ref,
    o_buf,
    whole,
    proj,
    line_send,
    line_recv,
    mate_send,
    mate_recv,
    tp_send,
    tp_recv,
    own_sem,
):
    me = lax.axis_index("sp")
    lane = lax.axis_index("tp")
    inner = lax.rem(me, pair)
    outer = me // pair
    steps = size // pair
    mate = outer * pair + lax.rem(inner + 1, pair)
    rows = k_ref.shape[0]
    pieces = doc_ref.shape[0]
    grouped = q_rot.shape[0] // rows
    parts = 3

    load = pltpu.make_async_copy(proj_hbm, proj, own_sem.at[0])
    load.start()
    own = [
        pltpu.make_async_copy(v_ref, kv.at[me, 1], own_sem.at[1]),
        pltpu.make_async_copy(doc_ref, docs.at[me], own_sem.at[2]),
    ]
    for copy in own:
        copy.start()

    def on_line(place):
        return (place >= 0) & (place < steps)

    barrier = pltpu.get_barrier_semaphore()

    def greet(target):
        pl.semaphore_signal(
            barrier, inc=1, device_id=target, device_id_type=pl.DeviceIdType.MESH
        )

    peers = jnp.int32(tp_size - 1 + (pair - 1))
    for sign in (1, -1):
        there = on_line(outer + sign)
        pl.when(there)(lambda sign=sign: greet({"sp": (outer + sign) * pair + inner}))
        peers = peers + there.astype(jnp.int32)
    if pair == 2:
        greet({"sp": mate})
    tp_targets = [lax.rem(lane + step, tp_size) for step in range(1, tp_size)]
    for target in tp_targets:
        greet({"tp": target})

    def piece(place, part, first):
        if part == 2:
            return (doc_ref if first else docs.at[place]), docs.at[place]
        return (v_ref if first and part == 1 else kv.at[place, part]), kv.at[place, part]

    def line_copy(way, step, part, first=False):
        sign = 1 - 2 * way
        place = (outer - sign * (step - 1)) * pair + inner
        src, dst = piece(place, part, first)
        return pltpu.make_async_remote_copy(
            src_ref=src,
            dst_ref=dst,
            send_sem=line_send.at[way, step, part],
            recv_sem=line_recv.at[way, step, part],
            device_id={"sp": (outer + sign) * pair + inner},
            device_id_type=pl.DeviceIdType.MESH,
        )

    def mate_copy(way, step, part, first=False):
        sign = 1 - 2 * way
        place = (outer - sign * step) * pair + inner
        src, dst = piece(place, part, first)
        return pltpu.make_async_remote_copy(
            src_ref=src,
            dst_ref=dst,
            send_sem=mate_send.at[way, step, part],
            recv_sem=mate_recv.at[way, step, part],
            device_id={"sp": mate},
            device_id_type=pl.DeviceIdType.MESH,
        )

    def send_own(part):
        for way in range(2):
            pl.when(on_line(outer + 1 - 2 * way))(
                lambda way=way: line_copy(way, 1, part, True).start()
            )
        if pair == 2:
            mate_copy(0, 0, part, True).start()

    lanes = lax.broadcasted_iota(jnp.int32, (1, HEAD), 1)
    along = lax.rem(lanes, HEAD // 2) < HEAD // 4
    side = jnp.where(lanes < HEAD // 2, -1.0, 1.0)
    first_row = (me * (rows // GRID)).astype(jnp.float32)
    for table, start, mask in ((row_ref, first_row, along), (col_ref, 0.0, ~along)):
        numbers = lax.broadcasted_iota(jnp.int32, table.shape[1:], 0).astype(jnp.float32)
        angles = (numbers + start) * freq_ref[...]
        table[0] = jnp.where(mask, jnp.cos(angles), 0.0)
        table[1] = jnp.where(mask, jnp.sin(angles) * side, 0.0)
    grid_rows = row_ref.shape[1]
    span = col_ref.shape[1]

    def tables(block):
        cosine = row_ref[0, pl.ds(block, 1)] + col_ref[0]
        sine = row_ref[1, pl.ds(block, 1)] + col_ref[1]
        return cosine, sine

    def turn_keys(block, unused):
        cosine, sine = tables(block)
        here = pl.ds(pl.multiple_of(block * span, span), span)
        kv[me, 0, here] = turned(k_ref[here].astype(jnp.float32), k_gain_ref[...], cosine, sine)
        return unused

    lax.fori_loop(0, grid_rows, turn_keys, 0)
    pl.semaphore_wait(barrier, peers)
    for part in (1, 2, 0):
        send_own(part)

    def turn_queries(block, unused):
        cosine, sine = tables(block)
        here = pl.ds(pl.multiple_of(block * span, span), span)
        for head in range(grouped):
            there = pl.ds(pl.multiple_of(head * rows + block * span, span), span)
            q_rot[there] = turned(
                q_ref[here, head * HEAD : (head + 1) * HEAD].astype(jnp.float32),
                q_gain_ref[...],
                cosine,
                sine,
            )
        return unused

    lax.fori_loop(0, grid_rows, turn_queries, 0)
    down = lax.broadcasted_iota(jnp.int32, (HEAD, HEAD), 0)
    over = lax.broadcasted_iota(jnp.int32, (HEAD, HEAD), 1)
    for number in range(pieces):
        named = doc_ref[number : number + 1].astype(jnp.float32)
        column = jnp.sum(jnp.where(down == over, named, 0.0), axis=1, keepdims=True)
        column = jnp.broadcast_to(column, (HEAD, HEAD)).astype(jnp.int32)
        for head in range(grouped):
            qdoc_ref[pl.ds(head * rows + number * HEAD, HEAD)] = column
    m_ref[...] = jnp.full(m_ref.shape, -1e30, jnp.float32)
    l_ref[...] = jnp.zeros(l_ref.shape, jnp.float32)
    acc_ref[...] = jnp.zeros(acc_ref.shape, jnp.float32)
    for copy in own:
        copy.wait()

    def advance(place):
        keys = kv[place, 0]
        values = kv[place, 1]
        doc_rows = docs[place]
        key_docs = jnp.concatenate([doc_rows[i : i + 1] for i in range(pieces)], axis=1)
        scores = lax.dot_general(
            q_rot[...], keys, (((1,), (1,)), ((), ())), preferred_element_type=jnp.float32
        )
        allowed = qdoc_ref[:, 0:1] == key_docs
        scores = jnp.where(allowed, scores * score_factor, -1e30)
        old_max = m_ref[...]
        new_max = jnp.maximum(old_max, jnp.max(scores, axis=1, keepdims=True))
        base = jnp.maximum(new_max[:, 0:1], -1e29)
        weights = jnp.exp2(scores - base)
        rescale = jnp.exp2(old_max - new_max)
        l_ref[...] = l_ref[...] * rescale + jnp.sum(weights, axis=1, keepdims=True)
        acc_ref[...] = acc_ref[...] * rescale + jnp.dot(
            weights.astype(jnp.bfloat16), values, preferred_element_type=jnp.float32
        )
        m_ref[...] = new_max

    reach = (size * rows * LONGEST[0] // LONGEST[1] - 2) // rows + 1

    def receive(step):
        for group in ((1, 2), (0,)):
            for way in range(2):
                sign = 1 - 2 * way

                def take(way=way, sign=sign, group=group):
                    for part in group:
                        line_copy(way, step, part).wait_recv()

                    def pass_on():
                        for part in group:
                            line_copy(way, step + 1, part).start()

                    pl.when(on_line(outer + sign))(pass_on)
                    if pair == 2:
                        for part in group:
                            mate_copy(way, step, part).start()

                pl.when((step > 0) & on_line(outer - sign * step))(take)

    def stage(step, unused):
        def visit(number, unused):
            way = lax.rem(number, 2)
            across = number // 2
            there = outer - (1 - 2 * way) * step

            def work():
                if pair == 2:

                    def arrive():
                        for part in range(parts):
                            mate_copy(way, step, part).wait_recv()

                    pl.when(across == 1)(arrive)
                block = there * pair + lax.rem(inner + across, pair)
                close = (block - me <= reach) & (me - block <= reach)
                pl.when(close)(lambda: advance(block))

            pl.when(on_line(there) & ((step > 0) | (way == 0)))(work)
            return unused

        lax.fori_loop(0, 2, visit, 0)
        pl.when(step + 1 < steps)(lambda: receive(step + 1))
        lax.fori_loop(2, 2 * pair, visit, 0)
        return unused

    lax.fori_loop(0, steps, stage, 0)
    for head in range(grouped):
        o_buf[:, head * HEAD : (head + 1) * HEAD] = (
            acc_ref[head * rows : (head + 1) * rows] / l_ref[head * rows : (head + 1) * rows]
        ).astype(
            o_buf.dtype
        )

    out_rows, width = whole.shape[0], o_buf.shape[1]

    def rows_of(number):
        return pl.ds(pl.multiple_of(number * out_rows, out_rows), out_rows)

    mine = whole.at[:, pl.ds(pl.multiple_of(lane * width, width), width)]
    swaps = []
    for step, target in enumerate(tp_targets):
        copy = pltpu.make_async_remote_copy(
            src_ref=o_buf.at[rows_of(target)],
            dst_ref=mine,
            send_sem=tp_send.at[step],
            recv_sem=tp_recv.at[step],
            device_id={"tp": target},
            device_id_type=pl.DeviceIdType.MESH,
        )
        copy.start()
        swaps.append(copy)
    keep = pltpu.make_async_copy(o_buf.at[rows_of(lane)], mine, own_sem.at[3])
    keep.start()

    load.wait()
    for copy in swaps:
        copy.wait_recv()
    keep.wait()
    taken = whole[...].astype(jnp.float32)
    mean_square = jnp.mean(taken * taken, axis=1, keepdims=True)
    scaled = (taken * gain_ref[...]).astype(jnp.bfloat16)
    projected = jnp.dot(scaled, proj[...], preferred_element_type=jnp.float32)
    projected = projected * lax.rsqrt(mean_square + eps_norm)
    stream = alpha_mix * res_ref[...].astype(jnp.float32) + projected
    middle = layer_norm(stream, mid_gain_ref[...], mid_bias_ref[...]).astype(jnp.bfloat16)
    block = mid_ref.shape[2]
    for chunk in range(mid_ref.shape[0]):
        mid_ref[chunk] = middle[:, chunk * block : (chunk + 1) * block]

    for copy in swaps:
        copy.wait_send()

    def settle(step, unused):
        for way in range(2):
            sign = 1 - 2 * way

            def sent(way=way):
                for part in range(parts):
                    line_copy(way, step + 1, part).wait_send()

            pl.when(on_line(outer - sign * step) & on_line(outer + sign))(sent)
            if pair == 2:

                def gave(way=way):
                    for part in range(parts):
                        mate_copy(way, step, part).wait_send()

                first = (step > 0) | (way == 0)
                pl.when(on_line(outer - sign * step) & first)(gave)
        return unused

    lax.fori_loop(0, steps, settle, 0)


def run_front(
    queries,
    keys,
    values,
    documents,
    query_gain,
    key_gain,
    out_gain,
    out_proj,
    residual,
    mid_gain,
    mid_bias,
    size,
    tp_size,
    chunks,
):
    pair = 2 if size % 2 == 0 else 1
    rows, width = queries.shape
    grouped = width // HEAD
    out_rows, model_width = residual.shape
    steps = size // pair
    pair_count = HEAD // 4
    inv_freq = theta_base ** (-np.arange(pair_count, dtype=np.float32) / pair_count)
    dma = pltpu.SemaphoreType.DMA
    return pl.pallas_call(
        functools.partial(front_kernel, size, pair, tp_size),
        out_shape=jax.ShapeDtypeStruct((chunks, out_rows, model_width // chunks), jnp.bfloat16),
        in_specs=[VMEM] * 8 + [ANY] + [VMEM] * 3,
        out_specs=VMEM,
        scratch_shapes=[
            pltpu.VMEM((size, 2, rows, HEAD), jnp.bfloat16),
            pltpu.VMEM((size, rows // HEAD, HEAD), jnp.int32),
            pltpu.VMEM((grouped * rows, HEAD), jnp.int32),
            pltpu.VMEM((2, rows // GRID, HEAD), jnp.float32),
            pltpu.VMEM((2, GRID, HEAD), jnp.float32),
            pltpu.VMEM((grouped * rows, HEAD), jnp.bfloat16),
            pltpu.VMEM((grouped * rows, HEAD), jnp.float32),
            pltpu.VMEM((grouped * rows, HEAD), jnp.float32),
            pltpu.VMEM((grouped * rows, HEAD), jnp.float32),
            pltpu.VMEM((rows, width), jnp.bfloat16),
            pltpu.VMEM((out_rows, width * tp_size), jnp.bfloat16),
            pltpu.VMEM(out_proj.shape, out_proj.dtype),
            dma((2, steps + 1, 3)),
            dma((2, steps + 1, 3)),
            dma((2, steps, 3)),
            dma((2, steps, 3)),
            dma((tp_size,)),
            dma((tp_size,)),
            dma((4,)),
        ],
        compiler_params=pltpu.CompilerParams(
            collective_id=0, has_side_effects=True, vmem_limit_bytes=56 * 1024 * 1024
        ),
    )(
        queries,
        keys,
        values,
        documents.reshape(rows // HEAD, HEAD),
        query_gain[None, :],
        key_gain[None, :],
        np.tile(inv_freq.astype(np.float32), 4)[None, :],
        out_gain[None, :],
        out_proj,
        residual,
        mid_gain[None, :],
        mid_bias[None, :],
    )


def expert_kernel(
    steps,
    plane,
    tp_size,
    x_ref,
    route_ref,
    weight_ref,
    gate_hbm,
    up_hbm,
    down_hbm,
    gain_ref,
    bias_ref,
    o_ref,
    xs,
    routes,
    weights,
    slots,
    outb,
    held,
    served,
    back,
    given,
    brought,
    own_sum,
    gate_acc,
    up_acc,
    selects,
    picks,
    scales,
    gate_w,
    up_w,
    down_w,
    line_send,
    line_recv,
    out_send,
    out_recv,
    back_send,
    back_recv,
    sum_send,
    sum_recv,
    own_sem,
):
    me = lax.axis_index("sp") * tp_size + lax.axis_index("tp")
    outer = me // plane
    inner = lax.rem(me, plane)
    chunks, rows, width = x_ref.shape
    block = outb.shape[3]
    spots = plane * block
    top = route_ref.shape[0]
    parts = chunks + 2
    order = [chunks, chunks + 1] + list(range(chunks))

    loads = [
        pltpu.make_async_copy(x_ref, xs.at[outer], own_sem.at[0]),
        pltpu.make_async_copy(route_ref, routes.at[outer], own_sem.at[1]),
        pltpu.make_async_copy(weight_ref, weights.at[outer], own_sem.at[2]),
        pltpu.make_async_copy(gate_hbm, gate_w, own_sem.at[3]),
        pltpu.make_async_copy(up_hbm, up_w, own_sem.at[4]),
        pltpu.make_async_copy(down_hbm, down_w, own_sem.at[5]),
    ]
    for copy in loads:
        copy.start()

    def device(place, number):
        index = place * plane + number
        return {"sp": index // tp_size, "tp": lax.rem(index, tp_size)}

    def on_line(place):
        return (place >= 0) & (place < steps)

    barrier = pltpu.get_barrier_semaphore()

    def greet(place, number):
        pl.semaphore_signal(
            barrier,
            inc=1,
            device_id=device(place, number),
            device_id_type=pl.DeviceIdType.MESH,
        )

    peers = jnp.int32(plane - 1)
    for sign in (1, -1):
        there = on_line(outer + sign)
        pl.when(there)(lambda sign=sign: greet(outer + sign, inner))
        peers = peers + there.astype(jnp.int32)

    def greet_plane(step, unused):
        greet(outer, lax.rem(inner + step, plane))
        return unused

    lax.fori_loop(1, plane, greet_plane, 0)

    def piece(place, part, first):
        if part == chunks:
            return (route_ref if first else routes.at[place]), routes.at[place]
        if part == chunks + 1:
            return (weight_ref if first else weights.at[place]), weights.at[place]
        return (x_ref.at[part] if first else xs.at[place, part]), xs.at[place, part]

    def line_copy(way, step, part, first=False):
        sign = 1 - 2 * way
        place = outer - sign * (step - 1)
        src, dst = piece(place, part, first)
        return pltpu.make_async_remote_copy(
            src_ref=src,
            dst_ref=dst,
            send_sem=line_send.at[way, step, part],
            recv_sem=line_recv.at[way, step, part],
            device_id=device(outer + sign, inner),
            device_id_type=pl.DeviceIdType.MESH,
        )

    half = chunks // 2
    depth = (outer, steps - 1 - outer)

    def send_own(way, send):
        there = on_line(outer + 1 - 2 * way)
        for part in send:
            pl.when(there)(lambda part=part: line_copy(way, 1, part, True).start())

    def out_copy(source, chunk, target):
        return pltpu.make_async_remote_copy(
            src_ref=outb.at[source, chunk, target],
            dst_ref=held.at[source, chunk, inner],
            send_sem=out_send.at[source, chunk],
            recv_sem=out_recv.at[source, chunk],
            device_id=device(outer, target),
            device_id_type=pl.DeviceIdType.MESH,
        )

    def back_copy(source, chunk, target):
        return pltpu.make_async_remote_copy(
            src_ref=served.at[source, chunk, target],
            dst_ref=back.at[source, chunk, inner],
            send_sem=back_send.at[source, chunk],
            recv_sem=back_recv.at[source, chunk],
            device_id=device(outer, target),
            device_id_type=pl.DeviceIdType.MESH,
        )

    def others(from_buffer, to_buffer, source, chunk, send_sem, recv_sem):
        return pltpu.make_async_remote_copy(
            src_ref=from_buffer.at[source, chunk, pl.ds(0, plane - 1)],
            dst_ref=to_buffer.at[source, chunk, pl.ds(0, plane - 1)],
            send_sem=send_sem.at[source, chunk],
            recv_sem=recv_sem.at[source, chunk],
            device_id=device(outer, inner),
            device_id_type=pl.DeviceIdType.MESH,
        )

    def all_out(source, chunk):
        return others(outb, held, source, chunk, out_send, out_recv)

    def all_back(source, chunk):
        return others(served, back, source, chunk, back_send, back_recv)

    def sum_copy(way, dest, chunk):
        target = outer + 1 - 2 * way
        slot = jnp.where((dest == target) & (way == 1), steps, dest)
        return pltpu.make_async_remote_copy(
            src_ref=given.at[dest, chunk],
            dst_ref=brought.at[slot, chunk],
            send_sem=sum_send.at[way, dest, chunk],
            recv_sem=sum_recv.at[way, dest, chunk],
            device_id=device(target, inner),
            device_id_type=pl.DeviceIdType.MESH,
        )

    def over_ways(step, act):
        def one(way, unused):
            source = outer - (1 - 2 * way) * step
            pl.when(on_line(source) & ((step > 0) | (way == 0)))(lambda: act(way, source))
            return unused

        lax.fori_loop(0, 2, one, 0)

    def over_chunks(act):
        def one(chunk, unused):
            act(chunk)
            return unused

        lax.fori_loop(0, chunks, one, 0)

    down_iota = lax.broadcasted_iota(jnp.int32, (rows, rows), 0)
    over_iota = lax.broadcasted_iota(jnp.int32, (rows, rows), 1)

    def place_rows(source):
        earlier = jnp.where(down_iota < over_iota, 1.0, 0.0).astype(jnp.bfloat16)
        names = outer * plane + lax.broadcasted_iota(jnp.int32, (plane, rows), 0)
        start = lax.broadcasted_iota(jnp.int32, (plane, rows), 0).astype(jnp.float32) * block
        passed = jnp.zeros((plane, 1), jnp.float32)
        for route in range(top):
            one_hot = jnp.where(names == routes[source, route : route + 1, :], 1.0, 0.0)
            before = passed + jnp.dot(
                one_hot.astype(jnp.bfloat16), earlier, preferred_element_type=jnp.float32
            )
            there = jnp.sum(one_hot, axis=0, keepdims=True)
            slot = jnp.sum((before + start) * one_hot, axis=0, keepdims=True)
            slots[source, route : route + 1, :] = slot + there - 1.0
            passed = passed + jnp.sum(one_hot, axis=1, keepdims=True)
        spot = lax.broadcasted_iota(jnp.int32, (spots, rows), 0).astype(jnp.float32)
        chosen = spot == slots[source, 0:1, :]
        for route in range(1, top):
            chosen = chosen | (spot == slots[source, route : route + 1, :])
        selects[source] = jnp.where(chosen, 1.0, 0.0).astype(jnp.bfloat16)

    def dispatch(source, chunk):
        pl.when(chunk == 0)(lambda: place_rows(source))
        choose(source, chunk)
        hand_out(source, chunk)

    def choose(source, chunk):
        picked = jnp.dot(selects[source], xs[source, chunk], preferred_element_type=jnp.float32)
        outb[source, chunk] = picked.astype(jnp.bfloat16).reshape(plane, block, width)
        held[source, chunk, inner] = outb[source, chunk, inner]

    def hand_out(source, chunk):
        def give(number, unused):
            out_copy(source, chunk, lax.rem(inner + number, plane)).start()
            return unused

        lax.fori_loop(1, plane, give, 0)

    def place_of(way, number, full):
        pairs = number // half
        out = pairs < full
        step = jnp.where(out, pairs + 1, 2 * full - pairs)
        chunk = jnp.where(out, 0, half) + lax.rem(number, half)
        return step, chunk, outer - (1 - 2 * way) * step

    def receive(way, number, full):
        step, chunk, source = place_of(way, number, full)

        def small():
            for part in order[:2]:
                wait_part(way, step, part)

        pl.when(chunk == 0)(small)
        line_dynamic(way, step, chunk).wait_recv()
        pl.when(on_line(outer + 1 - 2 * way))(
            lambda: line_dynamic(way, step + 1, chunk).start()
        )

    def wait_part(way, step, part):
        line_copy(way, step, part).wait_recv()
        pl.when(on_line(outer + 1 - 2 * way))(lambda: line_copy(way, step + 1, part).start())

    def line_dynamic(way, step, chunk):
        sign = 1 - 2 * way
        place = outer - sign * (step - 1)
        return pltpu.make_async_remote_copy(
            src_ref=xs.at[place, chunk],
            dst_ref=xs.at[place, chunk],
            send_sem=line_send.at[way, step, chunk],
            recv_sem=line_recv.at[way, step, chunk],
            device_id=device(outer + sign, inner),
            device_id_type=pl.DeviceIdType.MESH,
        )

    def serve(source, chunk):
        all_out(source, chunk).wait_recv()
        taken = held[source, chunk].reshape(spots, width)
        gate = jnp.dot(taken, gate_w[chunk], preferred_element_type=jnp.float32)
        up = jnp.dot(taken, up_w[chunk], preferred_element_type=jnp.float32)

        def fresh():
            gate_acc[source] = gate
            up_acc[source] = up

        def add():
            gate_acc[source] += gate
            up_acc[source] += up

        pl.when(chunk == 0)(fresh)
        pl.when(chunk > 0)(add)
        pl.when(chunk == chunks - 1)(lambda: finish(source))

    def finish(source):
        gate = gate_acc[source]
        hidden = (gate / (1.0 + jnp.exp(-gate)) * up_acc[source]).astype(jnp.bfloat16)
        for chunk in range(chunks):
            part = slice(chunk * width, (chunk + 1) * width)
            result = jnp.dot(hidden, down_w[:, part], preferred_element_type=jnp.float32)
            served[source, chunk] = result.astype(jnp.bfloat16).reshape(plane, block, width)
            back[source, chunk, inner] = served[source, chunk, inner]

            def give(number, unused, chunk=chunk):
                back_copy(source, chunk, lax.rem(inner + number, plane)).start()
                return unused

            lax.fori_loop(1, plane, give, 0)

    def column(row):
        return jnp.sum(jnp.where(down_iota == over_iota, row, 0.0), axis=1, keepdims=True)

    def combine(way, source, chunk):
        def prepare():
            spot = lax.broadcasted_iota(jnp.int32, (rows, spots), 1).astype(jnp.float32)
            for route in range(top):
                at = column(slots[source, route : route + 1, :])
                picks[way, route] = jnp.where(spot == at, 1.0, 0.0).astype(jnp.bfloat16)
                scale = column(weights[source, route : route + 1, :])
                scales[way, route] = jnp.broadcast_to(scale, scales.shape[2:])

        pl.when(chunk == 0)(prepare)
        all_back(source, chunk).wait_recv()
        came = back[source, chunk].reshape(spots, width)
        chosen = picks[way].reshape(top * rows, spots)
        picked = jnp.dot(chosen, came, preferred_element_type=jnp.float32)
        total = None
        for route in range(top):
            term = picked[route * rows : (route + 1) * rows] * scales[way, route][:, 0:1]
            total = term if total is None else total + term

        def keep():
            own_sum[chunk] = total

        def hand():
            given[source, chunk] = total.astype(jnp.bfloat16)
            pl.when(jnp.logical_not(on_line(outer - (1 - 2 * (1 - way)))))(
                lambda: sum_copy(1 - way, source, chunk).start()
            )

        pl.when(way == 2)(keep)
        pl.when(way < 2)(hand)

    ahead = 2 * (2 * outer - (steps - 1))
    delays = (jnp.maximum(ahead, 0), jnp.maximum(-ahead, 0))

    def pass_sums(number, unused):
        for way in range(2):
            at = number - delays[way]
            turn = at // chunks
            chunk = lax.rem(at, chunks)
            dest = steps - 1 - turn if way == 0 else turn
            beyond = (dest > outer) if way == 0 else (dest < outer)
            live = (at >= 0) & (turn < steps - 1) & beyond & on_line(outer - (1 - 2 * way))

            def add(way=way, dest=dest, chunk=chunk):
                sum_copy(way, dest, chunk).wait_recv()
                given[dest, chunk] = (
                    given[dest, chunk].astype(jnp.float32)
                    + brought[dest, chunk].astype(jnp.float32)
                ).astype(jnp.bfloat16)
                sum_copy(way, dest, chunk).start()

            pl.when(live)(add)
        return unused

    edge = (outer == 0) | (outer == steps - 1)
    serve_lag = jnp.where(edge, EDGE_SERVE_LAG, SERVE_LAG)
    combine_lag = jnp.where(edge, EDGE_COMBINE_LAG, COMBINE_LAG)
    pl.semaphore_wait(barrier, peers)
    for way in range(2):
        send_own(way, order[: 2 + half])
        pl.when(depth[way] == 0)(lambda way=way: send_own(way, order[2 + half :]))
    for copy in loads[:3]:
        copy.wait()

    def own_rows(chunk, unused):
        choose(outer, chunk)
        hand_out(outer, chunk)
        return unused

    place_rows(outer)
    lax.fori_loop(0, chunks, own_rows, 0)

    def stage(number, unused):
        def load_weights():
            for copy in loads[3:]:
                copy.wait()

        def each_way(way, unused):
            full = jnp.where(way == 0, depth[0], depth[1])

            def take():
                receive(way, number, full)

                def rest():
                    for part in order[2 + half :]:
                        line_copy(way, 1, part, True).start()

                pl.when((number == full * chunks - 1) & on_line(outer + 1 - 2 * way))(rest)
                step, chunk, source = place_of(way, number, full)
                dispatch(source, chunk)

            pl.when(number < full * chunks)(take)
            return unused

        lax.fori_loop(0, 2, each_way, 0)
        pl.when(number == 0)(load_weights)

        def serve_way(way, unused):
            full = jnp.where(way == 0, depth[0], depth[1])
            at = number - serve_lag
            step, chunk, source = place_of(way, at, full)
            mine = way == 2
            source = jnp.where(mine, outer, source)
            chunk = jnp.where(mine, number, chunk)
            live = jnp.where(mine, number < chunks, (at >= 0) & (at < full * chunks))
            pl.when(live)(lambda: serve(source, chunk))
            return unused

        lax.fori_loop(0, 3, serve_way, 0)

        def combine_way(turn, unused):
            way = turn // 2
            full = jnp.where(way == 0, depth[0], depth[1])
            start = (full + 1) * half - 1 + serve_lag + combine_lag
            raw = 2 * (number - start) + lax.rem(turn, 2)
            later = raw - 2 * gap
            mine = way == 2
            at = jnp.where(raw < chunks, raw, later)
            at = jnp.where(mine, 2 * (number - (chunks + combine_lag)) + lax.rem(turn, 2), at)
            timely = mine | (raw < chunks) | (later >= chunks)
            source = jnp.where(mine, outer, outer - (1 - 2 * way) * (full - at // chunks))
            limit = jnp.where(mine, chunks, full * chunks)
            live = timely & (at >= 0) & (at < limit)
            pl.when(live)(lambda: combine(way, source, lax.rem(at, chunks)))
            return unused

        lax.fori_loop(0, 6, combine_way, 0)
        deep = jnp.maximum(depth[0], depth[1])
        opening = (deep + 1) * half - 1 + serve_lag + combine_lag + PASS_LAG

        def pass_one(turn, unused):
            def go():
                pass_sums(2 * (number - opening) + turn, 0)

            pl.when(number >= opening)(go)
            return unused

        lax.fori_loop(0, 2, pass_one, 0)
        return unused

    gap = jnp.where(edge, 0, PASS_GAP)
    most = max(SERVE_LAG + COMBINE_LAG, EDGE_SERVE_LAG + EDGE_COMBINE_LAG)
    last = chunks * (steps - 1) + most + chunks + PASS_LAG + half * (steps - 1)
    lax.fori_loop(0, last, stage, 0)

    def gather(chunk):
        def from_way(way, unused):
            def add():
                sum_copy(way, outer, chunk).wait_recv()
                slot = jnp.where(way == 0, outer, steps)
                own_sum[chunk] += brought[slot, chunk].astype(jnp.float32)

            pl.when(on_line(outer - (1 - 2 * way)))(add)
            return unused

        lax.fori_loop(0, 2, from_way, 0)
        own_sum[chunk] += alpha_mix * x_ref[chunk].astype(jnp.float32)

    over_chunks(gather)
    features = chunks * width
    total = None
    for chunk in range(chunks):
        term = jnp.sum(own_sum[chunk], axis=1, keepdims=True)
        total = term if total is None else total + term
    center = total / features
    total = None
    for chunk in range(chunks):
        term = jnp.sum(jnp.square(own_sum[chunk] - center), axis=1, keepdims=True)
        total = term if total is None else total + term
    spread = lax.rsqrt(total / features + eps_norm)
    for chunk in range(chunks):
        part = slice(chunk * width, (chunk + 1) * width)
        o_ref[:, part] = (
            (own_sum[chunk] - center) * spread * gain_ref[:, part] + bias_ref[:, part]
        ).astype(o_ref.dtype)

    def settle(step, unused):
        def sent(way, source):
            def onward():
                for part in range(parts):
                    line_copy(way, step + 1, part).wait_send()

            pl.when(on_line(outer + 1 - 2 * way))(onward)

            def one(chunk):
                all_out(source, chunk).wait_send()
                all_back(source, chunk).wait_send()
                pl.when(step > 0)(lambda: sum_copy(1 - way, source, chunk).wait_send())

            over_chunks(one)

        def own_up(way, unused):
            pl.when((step == 0) & (way == 1) & on_line(outer - 1))(own_down)
            return unused

        def own_down():
            for part in range(parts):
                line_copy(1, 1, part).wait_send()

        over_ways(step, sent)
        own_up(1, 0)
        return unused

    lax.fori_loop(0, steps, settle, 0)


def run_experts(x, routes, route_weights, gate, up, down, gain, bias, sp_size, tp_size):
    pair = 2 if sp_size % 2 == 0 else 1
    steps, plane = sp_size // pair, pair * tp_size
    chunks, rows, width = x.shape
    top = routes.shape[1]
    hidden = gate.shape[2]
    spots = plane * (2 * rows * top // (sp_size * tp_size))
    bf16, f32, dma = jnp.bfloat16, jnp.float32, pltpu.SemaphoreType.DMA
    blocks = pltpu.VMEM((steps, chunks, plane, spots // plane, width), bf16)
    return pl.pallas_call(
        functools.partial(expert_kernel, steps, plane, tp_size),
        out_shape=jax.ShapeDtypeStruct((rows, chunks * width), bf16),
        in_specs=[VMEM] * 3 + [ANY] * 3 + [VMEM] * 2,
        out_specs=VMEM,
        scratch_shapes=[
            pltpu.VMEM((steps, chunks, rows, width), bf16),
            pltpu.VMEM((steps, top, rows), jnp.int32),
            pltpu.VMEM((steps, top, rows), f32),
            pltpu.VMEM((steps, top, rows), f32),
            blocks,
            blocks,
            blocks,
            blocks,
            pltpu.VMEM((steps, chunks, rows, width), bf16),
            pltpu.VMEM((steps + 1, chunks, rows, width), bf16),
            pltpu.VMEM((chunks, rows, width), f32),
            pltpu.VMEM((steps, spots, hidden), f32),
            pltpu.VMEM((steps, spots, hidden), f32),
            pltpu.VMEM((steps, spots, rows), bf16),
            pltpu.VMEM((3, top, rows, spots), bf16),
            pltpu.VMEM((3, top, rows, HEAD), f32),
            pltpu.VMEM((chunks, width, hidden), gate.dtype),
            pltpu.VMEM((chunks, width, hidden), up.dtype),
            pltpu.VMEM(down.shape[1:], down.dtype),
            dma((2, steps + 1, chunks + 2)),
            dma((2, steps + 1, chunks + 2)),
            dma((steps, chunks)),
            dma((steps, chunks)),
            dma((steps, chunks)),
            dma((steps, chunks)),
            dma((2, steps, chunks)),
            dma((2, steps, chunks)),
            dma((6,)),
        ],
        compiler_params=pltpu.CompilerParams(
            collective_id=2, has_side_effects=True, vmem_limit_bytes=60 * 1024 * 1024
        ),
    )(
        x,
        routes.T,
        route_weights.T,
        gate.reshape(chunks, width, hidden),
        up.reshape(chunks, width, hidden),
        down.reshape(down.shape[1:]),
        gain[None, :],
        bias[None, :],
    )


def per_device(
    queries,
    key_heads,
    value_heads,
    documents,
    query_gain,
    key_gain,
    out_gain,
    out_proj,
    residual,
    mid_gain,
    mid_bias,
    routes,
    route_weights,
    expert_gate,
    expert_up,
    expert_down,
    final_gain,
    final_bias,
):
    sp_size = lax.axis_size("sp")
    tp_size = lax.axis_size("tp")
    if key_heads.shape[1] != HEAD or expert_gate.shape[0] != 1:
        raise ValueError("unsupported placement")
    middle = run_front(
        queries,
        key_heads,
        value_heads,
        documents,
        query_gain,
        key_gain,
        out_gain,
        out_proj,
        residual,
        mid_gain,
        mid_bias,
        sp_size,
        tp_size,
        CHUNKS,
    )
    return run_experts(
        middle,
        routes,
        route_weights,
        expert_gate,
        expert_up,
        expert_down,
        final_gain,
        final_bias,
        sp_size,
        tp_size,
    )


def solution(mesh):
    return jax.shard_map(
        per_device,
        mesh=mesh,
        in_specs=(
            P("sp", "tp"),
            P("sp", "tp"),
            P("sp", "tp"),
            P("sp"),
            P(),
            P(),
            P(),
            P(),
            P(("sp", "tp"), None),
            P(),
            P(),
            P(("sp", "tp"), None),
            P(("sp", "tp"), None),
            P(("sp", "tp"), None, None),
            P(("sp", "tp"), None, None),
            P(("sp", "tp"), None, None),
            P(),
            P(),
        ),
        out_specs=P(("sp", "tp"), None),
        check_vma=False,
    )
```

```python
import functools

import jax
import jax.numpy as jnp
import numpy as np
from jax import lax
from jax.experimental import pallas as pl
from jax.experimental.pallas import tpu as pltpu
from jax.sharding import PartitionSpec as P

HEAD = 128
GRID = 64
LONGEST = (5, 8)
CHUNKS = 4
SERVE_LAG = 4
COMBINE_LAG = 2
EDGE_SERVE_LAG = 2
EDGE_COMBINE_LAG = 0
PASS_LAG = 2
PASS_GAP = 2


eps_norm = 1e-06
alpha_mix = 8.0**0.25
theta_base = 10000.0
score_factor = HEAD ** (-0.5) * 1.4426950408889634
VMEM = pl.BlockSpec(memory_space=pltpu.VMEM)
ANY = pl.BlockSpec(memory_space=pl.ANY)
SMEM = pl.BlockSpec(memory_space=pltpu.SMEM)


def layer_norm(stream, gain_vec, bias_vec):
    center = jnp.mean(stream, axis=-1, keepdims=True)
    spread = jnp.mean(jnp.square(stream - center), axis=-1, keepdims=True)
    return (stream - center) * lax.rsqrt(spread + eps_norm) * gain_vec + bias_vec


def turned(values, gain, cosine, sine):
    inv_rms = lax.rsqrt(jnp.mean(values * values, axis=1, keepdims=True) + eps_norm)
    values = values * inv_rms * gain
    return (values * cosine + pltpu.roll(values, HEAD // 2, 1) * sine).astype(jnp.bfloat16)


def front_kernel(
    size,
    pair,
    tp_size,
    q_ref,
    k_ref,
    v_ref,
    doc_ref,
    q_gain_ref,
    k_gain_ref,
    freq_ref,
    gain_ref,
    proj_hbm,
    res_ref,
    mid_gain_ref,
    mid_bias_ref,
    mid_ref,
    kv,
    docs,
    qdoc_ref,
    row_ref,
    col_ref,
    q_rot,
    m_ref,
    l_ref,
    acc_ref,
    o_buf,
    whole,
    proj,
    line_send,
    line_recv,
    mate_send,
    mate_recv,
    tp_send,
    tp_recv,
    own_sem,
):
    me = lax.axis_index("sp")
    lane = lax.axis_index("tp")
    inner = lax.rem(me, pair)
    outer = me // pair
    steps = size // pair
    mate = outer * pair + lax.rem(inner + 1, pair)
    rows = k_ref.shape[0]
    pieces = doc_ref.shape[0]
    grouped = q_rot.shape[0] // rows
    parts = 3

    load = pltpu.make_async_copy(proj_hbm, proj, own_sem.at[0])
    load.start()
    own = [
        pltpu.make_async_copy(v_ref, kv.at[me, 1], own_sem.at[1]),
        pltpu.make_async_copy(doc_ref, docs.at[me], own_sem.at[2]),
    ]
    for copy in own:
        copy.start()

    def on_line(place):
        return (place >= 0) & (place < steps)

    barrier = pltpu.get_barrier_semaphore()

    def greet(target):
        pl.semaphore_signal(
            barrier, inc=1, device_id=target, device_id_type=pl.DeviceIdType.MESH
        )

    peers = jnp.int32(tp_size - 1 + (pair - 1))
    for sign in (1, -1):
        there = on_line(outer + sign)
        pl.when(there)(lambda sign=sign: greet({"sp": (outer + sign) * pair + inner}))
        peers = peers + there.astype(jnp.int32)
    if pair == 2:
        greet({"sp": mate})
    tp_targets = [lax.rem(lane + step, tp_size) for step in range(1, tp_size)]
    for target in tp_targets:
        greet({"tp": target})

    def piece(place, part, first):
        if part == 2:
            return (doc_ref if first else docs.at[place]), docs.at[place]
        return (v_ref if first and part == 1 else kv.at[place, part]), kv.at[place, part]

    def line_copy(way, step, part, first=False):
        sign = 1 - 2 * way
        place = (outer - sign * (step - 1)) * pair + inner
        src, dst = piece(place, part, first)
        return pltpu.make_async_remote_copy(
            src_ref=src,
            dst_ref=dst,
            send_sem=line_send.at[way, step, part],
            recv_sem=line_recv.at[way, step, part],
            device_id={"sp": (outer + sign) * pair + inner},
            device_id_type=pl.DeviceIdType.MESH,
        )

    def mate_copy(way, step, part, first=False):
        sign = 1 - 2 * way
        place = (outer - sign * step) * pair + inner
        src, dst = piece(place, part, first)
        return pltpu.make_async_remote_copy(
            src_ref=src,
            dst_ref=dst,
            send_sem=mate_send.at[way, step, part],
            recv_sem=mate_recv.at[way, step, part],
            device_id={"sp": mate},
            device_id_type=pl.DeviceIdType.MESH,
        )

    def send_own(part):
        for way in range(2):
            pl.when(on_line(outer + 1 - 2 * way))(
                lambda way=way: line_copy(way, 1, part, True).start()
            )
        if pair == 2:
            mate_copy(0, 0, part, True).start()

    lanes = lax.broadcasted_iota(jnp.int32, (1, HEAD), 1)
    along = lax.rem(lanes, HEAD // 2) < HEAD // 4
    side = jnp.where(lanes < HEAD // 2, -1.0, 1.0)
    first_row = (me * (rows // GRID)).astype(jnp.float32)
    for table, start, mask in ((row_ref, first_row, along), (col_ref, 0.0, ~along)):
        numbers = lax.broadcasted_iota(jnp.int32, table.shape[1:], 0).astype(jnp.float32)
        angles = (numbers + start) * freq_ref[...]
        table[0] = jnp.where(mask, jnp.cos(angles), 0.0)
        table[1] = jnp.where(mask, jnp.sin(angles) * side, 0.0)
    grid_rows = row_ref.shape[1]
    span = col_ref.shape[1]

    def tables(block):
        cosine = row_ref[0, pl.ds(block, 1)] + col_ref[0]
        sine = row_ref[1, pl.ds(block, 1)] + col_ref[1]
        return cosine, sine

    def turn_keys(block, unused):
        cosine, sine = tables(block)
        here = pl.ds(pl.multiple_of(block * span, span), span)
        kv[me, 0, here] = turned(k_ref[here].astype(jnp.float32), k_gain_ref[...], cosine, sine)
        return unused

    lax.fori_loop(0, grid_rows, turn_keys, 0)
    pl.semaphore_wait(barrier, peers)
    for part in (1, 2, 0):
        send_own(part)

    def turn_queries(block, unused):
        cosine, sine = tables(block)
        here = pl.ds(pl.multiple_of(block * span, span), span)
        for head in range(grouped):
            there = pl.ds(pl.multiple_of(head * rows + block * span, span), span)
            q_rot[there] = turned(
                q_ref[here, head * HEAD : (head + 1) * HEAD].astype(jnp.float32),
                q_gain_ref[...],
                cosine,
                sine,
            )
        return unused

    lax.fori_loop(0, grid_rows, turn_queries, 0)
    down = lax.broadcasted_iota(jnp.int32, (HEAD, HEAD), 0)
    over = lax.broadcasted_iota(jnp.int32, (HEAD, HEAD), 1)
    for number in range(pieces):
        named = doc_ref[number : number + 1].astype(jnp.float32)
        column = jnp.sum(jnp.where(down == over, named, 0.0), axis=1, keepdims=True)
        column = jnp.broadcast_to(column, (HEAD, HEAD)).astype(jnp.int32)
        for head in range(grouped):
            qdoc_ref[pl.ds(head * rows + number * HEAD, HEAD)] = column
    m_ref[...] = jnp.full(m_ref.shape, -1e30, jnp.float32)
    l_ref[...] = jnp.zeros(l_ref.shape, jnp.float32)
    acc_ref[...] = jnp.zeros(acc_ref.shape, jnp.float32)
    for copy in own:
        copy.wait()

    def advance(place):
        keys = kv[place, 0]
        values = kv[place, 1]
        doc_rows = docs[place]
        key_docs = jnp.concatenate([doc_rows[i : i + 1] for i in range(pieces)], axis=1)
        scores = lax.dot_general(
            q_rot[...], keys, (((1,), (1,)), ((), ())), preferred_element_type=jnp.float32
        )
        allowed = qdoc_ref[:, 0:1] == key_docs
        scores = jnp.where(allowed, scores * score_factor, -1e30)
        old_max = m_ref[...]
        new_max = jnp.maximum(old_max, jnp.max(scores, axis=1, keepdims=True))
        base = jnp.maximum(new_max[:, 0:1], -1e29)
        weights = jnp.exp2(scores - base)
        rescale = jnp.exp2(old_max - new_max)
        l_ref[...] = l_ref[...] * rescale + jnp.sum(weights, axis=1, keepdims=True)
        acc_ref[...] = acc_ref[...] * rescale + jnp.dot(
            weights.astype(jnp.bfloat16), values, preferred_element_type=jnp.float32
        )
        m_ref[...] = new_max

    reach = (size * rows * LONGEST[0] // LONGEST[1] - 2) // rows + 1

    def receive(step):
        for group in ((1, 2), (0,)):
            for way in range(2):
                sign = 1 - 2 * way

                def take(way=way, sign=sign, group=group):
                    for part in group:
                        line_copy(way, step, part).wait_recv()

                    def pass_on():
                        for part in group:
                            line_copy(way, step + 1, part).start()

                    pl.when(on_line(outer + sign))(pass_on)
                    if pair == 2:
                        for part in group:
                            mate_copy(way, step, part).start()

                pl.when((step > 0) & on_line(outer - sign * step))(take)

    def stage(step, unused):
        def visit(number, unused):
            way = lax.rem(number, 2)
            across = number // 2
            there = outer - (1 - 2 * way) * step

            def work():
                if pair == 2:

                    def arrive():
                        for part in range(parts):
                            mate_copy(way, step, part).wait_recv()

                    pl.when(across == 1)(arrive)
                block = there * pair + lax.rem(inner + across, pair)
                close = (block - me <= reach) & (me - block <= reach)
                pl.when(close)(lambda: advance(block))

            pl.when(on_line(there) & ((step > 0) | (way == 0)))(work)
            return unused

        lax.fori_loop(0, 2, visit, 0)
        pl.when(step + 1 < steps)(lambda: receive(step + 1))
        lax.fori_loop(2, 2 * pair, visit, 0)
        return unused

    lax.fori_loop(0, steps, stage, 0)
    for head in range(grouped):
        o_buf[:, head * HEAD : (head + 1) * HEAD] = (
            acc_ref[head * rows : (head + 1) * rows] / l_ref[head * rows : (head + 1) * rows]
        ).astype(
            o_buf.dtype
        )

    out_rows, width = whole.shape[0], o_buf.shape[1]

    def rows_of(number):
        return pl.ds(pl.multiple_of(number * out_rows, out_rows), out_rows)

    mine = whole.at[:, pl.ds(pl.multiple_of(lane * width, width), width)]
    swaps = []
    for step, target in enumerate(tp_targets):
        copy = pltpu.make_async_remote_copy(
            src_ref=o_buf.at[rows_of(target)],
            dst_ref=mine,
            send_sem=tp_send.at[step],
            recv_sem=tp_recv.at[step],
            device_id={"tp": target},
            device_id_type=pl.DeviceIdType.MESH,
        )
        copy.start()
        swaps.append(copy)
    keep = pltpu.make_async_copy(o_buf.at[rows_of(lane)], mine, own_sem.at[3])
    keep.start()

    load.wait()
    for copy in swaps:
        copy.wait_recv()
    keep.wait()
    taken = whole[...].astype(jnp.float32)
    mean_square = jnp.mean(taken * taken, axis=1, keepdims=True)
    scaled = (taken * gain_ref[...]).astype(jnp.bfloat16)
    projected = jnp.dot(scaled, proj[...], preferred_element_type=jnp.float32)
    projected = projected * lax.rsqrt(mean_square + eps_norm)
    stream = alpha_mix * res_ref[...].astype(jnp.float32) + projected
    middle = layer_norm(stream, mid_gain_ref[...], mid_bias_ref[...]).astype(jnp.bfloat16)
    block = mid_ref.shape[2]
    for chunk in range(mid_ref.shape[0]):
        mid_ref[chunk] = middle[:, chunk * block : (chunk + 1) * block]

    for copy in swaps:
        copy.wait_send()

    def settle(step, unused):
        for way in range(2):
            sign = 1 - 2 * way

            def sent(way=way):
                for part in range(parts):
                    line_copy(way, step + 1, part).wait_send()

            pl.when(on_line(outer - sign * step) & on_line(outer + sign))(sent)
            if pair == 2:

                def gave(way=way):
                    for part in range(parts):
                        mate_copy(way, step, part).wait_send()

                first = (step > 0) | (way == 0)
                pl.when(on_line(outer - sign * step) & first)(gave)
        return unused

    lax.fori_loop(0, steps, settle, 0)


def run_front(
    queries,
    keys,
    values,
    documents,
    query_gain,
    key_gain,
    out_gain,
    out_proj,
    residual,
    mid_gain,
    mid_bias,
    size,
    tp_size,
    chunks,
):
    pair = 2 if size % 2 == 0 else 1
    rows, width = queries.shape
    grouped = width // HEAD
    out_rows, model_width = residual.shape
    steps = size // pair
    pair_count = HEAD // 4
    inv_freq = theta_base ** (-np.arange(pair_count, dtype=np.float32) / pair_count)
    dma = pltpu.SemaphoreType.DMA
    return pl.pallas_call(
        functools.partial(front_kernel, size, pair, tp_size),
        out_shape=pltpu.VMEM((chunks, out_rows, model_width // chunks), jnp.bfloat16),
        in_specs=[VMEM] * 8 + [ANY] + [VMEM] * 3,
        out_specs=VMEM,
        scratch_shapes=[
            pltpu.VMEM((size, 2, rows, HEAD), jnp.bfloat16),
            pltpu.VMEM((size, rows // HEAD, HEAD), jnp.int32),
            pltpu.VMEM((grouped * rows, HEAD), jnp.int32),
            pltpu.VMEM((2, rows // GRID, HEAD), jnp.float32),
            pltpu.VMEM((2, GRID, HEAD), jnp.float32),
            pltpu.VMEM((grouped * rows, HEAD), jnp.bfloat16),
            pltpu.VMEM((grouped * rows, HEAD), jnp.float32),
            pltpu.VMEM((grouped * rows, HEAD), jnp.float32),
            pltpu.VMEM((grouped * rows, HEAD), jnp.float32),
            pltpu.VMEM((rows, width), jnp.bfloat16),
            pltpu.VMEM((out_rows, width * tp_size), jnp.bfloat16),
            pltpu.VMEM(out_proj.shape, out_proj.dtype),
            dma((2, steps + 1, 3)),
            dma((2, steps + 1, 3)),
            dma((2, steps, 3)),
            dma((2, steps, 3)),
            dma((tp_size,)),
            dma((tp_size,)),
            dma((4,)),
        ],
        compiler_params=pltpu.CompilerParams(
            collective_id=0, has_side_effects=True, vmem_limit_bytes=56 * 1024 * 1024
        ),
    )(
        queries,
        keys,
        values,
        documents.reshape(rows // HEAD, HEAD),
        query_gain[None, :],
        key_gain[None, :],
        np.tile(inv_freq.astype(np.float32), 4)[None, :],
        out_gain[None, :],
        out_proj,
        residual,
        mid_gain[None, :],
        mid_bias[None, :],
    )


def expert_kernel(
    steps,
    plane,
    tp_size,
    x_ref,
    route_ref,
    weight_ref,
    gate_hbm,
    up_hbm,
    down_hbm,
    gain_ref,
    bias_ref,
    o_ref,
    xs,
    routes,
    weights,
    slots,
    outb,
    held,
    served,
    back,
    given,
    brought,
    own_sum,
    gate_acc,
    up_acc,
    selects,
    picks,
    scales,
    gate_w,
    up_w,
    down_w,
    line_send,
    line_recv,
    out_send,
    out_recv,
    back_send,
    back_recv,
    sum_send,
    sum_recv,
    own_sem,
):
    me = lax.axis_index("sp") * tp_size + lax.axis_index("tp")
    outer = me // plane
    inner = lax.rem(me, plane)
    chunks, rows, width = x_ref.shape
    block = outb.shape[3]
    spots = plane * block
    top = route_ref.shape[0]
    parts = chunks + 2
    order = [chunks, chunks + 1] + list(range(chunks))

    loads = [
        pltpu.make_async_copy(x_ref, xs.at[outer], own_sem.at[0]),
        pltpu.make_async_copy(route_ref, routes.at[outer], own_sem.at[1]),
        pltpu.make_async_copy(weight_ref, weights.at[outer], own_sem.at[2]),
        pltpu.make_async_copy(gate_hbm, gate_w, own_sem.at[3]),
        pltpu.make_async_copy(up_hbm, up_w, own_sem.at[4]),
        pltpu.make_async_copy(down_hbm, down_w, own_sem.at[5]),
    ]
    for copy in loads:
        copy.start()

    def device(place, number):
        index = place * plane + number
        return {"sp": index // tp_size, "tp": lax.rem(index, tp_size)}

    def on_line(place):
        return (place >= 0) & (place < steps)

    barrier = pltpu.get_barrier_semaphore()

    def greet(place, number):
        pl.semaphore_signal(
            barrier,
            inc=1,
            device_id=device(place, number),
            device_id_type=pl.DeviceIdType.MESH,
        )

    peers = jnp.int32(plane - 1)
    for sign in (1, -1):
        there = on_line(outer + sign)
        pl.when(there)(lambda sign=sign: greet(outer + sign, inner))
        peers = peers + there.astype(jnp.int32)

    def greet_plane(step, unused):
        greet(outer, lax.rem(inner + step, plane))
        return unused

    lax.fori_loop(1, plane, greet_plane, 0)

    def piece(place, part, first):
        if part == chunks:
            return (route_ref if first else routes.at[place]), routes.at[place]
        if part == chunks + 1:
            return (weight_ref if first else weights.at[place]), weights.at[place]
        return (x_ref.at[part] if first else xs.at[place, part]), xs.at[place, part]

    def line_copy(way, step, part, first=False):
        sign = 1 - 2 * way
        place = outer - sign * (step - 1)
        src, dst = piece(place, part, first)
        return pltpu.make_async_remote_copy(
            src_ref=src,
            dst_ref=dst,
            send_sem=line_send.at[way, step, part],
            recv_sem=line_recv.at[way, step, part],
            device_id=device(outer + sign, inner),
            device_id_type=pl.DeviceIdType.MESH,
        )

    half = chunks // 2
    depth = (outer, steps - 1 - outer)

    def send_own(way, send):
        there = on_line(outer + 1 - 2 * way)
        for part in send:
            pl.when(there)(lambda part=part: line_copy(way, 1, part, True).start())

    def out_copy(source, chunk, target):
        return pltpu.make_async_remote_copy(
            src_ref=outb.at[source, chunk, target],
            dst_ref=held.at[source, chunk, inner],
            send_sem=out_send.at[source, chunk],
            recv_sem=out_recv.at[source, chunk],
            device_id=device(outer, target),
            device_id_type=pl.DeviceIdType.MESH,
        )

    def back_copy(source, chunk, target):
        return pltpu.make_async_remote_copy(
            src_ref=served.at[source, chunk, target],
            dst_ref=back.at[source, chunk, inner],
            send_sem=back_send.at[source, chunk],
            recv_sem=back_recv.at[source, chunk],
            device_id=device(outer, target),
            device_id_type=pl.DeviceIdType.MESH,
        )

    def others(from_buffer, to_buffer, source, chunk, send_sem, recv_sem):
        return pltpu.make_async_remote_copy(
            src_ref=from_buffer.at[source, chunk, pl.ds(0, plane - 1)],
            dst_ref=to_buffer.at[source, chunk, pl.ds(0, plane - 1)],
            send_sem=send_sem.at[source, chunk],
            recv_sem=recv_sem.at[source, chunk],
            device_id=device(outer, inner),
            device_id_type=pl.DeviceIdType.MESH,
        )

    def all_out(source, chunk):
        return others(outb, held, source, chunk, out_send, out_recv)

    def all_back(source, chunk):
        return others(served, back, source, chunk, back_send, back_recv)

    def sum_copy(way, dest, chunk):
        target = outer + 1 - 2 * way
        slot = jnp.where((dest == target) & (way == 1), steps, dest)
        return pltpu.make_async_remote_copy(
            src_ref=given.at[dest, chunk],
            dst_ref=brought.at[slot, chunk],
            send_sem=sum_send.at[way, dest, chunk],
            recv_sem=sum_recv.at[way, dest, chunk],
            device_id=device(target, inner),
            device_id_type=pl.DeviceIdType.MESH,
        )

    def over_ways(step, act):
        def one(way, unused):
            source = outer - (1 - 2 * way) * step
            pl.when(on_line(source) & ((step > 0) | (way == 0)))(lambda: act(way, source))
            return unused

        lax.fori_loop(0, 2, one, 0)

    def over_chunks(act):
        def one(chunk, unused):
            act(chunk)
            return unused

        lax.fori_loop(0, chunks, one, 0)

    down_iota = lax.broadcasted_iota(jnp.int32, (rows, rows), 0)
    over_iota = lax.broadcasted_iota(jnp.int32, (rows, rows), 1)

    def place_rows(source):
        earlier = jnp.where(down_iota < over_iota, 1.0, 0.0).astype(jnp.bfloat16)
        names = outer * plane + lax.broadcasted_iota(jnp.int32, (plane, rows), 0)
        start = lax.broadcasted_iota(jnp.int32, (plane, rows), 0).astype(jnp.float32) * block
        passed = jnp.zeros((plane, 1), jnp.float32)
        for route in range(top):
            one_hot = jnp.where(names == routes[source, route : route + 1, :], 1.0, 0.0)
            before = passed + jnp.dot(
                one_hot.astype(jnp.bfloat16), earlier, preferred_element_type=jnp.float32
            )
            there = jnp.sum(one_hot, axis=0, keepdims=True)
            slot = jnp.sum((before + start) * one_hot, axis=0, keepdims=True)
            slots[source, route : route + 1, :] = slot + there - 1.0
            passed = passed + jnp.sum(one_hot, axis=1, keepdims=True)
        spot = lax.broadcasted_iota(jnp.int32, (spots, rows), 0).astype(jnp.float32)
        chosen = spot == slots[source, 0:1, :]
        for route in range(1, top):
            chosen = chosen | (spot == slots[source, route : route + 1, :])
        selects[source] = jnp.where(chosen, 1.0, 0.0).astype(jnp.bfloat16)

    def dispatch(source, chunk):
        pl.when(chunk == 0)(lambda: place_rows(source))
        choose(source, chunk)
        hand_out(source, chunk)

    def choose(source, chunk):
        picked = jnp.dot(selects[source], xs[source, chunk], preferred_element_type=jnp.float32)
        outb[source, chunk] = picked.astype(jnp.bfloat16).reshape(plane, block, width)
        held[source, chunk, inner] = outb[source, chunk, inner]

    def hand_out(source, chunk):
        def give(number, unused):
            out_copy(source, chunk, lax.rem(inner + number, plane)).start()
            return unused

        lax.fori_loop(1, plane, give, 0)

    def place_of(way, number, full):
        pairs = number // half
        out = pairs < full
        step = jnp.where(out, pairs + 1, 2 * full - pairs)
        chunk = jnp.where(out, 0, half) + lax.rem(number, half)
        return step, chunk, outer - (1 - 2 * way) * step

    def receive(way, number, full):
        step, chunk, source = place_of(way, number, full)

        def small():
            for part in order[:2]:
                wait_part(way, step, part)

        pl.when(chunk == 0)(small)
        line_dynamic(way, step, chunk).wait_recv()
        pl.when(on_line(outer + 1 - 2 * way))(
            lambda: line_dynamic(way, step + 1, chunk).start()
        )

    def wait_part(way, step, part):
        line_copy(way, step, part).wait_recv()
        pl.when(on_line(outer + 1 - 2 * way))(lambda: line_copy(way, step + 1, part).start())

    def line_dynamic(way, step, chunk):
        sign = 1 - 2 * way
        place = outer - sign * (step - 1)
        return pltpu.make_async_remote_copy(
            src_ref=xs.at[place, chunk],
            dst_ref=xs.at[place, chunk],
            send_sem=line_send.at[way, step, chunk],
            recv_sem=line_recv.at[way, step, chunk],
            device_id=device(outer + sign, inner),
            device_id_type=pl.DeviceIdType.MESH,
        )

    def serve(source, chunk):
        all_out(source, chunk).wait_recv()
        taken = held[source, chunk].reshape(spots, width)
        gate = jnp.dot(taken, gate_w[chunk], preferred_element_type=jnp.float32)
        up = jnp.dot(taken, up_w[chunk], preferred_element_type=jnp.float32)

        def fresh():
            gate_acc[source] = gate
            up_acc[source] = up

        def add():
            gate_acc[source] += gate
            up_acc[source] += up

        pl.when(chunk == 0)(fresh)
        pl.when(chunk > 0)(add)
        pl.when(chunk == chunks - 1)(lambda: finish(source))

    def finish(source):
        gate = gate_acc[source]
        hidden = (gate / (1.0 + jnp.exp(-gate)) * up_acc[source]).astype(jnp.bfloat16)
        for chunk in range(chunks):
            part = slice(chunk * width, (chunk + 1) * width)
            result = jnp.dot(hidden, down_w[:, part], preferred_element_type=jnp.float32)
            served[source, chunk] = result.astype(jnp.bfloat16).reshape(plane, block, width)
            back[source, chunk, inner] = served[source, chunk, inner]

            def give(number, unused, chunk=chunk):
                back_copy(source, chunk, lax.rem(inner + number, plane)).start()
                return unused

            lax.fori_loop(1, plane, give, 0)

    def column(row):
        return jnp.sum(jnp.where(down_iota == over_iota, row, 0.0), axis=1, keepdims=True)

    def combine(way, source, chunk):
        def prepare():
            spot = lax.broadcasted_iota(jnp.int32, (rows, spots), 1).astype(jnp.float32)
            for route in range(top):
                at = column(slots[source, route : route + 1, :])
                picks[way, route] = jnp.where(spot == at, 1.0, 0.0).astype(jnp.bfloat16)
                scale = column(weights[source, route : route + 1, :])
                scales[way, route] = jnp.broadcast_to(scale, scales.shape[2:])

        pl.when(chunk == 0)(prepare)
        all_back(source, chunk).wait_recv()
        came = back[source, chunk].reshape(spots, width)
        chosen = picks[way].reshape(top * rows, spots)
        picked = jnp.dot(chosen, came, preferred_element_type=jnp.float32)
        total = None
        for route in range(top):
            term = picked[route * rows : (route + 1) * rows] * scales[way, route][:, 0:1]
            total = term if total is None else total + term

        def keep():
            own_sum[chunk] = total

        def hand():
            given[source, chunk] = total.astype(jnp.bfloat16)
            pl.when(jnp.logical_not(on_line(outer - (1 - 2 * (1 - way)))))(
                lambda: sum_copy(1 - way, source, chunk).start()
            )

        pl.when(way == 2)(keep)
        pl.when(way < 2)(hand)

    ahead = 2 * (2 * outer - (steps - 1))
    delays = (jnp.maximum(ahead, 0), jnp.maximum(-ahead, 0))

    def pass_sums(number, unused):
        for way in range(2):
            at = number - delays[way]
            turn = at // chunks
            chunk = lax.rem(at, chunks)
            dest = steps - 1 - turn if way == 0 else turn
            beyond = (dest > outer) if way == 0 else (dest < outer)
            live = (at >= 0) & (turn < steps - 1) & beyond & on_line(outer - (1 - 2 * way))

            def add(way=way, dest=dest, chunk=chunk):
                sum_copy(way, dest, chunk).wait_recv()
                given[dest, chunk] = (
                    given[dest, chunk].astype(jnp.float32)
                    + brought[dest, chunk].astype(jnp.float32)
                ).astype(jnp.bfloat16)
                sum_copy(way, dest, chunk).start()

            pl.when(live)(add)
        return unused

    edge = (outer == 0) | (outer == steps - 1)
    serve_lag = jnp.where(edge, EDGE_SERVE_LAG, SERVE_LAG)
    combine_lag = jnp.where(edge, EDGE_COMBINE_LAG, COMBINE_LAG)
    pl.semaphore_wait(barrier, peers)
    for way in range(2):
        send_own(way, order[: 2 + half])
        pl.when(depth[way] == 0)(lambda way=way: send_own(way, order[2 + half :]))
    for copy in loads[:3]:
        copy.wait()

    def own_rows(chunk, unused):
        choose(outer, chunk)
        hand_out(outer, chunk)
        return unused

    place_rows(outer)
    lax.fori_loop(0, chunks, own_rows, 0)

    def stage(number, unused):
        def load_weights():
            for copy in loads[3:]:
                copy.wait()

        def each_way(way, unused):
            full = jnp.where(way == 0, depth[0], depth[1])

            def take():
                receive(way, number, full)

                def rest():
                    for part in order[2 + half :]:
                        line_copy(way, 1, part, True).start()

                pl.when((number == full * chunks - 1) & on_line(outer + 1 - 2 * way))(rest)
                step, chunk, source = place_of(way, number, full)
                dispatch(source, chunk)

            pl.when(number < full * chunks)(take)
            return unused

        lax.fori_loop(0, 2, each_way, 0)
        pl.when(number == 0)(load_weights)

        def serve_way(way, unused):
            full = jnp.where(way == 0, depth[0], depth[1])
            at = number - serve_lag
            step, chunk, source = place_of(way, at, full)
            mine = way == 2
            source = jnp.where(mine, outer, source)
            chunk = jnp.where(mine, number, chunk)
            live = jnp.where(mine, number < chunks, (at >= 0) & (at < full * chunks))
            pl.when(live)(lambda: serve(source, chunk))
            return unused

        lax.fori_loop(0, 3, serve_way, 0)

        def combine_way(turn, unused):
            way = turn // 2
            full = jnp.where(way == 0, depth[0], depth[1])
            start = (full + 1) * half - 1 + serve_lag + combine_lag
            raw = 2 * (number - start) + lax.rem(turn, 2)
            later = raw - 2 * gap
            mine = way == 2
            at = jnp.where(raw < chunks, raw, later)
            at = jnp.where(mine, 2 * (number - (chunks + combine_lag)) + lax.rem(turn, 2), at)
            timely = mine | (raw < chunks) | (later >= chunks)
            source = jnp.where(mine, outer, outer - (1 - 2 * way) * (full - at // chunks))
            limit = jnp.where(mine, chunks, full * chunks)
            live = timely & (at >= 0) & (at < limit)
            pl.when(live)(lambda: combine(way, source, lax.rem(at, chunks)))
            return unused

        lax.fori_loop(0, 6, combine_way, 0)
        deep = jnp.maximum(depth[0], depth[1])
        opening = (deep + 1) * half - 1 + serve_lag + combine_lag + PASS_LAG

        def pass_one(turn, unused):
            def go():
                pass_sums(2 * (number - opening) + turn, 0)

            pl.when(number >= opening)(go)
            return unused

        lax.fori_loop(0, 2, pass_one, 0)
        return unused

    gap = jnp.where(edge, 0, PASS_GAP)
    most = max(SERVE_LAG + COMBINE_LAG, EDGE_SERVE_LAG + EDGE_COMBINE_LAG)
    last = chunks * (steps - 1) + most + chunks + PASS_LAG + half * (steps - 1)
    lax.fori_loop(0, last, stage, 0)

    def gather(chunk):
        def from_way(way, unused):
            def add():
                sum_copy(way, outer, chunk).wait_recv()
                slot = jnp.where(way == 0, outer, steps)
                own_sum[chunk] += brought[slot, chunk].astype(jnp.float32)

            pl.when(on_line(outer - (1 - 2 * way)))(add)
            return unused

        lax.fori_loop(0, 2, from_way, 0)
        own_sum[chunk] += alpha_mix * x_ref[chunk].astype(jnp.float32)

    over_chunks(gather)
    features = chunks * width
    total = None
    for chunk in range(chunks):
        term = jnp.sum(own_sum[chunk], axis=1, keepdims=True)
        total = term if total is None else total + term
    center = total / features
    total = None
    for chunk in range(chunks):
        term = jnp.sum(jnp.square(own_sum[chunk] - center), axis=1, keepdims=True)
        total = term if total is None else total + term
    spread = lax.rsqrt(total / features + eps_norm)
    for chunk in range(chunks):
        part = slice(chunk * width, (chunk + 1) * width)
        o_ref[:, part] = (
            (own_sum[chunk] - center) * spread * gain_ref[:, part] + bias_ref[:, part]
        ).astype(o_ref.dtype)

    def settle(step, unused):
        def sent(way, source):
            def onward():
                for part in range(parts):
                    line_copy(way, step + 1, part).wait_send()

            pl.when(on_line(outer + 1 - 2 * way))(onward)

            def one(chunk):
                all_out(source, chunk).wait_send()
                all_back(source, chunk).wait_send()
                pl.when(step > 0)(lambda: sum_copy(1 - way, source, chunk).wait_send())

            over_chunks(one)

        def own_up(way, unused):
            pl.when((step == 0) & (way == 1) & on_line(outer - 1))(own_down)
            return unused

        def own_down():
            for part in range(parts):
                line_copy(1, 1, part).wait_send()

        over_ways(step, sent)
        own_up(1, 0)
        return unused

    lax.fori_loop(0, steps, settle, 0)


def run_experts(x, routes, route_weights, gate, up, down, gain, bias, sp_size, tp_size):
    pair = 2 if sp_size % 2 == 0 else 1
    steps, plane = sp_size // pair, pair * tp_size
    chunks, rows, width = x.shape
    top = routes.shape[1]
    hidden = gate.shape[2]
    spots = plane * (2 * rows * top // (sp_size * tp_size))
    bf16, f32, dma = jnp.bfloat16, jnp.float32, pltpu.SemaphoreType.DMA
    blocks = pltpu.VMEM((steps, chunks, plane, spots // plane, width), bf16)
    return pl.pallas_call(
        functools.partial(expert_kernel, steps, plane, tp_size),
        out_shape=jax.ShapeDtypeStruct((rows, chunks * width), bf16),
        in_specs=[VMEM] * 3 + [ANY] * 3 + [VMEM] * 2,
        out_specs=VMEM,
        scratch_shapes=[
            pltpu.VMEM((steps, chunks, rows, width), bf16),
            pltpu.VMEM((steps, top, rows), jnp.int32),
            pltpu.VMEM((steps, top, rows), f32),
            pltpu.VMEM((steps, top, rows), f32),
            blocks,
            blocks,
            blocks,
            blocks,
            pltpu.VMEM((steps, chunks, rows, width), bf16),
            pltpu.VMEM((steps + 1, chunks, rows, width), bf16),
            pltpu.VMEM((chunks, rows, width), f32),
            pltpu.VMEM((steps, spots, hidden), f32),
            pltpu.VMEM((steps, spots, hidden), f32),
            pltpu.VMEM((steps, spots, rows), bf16),
            pltpu.VMEM((3, top, rows, spots), bf16),
            pltpu.VMEM((3, top, rows, HEAD), f32),
            pltpu.VMEM((chunks, width, hidden), gate.dtype),
            pltpu.VMEM((chunks, width, hidden), up.dtype),
            pltpu.VMEM(down.shape[1:], down.dtype),
            dma((2, steps + 1, chunks + 2)),
            dma((2, steps + 1, chunks + 2)),
            dma((steps, chunks)),
            dma((steps, chunks)),
            dma((steps, chunks)),
            dma((steps, chunks)),
            dma((2, steps, chunks)),
            dma((2, steps, chunks)),
            dma((6,)),
        ],
        compiler_params=pltpu.CompilerParams(
            collective_id=2, has_side_effects=True, vmem_limit_bytes=60 * 1024 * 1024
        ),
    )(
        x,
        routes.T,
        route_weights.T,
        gate.reshape(chunks, width, hidden),
        up.reshape(chunks, width, hidden),
        down.reshape(down.shape[1:]),
        gain[None, :],
        bias[None, :],
    )


def per_device(
    queries,
    key_heads,
    value_heads,
    documents,
    query_gain,
    key_gain,
    out_gain,
    out_proj,
    residual,
    mid_gain,
    mid_bias,
    routes,
    route_weights,
    expert_gate,
    expert_up,
    expert_down,
    final_gain,
    final_bias,
):
    sp_size = lax.axis_size("sp")
    tp_size = lax.axis_size("tp")
    if key_heads.shape[1] != HEAD or expert_gate.shape[0] != 1:
        raise ValueError("unsupported placement")
    middle = run_front(
        queries,
        key_heads,
        value_heads,
        documents,
        query_gain,
        key_gain,
        out_gain,
        out_proj,
        residual,
        mid_gain,
        mid_bias,
        sp_size,
        tp_size,
        CHUNKS,
    )
    return run_experts(
        middle,
        routes,
        route_weights,
        expert_gate,
        expert_up,
        expert_down,
        final_gain,
        final_bias,
        sp_size,
        tp_size,
    )


def solution(mesh):
    return jax.shard_map(
        per_device,
        mesh=mesh,
        in_specs=(
            P("sp", "tp"),
            P("sp", "tp"),
            P("sp", "tp"),
            P("sp"),
            P(),
            P(),
            P(),
            P(),
            P(("sp", "tp"), None),
            P(),
            P(),
            P(("sp", "tp"), None),
            P(("sp", "tp"), None),
            P(("sp", "tp"), None, None),
            P(("sp", "tp"), None, None),
            P(("sp", "tp"), None, None),
            P(),
            P(),
        ),
        out_specs=P(("sp", "tp"), None),
        check_vma=False,
    )
```
